512 devices in a mesh: gr: 2 (over z_hi), sp: 32 (over z_lo, y), tp: 8 (over x, core).
Axes of the slice: x: 4, y: 4, z: 16 (z_hi: 2, z_lo: 8; z = z_hi * 8 + z_lo), core: 2. Of those that a mesh axis runs over, the one named last changes fastest.
Arguments:
- tokens: bfloat16 [8, 8192, 2048], P('gr', 'sp'), parts along dimension 0, may hold values from -6 to 6
- new_rows: bfloat16 [8, 2048], P('gr'), parts along dimension 0, may hold values from -6 to 6
- new_query: bfloat16 [8, 1024], P('gr', 'tp'), parts along dimension 0, may hold values from -6 to 6
- norm_gain: bfloat16 [2048], replicated, may hold values from 0.099609375 to 1.8984375
- key_weight: bfloat16 [2048, 1024], P('sp', 'tp'), may hold values from -0.125 to 0.125
- value_weight: bfloat16 [2048, 2048], P('sp', 'tp'), may hold values from -0.125 to 0.125
- input_weight: bfloat16 [2048, 16], replicated, may hold values from -0.125 to 0.125
- forget_weight: bfloat16 [2048, 16], replicated, may hold values from -0.125 to 0.125
- forget_bias: float32 [16], P('tp'), may hold values from 3 to 12
- gate_offsets: float32 [8, 8192, 2, 16], P('gr', 'sp', None, 'tp'), parts along dimension 0, may hold values from -6 to 250, as said below
Outputs:
- cache_keys: bfloat16 [64, 1024, 1024], P(('gr', 'sp'), None, 'tp'), parts along dimension 0
- cache_values: bfloat16 [64, 1024, 2048], P(('gr', 'sp'), None, 'tp'), parts along dimension 0
- cache_weights: float32 [64, 16, 1024], P(('gr', 'sp'), 'tp'), parts along dimension 0
- first_read: bfloat16 [8, 2048], P('gr', 'tp'), parts along dimension 0
The draws below stay inside these ranges and needn't reach their ends.
There are 2 independent parts, one for each index of `gr`. The reference program is written for one: setup_inputs(seed, part) draws one part's arguments, and reference() takes and returns one part's arrays. A program takes and returns all parts, laid end to end along the dimension named above; an argument that names none is the same for every part. Nothing has to cross between parts.
Inputs may be any that keep to these rules, and one draw needn't show every extreme that they name: `gate_offsets`: entry 1 along the third dimension is never positive.
All inputs are finite; a program needn't handle non-finite values.
Results may differ from the reference program's by a relative error of at most 0.012.
The reference program's roundings to bfloat16 on the way count: a program that leaves them out, or rounds other values in their place, can miss the bound.
Values may be sent and summed in bfloat16 or wider, within the bound.
A program may use at most 64 MiB of HBM per device.

```python
import math
import jax
import jax.numpy as jnp
from jax import lax

D = 2048
HEADS = 16
DK = 64
DV = 128
SEQS = 4
CONTEXT_SPAN = 8192
PIECES = 8
SUB = 32
N_SP = 32


def draw_forget_bias(key, part):
    pick_key, slow_key, fast_key = jax.random.split(key, 3)
    fast_share = 0.5
    is_fast = jax.random.uniform(pick_key, (HEADS,), jnp.float32) < fast_share
    slow_bias = math.log(3.3 * CONTEXT_SPAN) + jax.random.uniform(slow_key, (HEADS,), jnp.float32, -0.3, 0.3)
    fast_bias = math.log(60.0) + jax.random.uniform(fast_key, (HEADS,), jnp.float32, -0.5, 0.5)
    return jnp.where(is_fast, fast_bias, slow_bias).astype(jnp.float32)


def draw_gate_offsets(key, part):
    incomplete_key_vectors = jax.random.split(key, 4)
    tensor_dimension_count = (SEQS, CONTEXT_SPAN, HEADS)
    block_rate = jnp.exp(jax.random.uniform(incomplete_key_vectors[0], (SEQS, CONTEXT_SPAN // 32, HEADS), jnp.float32, math.log(0.25), 0.0))
    entire_throughput = jnp.repeat(block_rate, 32, axis=1)
    transfer_aligned = jax.random.uniform(incomplete_key_vectors[1], tensor_dimension_count, jnp.float32) < 2.0 / CONTEXT_SPAN
    transfer_span = jnp.log(jax.random.uniform(incomplete_key_vectors[2], tensor_dimension_count, jnp.float32, 0.5, 0.8))
    forgetting_shift = -entire_throughput / CONTEXT_SPAN + jnp.where(transfer_aligned, transfer_span, 0.0)
    input_shift = jnp.clip(jax.random.normal(incomplete_key_vectors[3], tensor_dimension_count, jnp.float32), -6.0, 6.0)
    return jnp.stack([input_shift, forgetting_shift], axis=2).astype(jnp.float32)


def shard_levels(key, extent, cuts, low, high):
    def one(dim, shards_of):
        steps = jax.random.uniform(jax.random.fold_in(jax.random.fold_in(key, 6), dim), (shards_of,), jnp.float32, low / len(cuts), high / len(cuts))
        return jnp.repeat(jnp.exp(steps), extent[dim] // shards_of).reshape((-1,) + (1,) * (len(extent) - dim - 1))

    level = one(*cuts[0])
    for cut in cuts[1:]:
        level = level * one(*cut)
    return level


def noise(rng, extent, spread, bound, cuts=(), dtype=jnp.bfloat16):
    factor_of = shard_levels(rng, extent, cuts, -0.22, 0.18) if cuts else 1.0
    result = jax.random.normal(rng, extent, jnp.float32) * spread * factor_of
    return jnp.minimum(jnp.maximum(result, -bound), bound).astype(dtype)


def setup_inputs(seed: int = 0, part: int = 0) -> dict:
    seeds = jax.random.split(jax.random.key(seed), 11)
    part_keys = jax.random.split(jax.random.fold_in(seeds[10], part), 11)
    tokens = noise(part_keys[0], (SEQS, CONTEXT_SPAN, D), 1.0, 6.0, ((1, 32),))
    new_rows = noise(part_keys[1], (SEQS, D), 1.0, 6.0)
    new_query = noise(part_keys[2], (SEQS, HEADS * DK), 1.0, 6.0, ((1, 8),))
    norm_gain = jnp.clip(1.0 + 0.18 * jax.random.normal(seeds[3], (D,), jnp.float32), 0.099609375, 1.8984375).astype(jnp.bfloat16)
    key_weight = noise(seeds[4], (D, HEADS * DK), D ** -0.5, 0.125, ((0, 32), (1, 8)))
    value_weight = noise(seeds[5], (D, HEADS * DV), D ** -0.5, 0.125, ((0, 32), (1, 8)))
    input_weight = noise(seeds[6], (D, HEADS), D ** -0.5, 0.125)
    forget_weight = noise(seeds[7], (D, HEADS), D ** -0.5, 0.125)
    forget_bias = draw_forget_bias(jax.random.fold_in(seeds[10], 71), part)
    gate_offsets = draw_gate_offsets(jax.random.fold_in(jax.random.fold_in(seeds[10], part), 71), part)
    return {"tokens": tokens, "new_rows": new_rows, "new_query": new_query, "norm_gain": norm_gain, "key_weight": key_weight, "value_weight": value_weight, "input_weight": input_weight, "forget_weight": forget_weight, "forget_bias": forget_bias, "gate_offsets": gate_offsets}


EPSILON = 1e-06

def normed_rows(source, norm_gain):
    widened = source.astype(jnp.float32)
    inverse_rms = lax.rsqrt(lax.optimization_barrier(jnp.mean(widened * widened, axis=-1, keepdims=True)) + EPSILON)
    return (widened * inverse_rms * norm_gain.astype(jnp.float32)).astype(jnp.bfloat16)

def suffix_sums(log_forget):
    flipped = jnp.cumsum(jnp.flip(log_forget, 1), axis=1)
    return jnp.flip(flipped, 1) - log_forget

def cache_order(rows):
    width = rows.shape[-1]
    split = rows.reshape(SEQS, N_SP, PIECES, SUB, width)
    return jnp.transpose(split, (0, 2, 1, 3, 4)).reshape(SEQS * PIECES, N_SP * SUB, width)

def reference(tokens, new_rows, new_query, norm_gain, key_weight, value_weight, input_weight, forget_weight, forget_bias, gate_offsets):
    seq_count = tokens.shape[0]
    flat_rows = normed_rows(tokens, norm_gain).reshape(seq_count * CONTEXT_SPAN, D)
    key_rows = (jnp.dot(flat_rows, key_weight, preferred_element_type=jnp.float32) * DK ** (-0.5)).astype(jnp.bfloat16)
    value_rows = jnp.dot(flat_rows, value_weight, preferred_element_type=jnp.float32).astype(jnp.bfloat16)
    input_gate = jnp.dot(flat_rows, input_weight, preferred_element_type=jnp.float32).reshape(seq_count, CONTEXT_SPAN, HEADS) + gate_offsets[:, :, 0, :]
    forget_pre = jnp.dot(flat_rows, forget_weight, preferred_element_type=jnp.float32).reshape(seq_count, CONTEXT_SPAN, HEADS)
    log_forget = jax.nn.log_sigmoid(forget_pre + forget_bias) + gate_offsets[:, :, 1, :]
    log_weight = input_gate + suffix_sums(log_forget)
    peak_log = lax.optimization_barrier(jnp.max(log_weight, axis=1))
    query_heads = new_query.reshape(seq_count, HEADS, DK).astype(jnp.float32)
    key_heads = key_rows.reshape(seq_count, CONTEXT_SPAN, HEADS, DK).astype(jnp.float32)
    value_heads = value_rows.reshape(seq_count, CONTEXT_SPAN, HEADS, DV).astype(jnp.float32)
    scores = jnp.einsum('nhd,nshd->nsh', query_heads, key_heads)
    weighted_terms = jnp.exp(log_weight - peak_log[:, None, :]) * scores
    rounded = lax.optimization_barrier(weighted_terms.astype(jnp.bfloat16)).astype(jnp.float32)
    numerator = jnp.einsum('nsh,nshd->nhd', rounded, value_heads)
    denominator = lax.optimization_barrier(jnp.sum(weighted_terms, axis=1))
    fresh_rows = normed_rows(new_rows, norm_gain)
    key_new = (jnp.dot(fresh_rows, key_weight, preferred_element_type=jnp.float32) * DK ** (-0.5)).astype(jnp.bfloat16)
    value_new = jnp.dot(fresh_rows, value_weight, preferred_element_type=jnp.float32).astype(jnp.bfloat16)
    gate_new = jnp.dot(fresh_rows, input_weight, preferred_element_type=jnp.float32)
    peak_new = jnp.maximum(peak_log, gate_new)
    old_part = jnp.exp(peak_log - peak_new)
    own_score = jnp.einsum('nhd,nhd->nh', query_heads, key_new.reshape(seq_count, HEADS, DK).astype(jnp.float32))
    new_part = jnp.exp(gate_new - peak_new) * own_score
    total_value = old_part[..., None] * numerator + new_part[..., None] * value_new.reshape(seq_count, HEADS, DV).astype(jnp.float32)
    total_weight = old_part * denominator + new_part
    read_out = total_value / jnp.maximum(jnp.abs(total_weight), 1.0)[..., None]
    return (cache_order(key_rows.reshape(seq_count, CONTEXT_SPAN, HEADS * DK)), cache_order(value_rows.reshape(seq_count, CONTEXT_SPAN, HEADS * DV)), jnp.transpose(cache_order(log_weight), (0, 2, 1)), read_out.reshape(seq_count, HEADS * DV).astype(jnp.bfloat16))
```

```python
import jax
import jax.numpy as jnp
from jax import lax
from jax.experimental import pallas as pl
from jax.experimental.pallas import tpu as pltpu
from jax.sharding import PartitionSpec as P

EPSILON = 1e-06
MESH = pl.DeviceIdType.MESH
F32 = jnp.float32
BF16 = jnp.bfloat16
NT = (((1,), (1,)), ((), ()))

D = 2048
ROWS = 1024
GROUP = 256
BLOCK = 32
CHUNK = 64


def iota(shape, dim):
    return lax.broadcasted_iota(jnp.int32, shape, dim)


def xor2(a, b):
    return 2 * ((a // 2 + b // 2) % 2) + (a % 2 + b % 2) % 2


def norm_chunk(read, write, gain_ref, rows):
    total = jnp.zeros((rows, 128), F32)
    for c in range(D // 128):
        v = read(c).astype(F32)
        total = total + v * v
    inverse = lax.rsqrt(jnp.sum(total, axis=-1, keepdims=True) * (1.0 / D) + EPSILON)
    for c in range(D // 128):
        v = read(c).astype(F32)
        write(c, (v * inverse * gain_ref[:, c * 128 : (c + 1) * 128].astype(F32)).astype(BF16))


def norm_group(src, start, dst, gain_ref):
    def body(u, carry):
        at = pl.multiple_of(start + u * CHUNK, CHUNK)
        to = pl.multiple_of(u * CHUNK, CHUNK)

        def read(c):
            return src[pl.ds(at, CHUNK), c * 128 : (c + 1) * 128]

        def write(c, v):
            dst[pl.ds(to, CHUNK), c * 128 : (c + 1) * 128] = v

        norm_chunk(read, write, gain_ref, CHUNK)
        return carry

    lax.fori_loop(0, GROUP // CHUNK, body, 0)


def kernel(
    tokens,
    new_rows,
    new_query,
    gain,
    key_weight,
    value_weight,
    input_weight,
    forget_weight,
    bias,
    offsets,
    out_keys,
    out_values,
    out_weights,
    out_read,
    T,
    X,
    N,
    W,
    OK,
    OV,
    G,
    GW,
    NN,
    IG,
    PRE,
    LF,
    S,
    R,
    L,
    LW,
    PEAK,
    Q8,
    NUM,
    DEN,
    KVN,
    GN,
    FS,
    FR,
    A0,
    A1,
    p1s,
    p1r,
    xl,
    xr,
    xf,
    dr,
    xs,
    lws,
    lwr,
    wc,
    wh,
    w2,
    wy,
    ws1,
    ws2,
    fs,
    fr,
    loc,
):
    s = lax.axis_index("sp")
    t = lax.axis_index("tp")
    z, y = s // 4, s % 4
    x, c = t // 2, t % 2
    k_me = s // 8
    n_me = s // 8
    right = ((x + 1) % 4) * 2 + c
    left = ((x + 3) % 4) * 2 + c
    across = ((x + 2) % 4) * 2 + c
    mate = t + 1 - 2 * c

    barrier = pltpu.get_barrier_semaphore()

    def greet(o, carry):
        pl.semaphore_signal(barrier, inc=1, device_id={"sp": (s + o) % 32}, device_id_type=MESH)
        return carry

    lax.fori_loop(1, 32, greet, 0)
    for who in (right, left, mate):
        pl.semaphore_signal(barrier, inc=1, device_id={"tp": who}, device_id_type=MESH)

    own_k = pltpu.make_async_copy(key_weight, W.at[z, y, :, 0:128], loc.at[4])
    own_v = pltpu.make_async_copy(value_weight, W.at[z, y, :, 128:384], loc.at[5])
    own_k.start()
    own_v.start()
    loads = [
        pltpu.make_async_copy(tokens.at[n * GROUP : (n + 1) * GROUP], X.at[n * GROUP : (n + 1) * GROUP], loc.at[n])
        for n in range(4)
    ]
    for load in loads:
        load.start()

    GW[0:16, :] = input_weight[...]
    GW[16:32, :] = forget_weight[...]

    for n in range(4):
        loads[n].wait()

        def gates(n=n):
            norm_group(X, n * GROUP, N, gain)
            G[n] = lax.dot_general(GW[...], N[...], NT, preferred_element_type=F32)

        gates()

    gate_row = iota((32, GROUP), 0)
    for n in range(4):
        for h in range(2):
            at = slice(2 * n + h, 2 * n + h + 1)
            mine = jnp.where(gate_row == 2 * t + h, G[n], 0.0)
            IG[at, :] = jnp.sum(mine, axis=0, keepdims=True) + offsets[n, 0, h : h + 1, :]
            mine = jnp.where(gate_row == 16 + 2 * t + h, G[n], 0.0)
            PRE[at, :] = jnp.sum(mine, axis=0, keepdims=True) + bias[h]
            LF[at, :] = offsets[n, 1, h : h + 1, :]

    lane = iota((8, GROUP), 1)
    pre = PRE[...]
    soft = jnp.minimum(pre, 0.0) - jnp.log1p(jnp.exp(-jnp.abs(pre)))
    log_forget = soft + LF[...]
    suffix = log_forget
    step = 1
    while step < GROUP:
        suffix = suffix + jnp.where(lane < GROUP - step, pltpu.roll(suffix, GROUP - step, 1), 0.0)
        step *= 2
    exclusive = jnp.where(lane < GROUP - 1, pltpu.roll(suffix, GROUP - 1, 1), 0.0)
    local = IG[...] + exclusive
    total = jnp.broadcast_to(suffix[:, 0:1], (8, 128))
    most = jnp.broadcast_to(jnp.max(local, axis=1, keepdims=True), (8, 128))
    lane = iota((8, 128), 1)
    tail_part = jnp.where(
        lane < 80,
        total,
        jnp.where(lane < 96, pltpu.roll(total, 7, 0), jnp.where(lane < 112, most, pltpu.roll(most, 7, 0))),
    )
    for half in range(2):
        part = local[:, half * 128 : (half + 1) * 128]
        for k in range(4):
            first = pltpu.roll(part, (128 - 32 * k) % 128, 1) if k else part
            second = pltpu.roll(pltpu.roll(part, 7, 0), (160 - 32 * k) % 128, 1) if k != 1 else pltpu.roll(part, 7, 0)
            row = jnp.where(lane < 32, first, jnp.where(lane < 64, second, tail_part))
            for n in range(4):
                S[n * 8 + half * 4 + k] = row[2 * n : 2 * n + 1, :]
    R[pl.ds(s, 1)] = S[pl.ds(s, 1)]

    own_k.wait()
    own_v.wait()
    pl.semaphore_wait(barrier, 34)

    half_z = (z // 4) * 4
    other_z = 4 - half_z
    far_z = (z + 4) % 8

    def shard_to(row, to_z, recv):
        pltpu.make_async_remote_copy(
            src_ref=W.at[row, y],
            dst_ref=W.at[row, y],
            send_sem=ws1,
            recv_sem=recv,
            device_id={"sp": to_z * 4 + y},
            device_id_type=MESH,
        ).start()

    shard_to(z, far_z, wc)
    for o in range(1, 4):
        shard_to(z, half_z + (z + o) % 4, wh)

    def send_rows(o, carry):
        peer = (s + o) % 32
        pltpu.make_async_remote_copy(
            src_ref=S.at[peer],
            dst_ref=R.at[s],
            send_sem=lws,
            recv_sem=lwr,
            device_id={"sp": peer},
            device_id_type=MESH,
        ).start()
        return carry

    lax.fori_loop(1, 32, send_rows, 0)

    def slot(i):
        return xor2(k_me, (2 * i + 1) % 5)

    def first_leg(i):
        dest = (t - s + 32) % 8 + 8 * slot(i)
        src = tokens.at[pl.ds(pl.multiple_of(dest * BLOCK, BLOCK), BLOCK)]
        dst = T.at[pl.ds(pl.multiple_of(s * BLOCK, BLOCK), BLOCK)]
        remote = pltpu.make_async_remote_copy(
            src_ref=src,
            dst_ref=dst,
            send_sem=p1s.at[i],
            recv_sem=p1r.at[i],
            device_id={"sp": dest},
            device_id_type=MESH,
        )
        return dest, src, dst, remote

    def start_leg(i, carry):
        dest, src, dst, remote = first_leg(i)

        @pl.when(dest != s)
        def _():
            remote.start()

        @pl.when(dest == s)
        def _():
            pltpu.make_async_copy(src, dst, p1r.at[i]).start()

        return carry

    lax.fori_loop(0, 4, start_leg, 0)

    def y_send(rows, column, to_y, which):
        pltpu.make_async_remote_copy(
            src_ref=W.at[pl.ds(rows, 4), column],
            dst_ref=W.at[pl.ds(rows, 4), column],
            send_sem=ws2,
            recv_sem=wy.at[which],
            device_id={"sp": z * 4 + to_y},
            device_id_type=MESH,
        ).start()

    def arrived(ref, sem):
        pltpu.make_async_copy(ref, ref, sem).wait()

    up, down = (y + 1) % 4, (y + 3) % 4

    arrived(W.at[0, 0], wc)
    for o in range(1, 4):
        shard_to(far_z, half_z + (z + o) % 4, w2)
    arrived(W.at[0:3, 0], wh)
    y_send(half_z, y, up, 0)
    y_send(half_z, y, down, 1)

    arrived(R.at[0:31], lwr)
    received = R[:, 0, :]
    row = iota((32, 128), 0)
    suffix = received
    step = 1
    while step < 32:
        suffix = suffix + jnp.where(row < 32 - step, pltpu.roll(suffix, 32 - step, 0), 0.0)
        step *= 2
    exclusive = jnp.where(row < 31, pltpu.roll(suffix, 31, 0), 0.0)
    tail0, tail1 = exclusive[:, 64:65], exclusive[:, 80:81]
    lane32 = iota((32, 128), 1)
    peak0 = jnp.max(received[:, 96:97] + tail0, axis=0, keepdims=True)
    peak1 = jnp.max(received[:, 112:113] + tail1, axis=0, keepdims=True)
    L[...] = received + jnp.where(lane32 < 32, tail0, tail1)
    even = iota((8, 128), 0) % 2 == 0
    PEAK[...] = jnp.where(even, jnp.broadcast_to(peak0, (8, 128)), jnp.broadcast_to(peak1, (8, 128)))
    for h in range(2):
        wide = jnp.zeros((8, 128), F32)
        for k in range(4):
            rows = L[pl.ds(k, 8, stride=4), :]
            shift = (32 * k - 32 * h) % 128
            moved = pltpu.roll(rows, shift, 1) if shift else rows
            wide = jnp.where((lane >= 32 * k) & (lane < 32 * k + 32), moved, wide)
        for g in range(8):
            LW[h : h + 1, g * 128 : (g + 1) * 128] = wide[g : g + 1, :]
    out_weights[...] = LW[...]

    query = new_query[...].astype(F32)
    lane1 = iota((1, 128), 1)
    for n in range(4):
        Q8[2 * n : 2 * n + 1, :] = jnp.where(lane1 < 64, query[n : n + 1, :], 0.0)
        Q8[2 * n + 1 : 2 * n + 2, :] = jnp.where(lane1 < 64, 0.0, query[n : n + 1, :])

    NUM[...] = jnp.zeros_like(NUM)
    DEN[...] = jnp.zeros_like(DEN)

    def block_of(owner, i):
        at = ((owner - s + 32) % 8 + 8 * slot(i)) * BLOCK
        return T.at[pl.ds(pl.multiple_of(at, BLOCK), BLOCK)]

    def pass_on(owner, i, to, recv):
        block = block_of(owner, i)
        pltpu.make_async_remote_copy(
            src_ref=block,
            dst_ref=block,
            send_sem=xs,
            recv_sem=recv,
            device_id={"tp": to},
            device_id_type=MESH,
        ).start()

    one_block = T.at[0:BLOCK]

    def stage_a(i):
        arrived(one_block, p1r.at[i])
        pass_on(t, i, right, xl.at[i])
        pass_on(t, i, left, xr.at[i])
        pass_on(t, i, mate, dr.at[i])

    def stage_b(i):
        arrived(one_block, xl.at[i])

        @pl.when(i % 2 == 0)
        def _():
            pass_on(left, i, right, xf.at[i])

        pass_on(left, i, mate, dr.at[i])
        arrived(one_block, xr.at[i])

        @pl.when(i % 2 == 1)
        def _():
            pass_on(right, i, left, xf.at[i])

        pass_on(right, i, mate, dr.at[i])

    def stage_c(i):
        arrived(one_block, xf.at[i])
        pass_on(across, i, mate, dr.at[i])

    def write_out(i):
        at = pl.ds(pl.multiple_of(slot(i) * GROUP, GROUP), GROUP)
        return (
            pltpu.make_async_copy(OK.at[at], out_keys.at[at], loc.at[6]),
            pltpu.make_async_copy(OV.at[at], out_values.at[at], loc.at[7]),
        )

    def stage_d(i):
        arrived(T.at[0 : 4 * BLOCK], dr.at[i])
        start = pl.multiple_of(slot(i) * GROUP, GROUP)
        norm_group(T, start, N, gain)
        both = jnp.dot(N[...], W[...].reshape(D, 384), preferred_element_type=F32)
        keys = (both[:, 0:128] * 0.125).astype(BF16)
        values = both[:, 128:384].astype(BF16)
        OK[pl.ds(start, GROUP), :] = keys
        OV[pl.ds(start, GROUP), :] = values
        scores = lax.dot_general(Q8[...].astype(BF16), keys, NT, preferred_element_type=F32)
        weights = LW[:, pl.ds(start, GROUP)]
        rows = iota((8, GROUP), 0)
        weights = jnp.where(rows % 2 == 0, weights[0:1, :], weights[1:2, :])
        terms = jnp.exp(weights - PEAK[:, 0:1]) * scores
        terms = jnp.where(rows // 2 == n_me, terms, 0.0)
        DEN[...] += jnp.broadcast_to(jnp.sum(terms, axis=1, keepdims=True), (8, 128))
        NUM[...] += jnp.dot(terms.astype(BF16), values, preferred_element_type=F32)
        for copy in write_out(i):
            copy.start()

    def along(j, carry):
        @pl.when(j < 4)
        def _():
            stage_a(j)
            stage_b(j)

        @pl.when(j == 0)
        def _():
            arrived(W.at[0:4, 0], wy.at[0])
            y_send(half_z, down, up, 2)
            arrived(W.at[0:3, 0], w2)
            y_send(other_z, y, up, 3)
            y_send(other_z, y, down, 4)

        @pl.when(j == 1)
        def _():
            arrived(W.at[0:4, 0], wy.at[4])
            y_send(other_z, up, down, 5)

        @pl.when((j >= 1) & (j < 5))
        def _():
            stage_c(j - 1)

        @pl.when(j == 2)
        def _():
            for which in (1, 2, 3, 5):
                arrived(W.at[0:4, 0], wy.at[which])
            wide = new_rows[...].astype(F32)
            inverse = lax.rsqrt(jnp.mean(wide * wide, axis=-1, keepdims=True) + EPSILON)
            NN[0:4, :] = wide * inverse * gain[...].astype(F32)
            NN[4:8, :] = jnp.zeros((4, D), F32)
            fresh = NN[...].astype(BF16)
            KVN[...] = jnp.dot(fresh, W[...].reshape(D, 384), preferred_element_type=F32)
            GN[...] = lax.dot_general(fresh, GW[...], NT, preferred_element_type=F32)

        @pl.when(j >= 2)
        def _():
            stage_d(j - 2)

        return carry

    lax.fori_loop(0, 6, along, 0)

    evens = (iota((8, 128), 0) % 2 == 0).astype(F32)
    odds = 1.0 - evens
    FS[0:1, :] = jnp.sum(NUM[:, 0:128] * evens, axis=0, keepdims=True)
    FS[1:2, :] = jnp.sum(NUM[:, 128:256] * odds, axis=0, keepdims=True)
    den0 = jnp.sum(DEN[...] * evens, axis=0, keepdims=True)
    den1 = jnp.sum(DEN[...] * odds, axis=0, keepdims=True)
    FS[2:3, :] = jnp.where(lane1 < 64, den0, den1)
    FS[3:4, :] = jnp.where(lane1 < 64, PEAK[0:1, :], PEAK[1:2, :])
    FR[pl.ds(s, 1)] = FS[...].reshape(1, 4, 128)

    def send_read(o, carry):
        pltpu.make_async_remote_copy(
            src_ref=FS,
            dst_ref=FR.at[s],
            send_sem=fs,
            recv_sem=fr,
            device_id={"sp": (s + o) % 32},
            device_id_type=MESH,
        ).start()
        return carry

    lax.fori_loop(1, 32, send_read, 0)

    own_head = iota((8, 32), 1)
    gate0 = jnp.sum(jnp.where(own_head == 2 * t, GN[...], 0.0), axis=1, keepdims=True)[0:4]
    gate1 = jnp.sum(jnp.where(own_head == 2 * t + 1, GN[...], 0.0), axis=1, keepdims=True)[0:4]
    key_new = (KVN[0:4, 0:128] * 0.125).astype(BF16).astype(F32)
    value_new = KVN[0:4, 128:384].astype(BF16).astype(F32)
    product = query * key_new
    lane4 = iota((4, 128), 1)
    own0 = jnp.sum(jnp.where(lane4 < 64, product, 0.0), axis=1, keepdims=True)
    own1 = jnp.sum(jnp.where(lane4 < 64, 0.0, product), axis=1, keepdims=True)

    arrived(OK, loc.at[6])
    arrived(OV, loc.at[7])

    arrived(FR.at[0:31], fr)
    for n in range(4):
        group = FR[n * 8 : n * 8 + 8]
        added = jnp.sum(group, axis=0)
        A0[n : n + 1, :] = added[0:1, :]
        A0[4 + n : 5 + n, :] = added[1:2, :]
        A1[n : n + 1, :] = added[2:3, :]
        A1[4 + n : 5 + n, :] = group[0, 3:4, :]

    for h, (gate, own) in enumerate(((gate0, own0), (gate1, own1))):
        numerator = A0[4 * h : 4 * h + 4, :]
        denominator = A1[0:4, 64 * h : 64 * h + 1]
        peak = A1[4:8, 64 * h : 64 * h + 1]
        top = jnp.maximum(peak, gate)
        old_part = jnp.exp(peak - top)
        new_part = jnp.exp(gate - top) * own
        value = old_part * numerator + new_part * value_new[:, h * 128 : (h + 1) * 128]
        weight = old_part * denominator + new_part
        out_read[:, h * 128 : (h + 1) * 128] = (value / jnp.maximum(jnp.abs(weight), 1.0)).astype(BF16)

    arrived(R.at[0:31], lws)
    arrived(FR.at[0:31], fs)
    arrived(W.at[0:7, 0], ws1)
    arrived(W.at[0:6], ws2)
    arrived(T.at[0 : 28 * BLOCK], xs)

    def leg_done(i, carry):
        dest, _, _, remote = first_leg(i)

        @pl.when(dest != s)
        def _():
            remote.wait_send()

        return carry

    lax.fori_loop(0, 4, leg_done, 0)


def per_device(
    tokens,
    new_rows,
    new_query,
    norm_gain,
    key_weight,
    value_weight,
    input_weight,
    forget_weight,
    forget_bias,
    gate_offsets,
):
    any_space = pl.BlockSpec(memory_space=pl.ANY)
    vmem = pl.BlockSpec(memory_space=pltpu.VMEM)
    smem = pl.BlockSpec(memory_space=pltpu.SMEM)
    dma = pltpu.SemaphoreType.DMA
    keys, values, weights, read = pl.pallas_call(
        kernel,
        out_shape=(
            jax.ShapeDtypeStruct((ROWS, 128), BF16),
            jax.ShapeDtypeStruct((ROWS, 256), BF16),
            jax.ShapeDtypeStruct((2, ROWS), F32),
            jax.ShapeDtypeStruct((4, 256), BF16),
        ),
        in_specs=[any_space, vmem, vmem, vmem, any_space, any_space, vmem, vmem, smem, vmem],
        out_specs=(any_space, any_space, vmem, vmem),
        scratch_shapes=[
            pltpu.VMEM((ROWS, D), BF16),
            pltpu.VMEM((ROWS, D), BF16),
            pltpu.VMEM((GROUP, D), BF16),
            pltpu.VMEM((8, 4, 64, 384), BF16),
            pltpu.VMEM((ROWS, 128), BF16),
            pltpu.VMEM((ROWS, 256), BF16),
            pltpu.VMEM((4, 32, GROUP), F32),
            pltpu.VMEM((32, D), BF16),
            pltpu.VMEM((8, D), F32),
            pltpu.VMEM((8, GROUP), F32),
            pltpu.VMEM((8, GROUP), F32),
            pltpu.VMEM((8, GROUP), F32),
            pltpu.VMEM((32, 1, 128), F32),
            pltpu.VMEM((32, 1, 128), F32),
            pltpu.VMEM((32, 128), F32),
            pltpu.VMEM((2, ROWS), F32),
            pltpu.VMEM((8, 128), F32),
            pltpu.VMEM((8, 128), F32),
            pltpu.VMEM((8, 256), F32),
            pltpu.VMEM((8, 128), F32),
            pltpu.VMEM((8, 384), F32),
            pltpu.VMEM((8, 32), F32),
            pltpu.VMEM((4, 128), F32),
            pltpu.VMEM((32, 4, 128), F32),
            pltpu.VMEM((8, 128), F32),
            pltpu.VMEM((8, 128), F32),
            dma((4,)),
            dma((4,)),
            dma((4,)),
            dma((4,)),
            dma((4,)),
            dma((4,)),
            dma,
            dma,
            dma,
            dma,
            dma,
            dma,
            dma((6,)),
            dma,
            dma,
            dma,
            dma,
            dma((8,)),
        ],
        compiler_params=pltpu.CompilerParams(collective_id=0, has_side_effects=True),
    )(
        tokens.reshape(ROWS, D),
        new_rows,
        new_query,
        norm_gain.reshape(1, D),
        key_weight,
        value_weight,
        input_weight.T,
        forget_weight.T,
        forget_bias,
        jnp.transpose(gate_offsets, (0, 2, 3, 1)),
    )
    return keys[None], values[None], weights[None], read


def solution(mesh):
    return jax.shard_map(
        per_device,
        mesh=mesh,
        in_specs=(
            P("gr", "sp", None),
            P("gr", None),
            P("gr", "tp"),
            P(),
            P("sp", "tp"),
            P("sp", "tp"),
            P(),
            P(),
            P("tp"),
            P("gr", "sp", None, "tp"),
        ),
        out_specs=(
            P(("gr", "sp"), None, "tp"),
            P(("gr", "sp"), None, "tp"),
            P(("gr", "sp"), "tp", None),
            P("gr", "tp"),
        ),
        check_vma=False,
    )
```

```python
import jax
import jax.numpy as jnp
from jax import lax
from jax.experimental import pallas as pl
from jax.experimental.pallas import tpu as pltpu
from jax.sharding import PartitionSpec as P

EPSILON = 1e-06
MESH = pl.DeviceIdType.MESH
F32 = jnp.float32
BF16 = jnp.bfloat16
NT = (((1,), (1,)), ((), ()))

D = 2048
ROWS = 1024
GROUP = 256
BLOCK = 32
CHUNK = 64


def iota(shape, dim):
    return lax.broadcasted_iota(jnp.int32, shape, dim)


def xor2(a, b):
    return 2 * ((a // 2 + b // 2) % 2) + (a % 2 + b % 2) % 2


def norm_chunk(read, write, gain_ref, rows):
    total = jnp.zeros((rows, 128), F32)
    for c in range(D // 128):
        v = read(c).astype(F32)
        total = total + v * v
    inverse = lax.rsqrt(jnp.sum(total, axis=-1, keepdims=True) * (1.0 / D) + EPSILON)
    for c in range(D // 128):
        v = read(c).astype(F32)
        write(c, (v * inverse * gain_ref[c : c + 1, :].astype(F32)).astype(BF16))


def norm_group(src, start, dst, gain_ref):
    def body(u, carry):
        at = pl.multiple_of(start + u * CHUNK, CHUNK)
        to = pl.multiple_of(u * CHUNK, CHUNK)

        def read(c):
            return src[pl.ds(at, CHUNK), c * 128 : (c + 1) * 128]

        def write(c, v):
            dst[pl.ds(to, CHUNK), c * 128 : (c + 1) * 128] = v

        norm_chunk(read, write, gain_ref, CHUNK)
        return carry

    lax.fori_loop(0, GROUP // CHUNK, body, 0)


def kernel(
    tokens,
    new_rows_in,
    new_query_in,
    gain_in,
    key_weight,
    value_weight,
    input_weight,
    forget_weight,
    bias,
    offsets_in,
    out_keys,
    out_values,
    out_weights,
    out_read,
    new_rows,
    new_query,
    gain,
    offsets,
    T,
    X,
    N,
    W,
    OK,
    OV,
    G,
    GW,
    NN,
    IG,
    PRE,
    LF,
    S,
    R,
    L,
    LW,
    PEAK,
    Q8,
    NUM,
    DEN,
    KVN,
    GN,
    FS,
    FR,
    A0,
    A1,
    p1s,
    p1r,
    xl,
    xr,
    xf,
    dr,
    xs,
    lws,
    lwr,
    wc,
    wh,
    w2,
    wy,
    ws1,
    ws2,
    fs,
    fr,
    loc,
):
    s = lax.axis_index("sp")
    t = lax.axis_index("tp")
    z, y = s // 4, s % 4
    x, c = t // 2, t % 2
    k_me = s // 8
    n_me = s // 8
    right = ((x + 1) % 4) * 2 + c
    left = ((x + 3) % 4) * 2 + c
    across = ((x + 2) % 4) * 2 + c
    mate = t + 1 - 2 * c

    barrier = pltpu.get_barrier_semaphore()

    def greet(o, carry):
        pl.semaphore_signal(barrier, inc=1, device_id={"sp": (s + o) % 32}, device_id_type=MESH)
        return carry

    lax.fori_loop(1, 32, greet, 0)
    for who in (right, left, mate):
        pl.semaphore_signal(barrier, inc=1, device_id={"tp": who}, device_id_type=MESH)

    own_k = pltpu.make_async_copy(key_weight, W.at[z, y, :, 0:128], loc.at[4])
    own_v = pltpu.make_async_copy(value_weight, W.at[z, y, :, 128:384], loc.at[5])
    own_k.start()
    own_v.start()
    loads = [
        pltpu.make_async_copy(tokens.at[n * GROUP : (n + 1) * GROUP], X.at[n * GROUP : (n + 1) * GROUP], loc.at[n])
        for n in range(4)
    ]
    loads[0].start()
    small = [
        pltpu.make_async_copy(src, dst, loc.at[8 + at])
        for at, (src, dst) in enumerate(
            (
                (gain_in, gain),
                (input_weight, GW.at[0:16]),
                (forget_weight, GW.at[16:32]),
                (offsets_in, offsets),
                (new_rows_in, new_rows),
                (new_query_in, new_query),
            )
        )
    ]
    for copy in small:
        copy.start()
    for load in loads[1:]:
        load.start()
    own_k.wait()
    own_v.wait()
    pl.semaphore_wait(barrier, 34)

    half_z = (z // 4) * 4
    other_z = 4 - half_z
    far_z = (z + 4) % 8

    def shard_to(row, to_z, recv):
        pltpu.make_async_remote_copy(
            src_ref=W.at[row, y],
            dst_ref=W.at[row, y],
            send_sem=ws1,
            recv_sem=recv,
            device_id={"sp": to_z * 4 + y},
            device_id_type=MESH,
        ).start()

    shard_to(z, far_z, wc)
    for o in range(1, 4):
        shard_to(z, half_z + (z + o) % 4, wh)

    def slot(i):
        return xor2(k_me, (2 * i + 1) % 5)

    def first_leg(i):
        dest = (t - s + 32) % 8 + 8 * slot(i)
        src = tokens.at[pl.ds(pl.multiple_of(dest * BLOCK, BLOCK), BLOCK)]
        dst = T.at[pl.ds(pl.multiple_of(s * BLOCK, BLOCK), BLOCK)]
        remote = pltpu.make_async_remote_copy(
            src_ref=src,
            dst_ref=dst,
            send_sem=p1s.at[i],
            recv_sem=p1r.at[i],
            device_id={"sp": dest},
            device_id_type=MESH,
        )
        return dest, src, dst, remote

    def start_leg(i):
        dest, src, dst, remote = first_leg(i)

        @pl.when(dest != s)
        def _():
            remote.start()

        @pl.when(dest == s)
        def _():
            pltpu.make_async_copy(src, dst, p1r.at[i]).start()

    start_leg(0)
    start_leg(1)

    for copy in small:
        copy.wait()
    for n in range(4):
        loads[n].wait()

        def gates(n=n):
            norm_group(X, n * GROUP, N, gain)
            G[n] = lax.dot_general(GW[...], N[...], NT, preferred_element_type=F32)

        gates()

    gate_row = iota((32, GROUP), 0)
    for n in range(4):
        for h in range(2):
            at = slice(2 * n + h, 2 * n + h + 1)
            mine = jnp.where(gate_row == 2 * t + h, G[n], 0.0)
            IG[at, :] = jnp.sum(mine, axis=0, keepdims=True) + offsets[n, 0, h : h + 1, :]
            mine = jnp.where(gate_row == 16 + 2 * t + h, G[n], 0.0)
            PRE[at, :] = jnp.sum(mine, axis=0, keepdims=True) + bias[h]
            LF[at, :] = offsets[n, 1, h : h + 1, :]

    lane = iota((8, GROUP), 1)
    pre = PRE[...]
    soft = jnp.minimum(pre, 0.0) - jnp.log1p(jnp.exp(-jnp.abs(pre)))
    log_forget = soft + LF[...]
    suffix = log_forget
    step = 1
    while step < GROUP:
        suffix = suffix + jnp.where(lane < GROUP - step, pltpu.roll(suffix, GROUP - step, 1), 0.0)
        step *= 2
    exclusive = jnp.where(lane < GROUP - 1, pltpu.roll(suffix, GROUP - 1, 1), 0.0)
    local = IG[...] + exclusive
    total = jnp.broadcast_to(suffix[:, 0:1], (8, 128))
    most = jnp.broadcast_to(jnp.max(local, axis=1, keepdims=True), (8, 128))
    lane = iota((8, 128), 1)
    tail_part = jnp.where(
        lane < 80,
        total,
        jnp.where(lane < 96, pltpu.roll(total, 7, 0), jnp.where(lane < 112, most, pltpu.roll(most, 7, 0))),
    )
    for half in range(2):
        part = local[:, half * 128 : (half + 1) * 128]
        for k in range(4):
            first = pltpu.roll(part, (128 - 32 * k) % 128, 1) if k else part
            second = pltpu.roll(pltpu.roll(part, 7, 0), (160 - 32 * k) % 128, 1) if k != 1 else pltpu.roll(part, 7, 0)
            row = jnp.where(lane < 32, first, jnp.where(lane < 64, second, tail_part))
            for n in range(4):
                S[n * 8 + half * 4 + k] = row[2 * n : 2 * n + 1, :]
    R[pl.ds(s, 1)] = S[pl.ds(s, 1)]

    def send_rows(o, carry):
        peer = (s + o) % 32
        pltpu.make_async_remote_copy(
            src_ref=S.at[peer],
            dst_ref=R.at[s],
            send_sem=lws,
            recv_sem=lwr,
            device_id={"sp": peer},
            device_id_type=MESH,
        ).start()
        return carry

    lax.fori_loop(1, 32, send_rows, 0)

    def y_send(rows, column, to_y, which):
        pltpu.make_async_remote_copy(
            src_ref=W.at[pl.ds(rows, 4), column],
            dst_ref=W.at[pl.ds(rows, 4), column],
            send_sem=ws2,
            recv_sem=wy.at[which],
            device_id={"sp": z * 4 + to_y},
            device_id_type=MESH,
        ).start()

    def arrived(ref, sem):
        pltpu.make_async_copy(ref, ref, sem).wait()

    up, down = (y + 1) % 4, (y + 3) % 4

    arrived(W.at[0, 0], wc)
    for o in range(1, 4):
        shard_to(far_z, half_z + (z + o) % 4, w2)
    arrived(W.at[0:3, 0], wh)
    y_send(half_z, y, up, 0)
    y_send(half_z, y, down, 1)

    def block_of(owner, i):
        at = ((owner - s + 32) % 8 + 8 * slot(i)) * BLOCK
        return T.at[pl.ds(pl.multiple_of(at, BLOCK), BLOCK)]

    def pass_on(owner, i, to, recv):
        block = block_of(owner, i)
        pltpu.make_async_remote_copy(
            src_ref=block,
            dst_ref=block,
            send_sem=xs,
            recv_sem=recv,
            device_id={"tp": to},
            device_id_type=MESH,
        ).start()

    half_block = BLOCK // 2

    def pass_half(owner, i, half, to):
        at = ((owner - s + 32) % 8 + 8 * slot(i)) * BLOCK + half * half_block
        part = T.at[pl.ds(pl.multiple_of(at, half_block), half_block)]
        pltpu.make_async_remote_copy(
            src_ref=part,
            dst_ref=part,
            send_sem=xs,
            recv_sem=xf.at[i, half],
            device_id={"tp": to},
            device_id_type=MESH,
        ).start()

    one_block = T.at[0:BLOCK]

    def stage_a(i):
        arrived(one_block, p1r.at[i])
        pass_on(t, i, right, xl.at[i])
        pass_on(t, i, left, xr.at[i])
        pass_on(t, i, mate, dr.at[i])

    def stage_b(i):
        arrived(one_block, xl.at[i])
        pass_half(left, i, 0, right)
        pass_on(left, i, mate, dr.at[i])
        arrived(one_block, xr.at[i])
        pass_half(right, i, 1, left)
        pass_on(right, i, mate, dr.at[i])

    def stage_c(i):
        arrived(T.at[0:half_block], xf.at[i, 0])
        arrived(T.at[0:half_block], xf.at[i, 1])
        pass_on(across, i, mate, dr.at[i])

    def write_out(i):
        at = pl.ds(pl.multiple_of(slot(i) * GROUP, GROUP), GROUP)
        return (
            pltpu.make_async_copy(OK.at[at], out_keys.at[at], loc.at[6]),
            pltpu.make_async_copy(OV.at[at], out_values.at[at], loc.at[7]),
        )

    def stage_d(i):
        arrived(T.at[0 : 4 * BLOCK], dr.at[i])
        start = pl.multiple_of(slot(i) * GROUP, GROUP)
        norm_group(T, start, N, gain)
        both = jnp.dot(N[...], W[...].reshape(D, 384), preferred_element_type=F32)
        keys = (both[:, 0:128] * 0.125).astype(BF16)
        values = both[:, 128:384].astype(BF16)
        OK[pl.ds(start, GROUP), :] = keys
        OV[pl.ds(start, GROUP), :] = values
        scores = lax.dot_general(Q8[...].astype(BF16), keys, NT, preferred_element_type=F32)
        weights = LW[:, pl.ds(start, GROUP)]
        rows = iota((8, GROUP), 0)
        weights = jnp.where(rows % 2 == 0, weights[0:1, :], weights[1:2, :])
        terms = jnp.exp(weights - PEAK[:, 0:1]) * scores
        terms = jnp.where(rows // 2 == n_me, terms, 0.0)
        DEN[...] += jnp.broadcast_to(jnp.sum(terms, axis=1, keepdims=True), (8, 128))
        NUM[...] += jnp.dot(terms.astype(BF16), values, preferred_element_type=F32)
        for copy in write_out(i):
            copy.start()

    def log_weights():
        arrived(R.at[0:31], lwr)
        received = R[:, 0, :]
        row = iota((32, 128), 0)
        suffix = received
        step = 1
        while step < 32:
            suffix = suffix + jnp.where(row < 32 - step, pltpu.roll(suffix, 32 - step, 0), 0.0)
            step *= 2
        exclusive = jnp.where(row < 31, pltpu.roll(suffix, 31, 0), 0.0)
        tail0, tail1 = exclusive[:, 64:65], exclusive[:, 80:81]
        lane32 = iota((32, 128), 1)
        peak0 = jnp.max(received[:, 96:97] + tail0, axis=0, keepdims=True)
        peak1 = jnp.max(received[:, 112:113] + tail1, axis=0, keepdims=True)
        L[...] = received + jnp.where(lane32 < 32, tail0, tail1)
        even = iota((8, 128), 0) % 2 == 0
        PEAK[...] = jnp.where(even, jnp.broadcast_to(peak0, (8, 128)), jnp.broadcast_to(peak1, (8, 128)))
        for h in range(2):
            wide = jnp.zeros((8, 128), F32)
            for k in range(4):
                rows = L[pl.ds(k, 8, stride=4), :]
                shift = (32 * k - 32 * h) % 128
                moved = pltpu.roll(rows, shift, 1) if shift else rows
                wide = jnp.where((lane >= 32 * k) & (lane < 32 * k + 32), moved, wide)
            for g in range(8):
                LW[h : h + 1, g * 128 : (g + 1) * 128] = wide[g : g + 1, :]
        out_weights[...] = LW[...]

        query = new_query[...].astype(F32)
        for n in range(4):
            Q8[2 * n : 2 * n + 1, :] = jnp.where(lane1 < 64, query[n : n + 1, :], 0.0)
            Q8[2 * n + 1 : 2 * n + 2, :] = jnp.where(lane1 < 64, 0.0, query[n : n + 1, :])

        NUM[...] = jnp.zeros_like(NUM)
        DEN[...] = jnp.zeros_like(DEN)

    query = new_query[...].astype(F32)
    lane1 = iota((1, 128), 1)
    lane = iota((8, 128), 1)

    def new_row_parts():
        total = jnp.zeros((4, 128), F32)
        for g in range(D // 128):
            v = new_rows[:, g * 128 : (g + 1) * 128].astype(F32)
            total = total + v * v
        inverse = lax.rsqrt(jnp.sum(total, axis=-1, keepdims=True) * (1.0 / D) + EPSILON)
        NN[...] = jnp.zeros_like(NN)
        for g in range(D // 128):
            at = slice(g * 128, (g + 1) * 128)
            NN[0:4, at] = new_rows[:, at].astype(F32) * inverse * gain[g : g + 1, :].astype(F32)
        fresh = NN[...].astype(BF16)
        KVN[...] = jnp.dot(fresh, W[...].reshape(D, 384), preferred_element_type=F32)
        GN[...] = lax.dot_general(fresh, GW[...], NT, preferred_element_type=F32)

    stage_a(0)
    start_leg(2)
    arrived(W.at[0:4, 0], wy.at[0])
    y_send(half_z, down, up, 2)
    arrived(W.at[0:3, 0], w2)
    y_send(other_z, y, up, 3)
    y_send(other_z, y, down, 4)
    stage_b(0)
    log_weights()
    stage_a(2)
    stage_a(1)
    start_leg(3)
    arrived(W.at[0:4, 0], wy.at[4])
    y_send(other_z, up, down, 5)
    stage_c(0)
    stage_b(2)
    stage_b(1)
    stage_c(2)
    stage_c(1)
    for which in (1, 2, 3, 5):
        arrived(W.at[0:4, 0], wy.at[which])
    new_row_parts()
    stage_d(0)
    stage_a(3)
    stage_d(2)
    stage_b(3)
    stage_d(1)
    stage_c(3)
    stage_d(3)

    evens = (iota((8, 128), 0) % 2 == 0).astype(F32)
    odds = 1.0 - evens
    FS[0:1, :] = jnp.sum(NUM[:, 0:128] * evens, axis=0, keepdims=True)
    FS[1:2, :] = jnp.sum(NUM[:, 128:256] * odds, axis=0, keepdims=True)
    den0 = jnp.sum(DEN[...] * evens, axis=0, keepdims=True)
    den1 = jnp.sum(DEN[...] * odds, axis=0, keepdims=True)
    FS[2:3, :] = jnp.where(lane1 < 64, den0, den1)
    FS[3:4, :] = jnp.where(lane1 < 64, PEAK[0:1, :], PEAK[1:2, :])
    FR[pl.ds(s, 1)] = FS[...].reshape(1, 4, 128)

    def send_read(o, carry):
        pltpu.make_async_remote_copy(
            src_ref=FS,
            dst_ref=FR.at[s],
            send_sem=fs,
            recv_sem=fr,
            device_id={"sp": (s + o) % 32},
            device_id_type=MESH,
        ).start()
        return carry

    lax.fori_loop(1, 32, send_read, 0)

    own_head = iota((8, 32), 1)
    gate0 = jnp.sum(jnp.where(own_head == 2 * t, GN[...], 0.0), axis=1, keepdims=True)[0:4]
    gate1 = jnp.sum(jnp.where(own_head == 2 * t + 1, GN[...], 0.0), axis=1, keepdims=True)[0:4]
    key_new = (KVN[0:4, 0:128] * 0.125).astype(BF16).astype(F32)
    value_new = KVN[0:4, 128:384].astype(BF16).astype(F32)
    product = query * key_new
    lane4 = iota((4, 128), 1)
    own0 = jnp.sum(jnp.where(lane4 < 64, product, 0.0), axis=1, keepdims=True)
    own1 = jnp.sum(jnp.where(lane4 < 64, 0.0, product), axis=1, keepdims=True)

    arrived(OK, loc.at[6])
    arrived(OV, loc.at[7])

    arrived(FR.at[0:31], fr)
    for n in range(4):
        group = FR[n * 8 : n * 8 + 8]
        added = jnp.sum(group, axis=0)
        A0[n : n + 1, :] = added[0:1, :]
        A0[4 + n : 5 + n, :] = added[1:2, :]
        A1[n : n + 1, :] = added[2:3, :]
        A1[4 + n : 5 + n, :] = group[0, 3:4, :]

    for h, (gate, own) in enumerate(((gate0, own0), (gate1, own1))):
        numerator = A0[4 * h : 4 * h + 4, :]
        denominator = A1[0:4, 64 * h : 64 * h + 1]
        peak = A1[4:8, 64 * h : 64 * h + 1]
        top = jnp.maximum(peak, gate)
        old_part = jnp.exp(peak - top)
        new_part = jnp.exp(gate - top) * own
        value = old_part * numerator + new_part * value_new[:, h * 128 : (h + 1) * 128]
        weight = old_part * denominator + new_part
        out_read[:, h * 128 : (h + 1) * 128] = (value / jnp.maximum(jnp.abs(weight), 1.0)).astype(BF16)

    arrived(R.at[0:31], lws)
    arrived(FR.at[0:31], fs)
    arrived(W.at[0:7, 0], ws1)
    arrived(W.at[0:6], ws2)
    arrived(T.at[0 : 28 * BLOCK], xs)

    def leg_done(i, carry):
        dest, _, _, remote = first_leg(i)

        @pl.when(dest != s)
        def _():
            remote.wait_send()

        return carry

    lax.fori_loop(0, 4, leg_done, 0)


def place(keys, values, weights, read, out_keys, out_values, out_weights, out_read, sems):
    copies = [
        pltpu.make_async_copy(keys, out_keys.at[0], sems.at[0]),
        pltpu.make_async_copy(values, out_values.at[0], sems.at[1]),
        pltpu.make_async_copy(weights, out_weights.at[0], sems.at[2]),
        pltpu.make_async_copy(read, out_read, sems.at[3]),
    ]
    for copy in copies:
        copy.start()
    for copy in copies:
        copy.wait()


def per_device(
    tokens,
    new_rows,
    new_query,
    norm_gain,
    key_weight,
    value_weight,
    input_weight,
    forget_weight,
    forget_bias,
    gate_offsets,
):
    any_space = pl.BlockSpec(memory_space=pl.ANY)
    vmem = pl.BlockSpec(memory_space=pltpu.VMEM)
    smem = pl.BlockSpec(memory_space=pltpu.SMEM)
    dma = pltpu.SemaphoreType.DMA
    keys, values, weights, read = pl.pallas_call(
        kernel,
        out_shape=(
            jax.ShapeDtypeStruct((ROWS, 128), BF16),
            jax.ShapeDtypeStruct((ROWS, 256), BF16),
            jax.ShapeDtypeStruct((2, ROWS), F32),
            jax.ShapeDtypeStruct((4, 256), BF16),
        ),
        in_specs=[any_space] * 8 + [smem, any_space],
        out_specs=(any_space, any_space, vmem, vmem),
        scratch_shapes=[
            pltpu.VMEM((4, D), BF16),
            pltpu.VMEM((4, 128), BF16),
            pltpu.VMEM((16, 128), BF16),
            pltpu.VMEM((4, 2, 2, GROUP), F32),
            pltpu.VMEM((ROWS, D), BF16),
            pltpu.VMEM((ROWS, D), BF16),
            pltpu.VMEM((GROUP, D), BF16),
            pltpu.VMEM((8, 4, 64, 384), BF16),
            pltpu.VMEM((ROWS, 128), BF16),
            pltpu.VMEM((ROWS, 256), BF16),
            pltpu.VMEM((4, 32, GROUP), F32),
            pltpu.VMEM((32, D), BF16),
            pltpu.VMEM((8, D), F32),
            pltpu.VMEM((8, GROUP), F32),
            pltpu.VMEM((8, GROUP), F32),
            pltpu.VMEM((8, GROUP), F32),
            pltpu.VMEM((32, 1, 128), F32),
            pltpu.VMEM((32, 1, 128), F32),
            pltpu.VMEM((32, 128), F32),
            pltpu.VMEM((2, ROWS), F32),
            pltpu.VMEM((8, 128), F32),
            pltpu.VMEM((8, 128), F32),
            pltpu.VMEM((8, 256), F32),
            pltpu.VMEM((8, 128), F32),
            pltpu.VMEM((8, 384), F32),
            pltpu.VMEM((8, 32), F32),
            pltpu.VMEM((4, 128), F32),
            pltpu.VMEM((32, 4, 128), F32),
            pltpu.VMEM((8, 128), F32),
            pltpu.VMEM((8, 128), F32),
            dma((4,)),
            dma((4,)),
            dma((4,)),
            dma((4,)),
            dma((4, 2)),
            dma((4,)),
            dma,
            dma,
            dma,
            dma,
            dma,
            dma,
            dma((6,)),
            dma,
            dma,
            dma,
            dma,
            dma((14,)),
        ],
        compiler_params=pltpu.CompilerParams(collective_id=0, has_side_effects=True),
    )(
        tokens.reshape(ROWS, D),
        new_rows,
        new_query,
        norm_gain.reshape(16, 128),
        key_weight,
        value_weight,
        input_weight.T,
        forget_weight.T,
        forget_bias,
        jnp.transpose(gate_offsets, (0, 2, 3, 1)),
    )
    return pl.pallas_call(
        place,
        out_shape=(
            jax.ShapeDtypeStruct((1, ROWS, 128), BF16),
            jax.ShapeDtypeStruct((1, ROWS, 256), BF16),
            jax.ShapeDtypeStruct((1, 2, ROWS), F32),
            jax.ShapeDtypeStruct((4, 256), BF16),
        ),
        in_specs=[vmem] * 4,
        out_specs=[any_space] * 4,
        scratch_shapes=[dma((4,))],
    )(keys, values, weights, read)


def solution(mesh):
    return jax.shard_map(
        per_device,
        mesh=mesh,
        in_specs=(
            P("gr", "sp", None),
            P("gr", None),
            P("gr", "tp"),
            P(),
            P("sp", "tp"),
            P("sp", "tp"),
            P(),
            P(),
            P("tp"),
            P("gr", "sp", None, "tp"),
        ),
        out_specs=(
            P(("gr", "sp"), None, "tp"),
            P(("gr", "sp"), None, "tp"),
            P(("gr", "sp"), "tp", None),
            P("gr", "tp"),
        ),
        check_vma=False,
    )
```

```python
import jax
import jax.numpy as jnp
from jax import lax
from jax.experimental import pallas as pl
from jax.experimental.pallas import tpu as pltpu
from jax.sharding import PartitionSpec as P

EPSILON = 1e-06
MESH = pl.DeviceIdType.MESH
F32 = jnp.float32
BF16 = jnp.bfloat16
NT = (((1,), (1,)), ((), ()))

D = 2048
ROWS = 1024
GROUP = 256
BLOCK = 32
CHUNK = 64


def iota(shape, dim):
    return lax.broadcasted_iota(jnp.int32, shape, dim)


def xor2(a, b):
    return 2 * ((a // 2 + b // 2) % 2) + (a % 2 + b % 2) % 2


def norm_chunk(read, write, gain_ref, rows):
    total = jnp.zeros((rows, 128), F32)
    for c in range(D // 128):
        v = read(c).astype(F32)
        total = total + v * v
    inverse = lax.rsqrt(jnp.sum(total, axis=-1, keepdims=True) * (1.0 / D) + EPSILON)
    for c in range(D // 128):
        v = read(c).astype(F32)
        write(c, (v * inverse * gain_ref[c : c + 1, :].astype(F32)).astype(BF16))


def norm_group(src, start, dst, first, gain_ref):
    def body(u, carry):
        at = pl.multiple_of(start + u * CHUNK, CHUNK)
        to = pl.multiple_of(first + u * CHUNK, CHUNK)

        def read(c):
            return src[pl.ds(at, CHUNK), c * 128 : (c + 1) * 128]

        def write(c, v):
            dst[pl.ds(to, CHUNK), c * 128 : (c + 1) * 128] = v

        norm_chunk(read, write, gain_ref, CHUNK)
        return carry

    lax.fori_loop(0, GROUP // CHUNK, body, 0)


def kernel(
    tokens,
    new_rows_in,
    new_query_in,
    gain_in,
    key_weight,
    value_weight,
    input_weight,
    forget_weight,
    bias,
    offsets_in,
    out_keys,
    out_values,
    out_weights,
    out_read,
    new_rows,
    new_query,
    gain,
    offsets,
    T,
    X,
    N,
    W,
    OK,
    OV,
    G,
    GW,
    NN,
    IG,
    PRE,
    LF,
    LOC,
    S,
    R,
    L,
    LW,
    PEAK,
    Q8,
    NUM,
    DEN,
    KN8,
    VN8,
    GN8,
    E1,
    E2,
    A0,
    p1s,
    p1r,
    xl,
    xr,
    xf,
    dr,
    xs,
    lws,
    lwr,
    wc,
    wh,
    w2,
    wy,
    ws1,
    ws2,
    es,
    er,
    loc,
):
    s = lax.axis_index("sp")
    t = lax.axis_index("tp")
    z, y = s // 4, s % 4
    x, c = t // 2, t % 2
    k_me = s // 8
    n_me = s // 8
    right = ((x + 1) % 4) * 2 + c
    left = ((x + 3) % 4) * 2 + c
    across = ((x + 2) % 4) * 2 + c
    mate = t + 1 - 2 * c

    barrier = pltpu.get_barrier_semaphore()

    def greet(o, carry):
        pl.semaphore_signal(barrier, inc=1, device_id={"sp": (s + o) % 32}, device_id_type=MESH)
        return carry

    lax.fori_loop(1, 32, greet, 0)
    for who in (right, left, mate):
        pl.semaphore_signal(barrier, inc=1, device_id={"tp": who}, device_id_type=MESH)

    own_k = pltpu.make_async_copy(key_weight, W.at[z, y, :, 0:128], loc.at[4])
    own_v = pltpu.make_async_copy(value_weight, W.at[z, y, :, 128:384], loc.at[5])
    own_k.start()
    own_v.start()
    loads = [
        pltpu.make_async_copy(tokens.at[n * GROUP : (n + 1) * GROUP], X.at[n * GROUP : (n + 1) * GROUP], loc.at[n])
        for n in range(4)
    ]
    loads[0].start()
    small = [
        pltpu.make_async_copy(src, dst, loc.at[8 + at])
        for at, (src, dst) in enumerate(
            (
                (gain_in, gain),
                (input_weight, GW.at[0:16]),
                (forget_weight, GW.at[16:32]),
                (offsets_in, offsets),
                (new_rows_in, new_rows),
                (new_query_in, new_query),
            )
        )
    ]
    for copy in small:
        copy.start()
    for load in loads[1:]:
        load.start()
    own_k.wait()
    own_v.wait()
    pl.semaphore_wait(barrier, 34)

    half_z = (z // 4) * 4
    other_z = 4 - half_z
    far_z = (z + 4) % 8

    def shard_to(row, to_z, recv):
        pltpu.make_async_remote_copy(
            src_ref=W.at[row, y],
            dst_ref=W.at[row, y],
            send_sem=ws1,
            recv_sem=recv,
            device_id={"sp": to_z * 4 + y},
            device_id_type=MESH,
        ).start()

    inner = (k_me // 2 + k_me % 2) % 2

    def sent_at(j):
        return inner * (0, 1, 2, 3)[j] + (1 - inner) * (0, 3, 2, 1)[j]

    def due_at(j):
        return inner * (0, 2, 1, 3)[j] + (1 - inner) * (0, 1, 3, 2)[j]

    def slot(i):
        return xor2(k_me, i)

    def first_leg(i):
        dest = (t - s + i + 32) % 8 + 8 * slot(i)
        src = tokens.at[pl.ds(pl.multiple_of(dest * BLOCK, BLOCK), BLOCK)]
        dst = T.at[pl.ds(pl.multiple_of(s * BLOCK, BLOCK), BLOCK)]
        remote = pltpu.make_async_remote_copy(
            src_ref=src,
            dst_ref=dst,
            send_sem=p1s.at[i],
            recv_sem=p1r.at[i],
            device_id={"sp": dest},
            device_id_type=MESH,
        )
        return dest, src, dst, remote

    def start_leg(j):
        i = sent_at(j)
        dest, src, dst, remote = first_leg(i)

        @pl.when(dest != s)
        def _():
            remote.start()

        @pl.when(dest == s)
        def _():
            pltpu.make_async_copy(src, dst, p1r.at[i]).start()

    shard_to(z, far_z, wc)
    for o in range(1, 4):
        shard_to(z, half_z + (z + o) % 4, wh)

    start_leg(0)

    def y_send(rows, column, to_y, which):
        pltpu.make_async_remote_copy(
            src_ref=W.at[pl.ds(rows, 4), column],
            dst_ref=W.at[pl.ds(rows, 4), column],
            send_sem=ws2,
            recv_sem=wy.at[which],
            device_id={"sp": z * 4 + to_y},
            device_id_type=MESH,
        ).start()

    def arrived(ref, sem):
        pltpu.make_async_copy(ref, ref, sem).wait()

    up, down = (y + 1) % 4, (y + 3) % 4

    def gates(n):
        loads[n].wait()
        norm_group(X, n * GROUP, X, n * GROUP, gain)
        own = X[n * GROUP : (n + 1) * GROUP, :]
        G[n] = lax.dot_general(GW[...], own, NT, preferred_element_type=F32)

    lane = iota((8, 128), 1)
    head_row = iota((8, 128), 0)

    def local_weights():
        gate_row = iota((32, GROUP), 0)
        for n in range(4):
            for h in range(2):
                at = slice(2 * n + h, 2 * n + h + 1)
                mine = jnp.where(gate_row == 2 * t + h, G[n], 0.0)
                IG[at, :] = jnp.sum(mine, axis=0, keepdims=True) + offsets[n, 0, h : h + 1, :]
                mine = jnp.where(gate_row == 16 + 2 * t + h, G[n], 0.0)
                PRE[at, :] = jnp.sum(mine, axis=0, keepdims=True) + bias[h]
                LF[at, :] = offsets[n, 1, h : h + 1, :]

        wide_lane = iota((8, GROUP), 1)
        pre = PRE[...]
        soft = jnp.minimum(pre, 0.0) - jnp.log1p(jnp.exp(-jnp.abs(pre)))
        log_forget = soft + LF[...]
        suffix = log_forget
        step = 1
        while step < GROUP:
            suffix = suffix + jnp.where(wide_lane < GROUP - step, pltpu.roll(suffix, GROUP - step, 1), 0.0)
            step *= 2
        exclusive = jnp.where(wide_lane < GROUP - 1, pltpu.roll(suffix, GROUP - 1, 1), 0.0)
        local = IG[...] + exclusive
        LOC[...] = local
        total = suffix[:, 0:1]
        most = jnp.max(local, axis=1, keepdims=True)
        tail_part = jnp.where(lane - 64 == head_row, total, jnp.where(lane - 72 == head_row, most, 0.0))
        tail_part = jnp.broadcast_to(jnp.sum(tail_part, axis=0, keepdims=True), (8, 128))
        for half in range(2):
            part = local[:, half * 128 : (half + 1) * 128]
            for k in range(4):
                first = pltpu.roll(part, (128 - 32 * k) % 128, 1) if k else part
                second = pltpu.roll(pltpu.roll(part, 7, 0), (160 - 32 * k) % 128, 1) if k != 1 else pltpu.roll(part, 7, 0)
                row = jnp.where(lane < 32, first, jnp.where(lane < 64, second, tail_part))
                for n in range(4):
                    S[n * 8 + half * 4 + k] = row[2 * n : 2 * n + 1, :]
        R[pl.ds(s, 1)] = S[pl.ds(s, 1)]

        def send_rows(o, carry):
            peer = (s + o) % 32
            pltpu.make_async_remote_copy(
                src_ref=S.at[peer],
                dst_ref=R.at[s],
                send_sem=lws,
                recv_sem=lwr,
                device_id={"sp": peer},
                device_id_type=MESH,
            ).start()
            return carry

        lax.fori_loop(1, 32, send_rows, 0)

    def block_of(owner, i):
        at = ((owner - s + i + 32) % 8 + 8 * slot(i)) * BLOCK
        return T.at[pl.ds(pl.multiple_of(at, BLOCK), BLOCK)]

    def pass_on(owner, i, to, recv):
        block = block_of(owner, i)
        pltpu.make_async_remote_copy(
            src_ref=block,
            dst_ref=block,
            send_sem=xs,
            recv_sem=recv,
            device_id={"tp": to},
            device_id_type=MESH,
        ).start()

    half_block = BLOCK // 2

    def pass_half(owner, i, half, to):
        at = ((owner - s + i + 32) % 8 + 8 * slot(i)) * BLOCK + half * half_block
        part = T.at[pl.ds(pl.multiple_of(at, half_block), half_block)]
        pltpu.make_async_remote_copy(
            src_ref=part,
            dst_ref=part,
            send_sem=xs,
            recv_sem=xf.at[i, half],
            device_id={"tp": to},
            device_id_type=MESH,
        ).start()

    one_block = T.at[0:BLOCK]

    def stage_a(j):
        i = due_at(j)
        arrived(one_block, p1r.at[i])
        pass_on(t, i, right, xl.at[i])
        pass_on(t, i, left, xr.at[i])
        pass_on(t, i, mate, dr.at[i])

    def stage_b(j):
        i = due_at(j)
        arrived(one_block, xl.at[i])
        pass_half(left, i, 0, right)
        pass_on(left, i, mate, dr.at[i])
        arrived(one_block, xr.at[i])
        pass_half(right, i, 1, left)
        pass_on(right, i, mate, dr.at[i])

    def stage_c(j):
        i = due_at(j)
        arrived(T.at[0:half_block], xf.at[i, 0])
        arrived(T.at[0:half_block], xf.at[i, 1])
        pass_on(across, i, mate, dr.at[i])

    def write_out(i):
        at = pl.ds(pl.multiple_of(slot(i) * GROUP, GROUP), GROUP)
        return (
            pltpu.make_async_copy(OK.at[at], out_keys.at[at], loc.at[6]),
            pltpu.make_async_copy(OV.at[at], out_values.at[at], loc.at[7]),
        )

    def stage_n(j):
        i = due_at(j)
        arrived(T.at[0 : 4 * BLOCK], dr.at[i])
        start = pl.multiple_of(slot(i) * GROUP, GROUP)
        norm_group(T, start, N, j * GROUP, gain)

    def stage_d(j):
        i = due_at(j)
        start = pl.multiple_of(slot(i) * GROUP, GROUP)
        keys, values = project(N[j * GROUP : (j + 1) * GROUP, :])
        OK[pl.ds(start, GROUP), :] = keys
        OV[pl.ds(start, GROUP), :] = values
        for copy in write_out(i):
            copy.start()

    def column(row, first):
        return jnp.sum(jnp.where(lane - first == head_row, row, 0.0), axis=1, keepdims=True)

    def log_weights():
        arrived(R.at[0:31], lwr)
        received = R[:, 0, :]
        row = iota((32, 128), 0)
        lane32 = iota((32, 128), 1)
        suffix = received
        step = 1
        while step < 32:
            suffix = suffix + jnp.where(row < 32 - step, pltpu.roll(suffix, 32 - step, 0), 0.0)
            step *= 2
        exclusive = jnp.where(row < 31, pltpu.roll(suffix, 31, 0), 0.0)
        peaks = jnp.max(received + pltpu.roll(exclusive, 8, 1), axis=0, keepdims=True)
        PEAK[...] = jnp.broadcast_to(column(peaks, 72), (8, 128))
        mine = jnp.sum(jnp.where(row == s, exclusive, 0.0), axis=0, keepdims=True)
        LOC[...] += column(mine, 64)
        tails = [
            jnp.sum(jnp.where(lane32 == 64 + 2 * n_me + h, exclusive, 0.0), axis=1, keepdims=True)
            for h in range(2)
        ]
        L[...] = received + jnp.where(lane32 < 32, tails[0], tails[1])
        for h in range(2):
            wide = jnp.zeros((8, 128), F32)
            for k in range(4):
                rows = L[pl.ds(k, 8, stride=4), :]
                shift = (32 * k - 32 * h) % 128
                moved = pltpu.roll(rows, shift, 1) if shift else rows
                wide = jnp.where((lane >= 32 * k) & (lane < 32 * k + 32), moved, wide)
            for g in range(8):
                LW[h : h + 1, g * 128 : (g + 1) * 128] = wide[g : g + 1, :]
        out_weights[...] = LW[...]

        query = new_query[...].astype(F32)
        for n in range(4):
            Q8[2 * n : 2 * n + 1, :] = jnp.where(lane1 < 64, query[n : n + 1, :], 0.0)
            Q8[2 * n + 1 : 2 * n + 2, :] = jnp.where(lane1 < 64, 0.0, query[n : n + 1, :])
        NUM[...] = jnp.zeros_like(NUM)
        DEN[...] = jnp.zeros_like(DEN)

    def project(rows):
        both = jnp.dot(rows, W[...].reshape(D, 384), preferred_element_type=F32)
        return (both[:, 0:128] * 0.125).astype(BF16), both[:, 128:384].astype(BF16)

    def own_read(n):
        keys, values = project(X[n * GROUP : (n + 1) * GROUP, :])
        scores = lax.dot_general(Q8[...].astype(BF16), keys, NT, preferred_element_type=F32)
        terms = jnp.exp(LOC[...] - PEAK[:, 0:1]) * scores
        terms = jnp.where(iota((8, GROUP), 0) // 2 == n, terms, 0.0)
        DEN[...] += jnp.broadcast_to(jnp.sum(terms, axis=1, keepdims=True), (8, 128))
        NUM[...] += jnp.dot(terms.astype(BF16), values, preferred_element_type=F32)

    def share(buffer, slot_of, peers, send, recv):
        for to in peers:
            pltpu.make_async_remote_copy(
                src_ref=buffer.at[slot_of],
                dst_ref=buffer.at[slot_of],
                send_sem=send,
                recv_sem=recv,
                device_id={"sp": to},
                device_id_type=MESH,
            ).start()

    def sum_y():
        value = jnp.where(head_row % 2 == 0, NUM[:, 0:128], NUM[:, 128:256])
        E1[pl.ds(y, 1)] = jnp.concatenate([value, DEN[...]], axis=0).reshape(1, 16, 128)
        share(E1, y, [z * 4 + (y + o) % 4 for o in range(1, 4)], es.at[0], er.at[0])

    def sum_z():
        arrived(E1.at[0:3], er.at[0])
        E2[pl.ds(z, 1)] = ((E1[0] + E1[1]) + (E1[2] + E1[3])).reshape(1, 16, 128)
        share(E2, z, [((z + o) % 8) * 4 + y for o in range(1, 8)], es.at[1], er.at[1])

    def finish():
        arrived(E2.at[0:7], er.at[1])
        total = jnp.sum(E2[...], axis=0)
        numerator, denominator = total[0:8], total[8:16, 0:1]
        peak = PEAK[:, 0:1]
        gate = jnp.sum(
            jnp.where(iota((8, 32), 1) == 2 * t + iota((8, 32), 0) % 2, GN8[...], 0.0), axis=1, keepdims=True
        )
        own = jnp.sum(Q8[...] * (KN8[...] * 0.125).astype(BF16).astype(F32), axis=1, keepdims=True)
        top = jnp.maximum(peak, gate)
        old_part = jnp.exp(peak - top)
        new_part = jnp.exp(gate - top) * own
        value = old_part * numerator + new_part * VN8[...].astype(BF16).astype(F32)
        weight = old_part * denominator + new_part
        read = value / jnp.maximum(jnp.abs(weight), 1.0)
        for n in range(4):
            for h in range(2):
                A0[n : n + 1, h * 128 : (h + 1) * 128] = read[2 * n + h : 2 * n + h + 1, :]
        out_read[...] = A0[...].astype(BF16)

    lane1 = iota((1, 128), 1)

    def new_row_parts():
        total = jnp.zeros((4, 128), F32)
        for g in range(D // 128):
            v = new_rows[:, g * 128 : (g + 1) * 128].astype(F32)
            total = total + v * v
        inverse = lax.rsqrt(jnp.sum(total, axis=-1, keepdims=True) * (1.0 / D) + EPSILON)
        NN[...] = jnp.zeros_like(NN)
        for g in range(D // 128):
            at = slice(g * 128, (g + 1) * 128)
            NN[0:4, at] = new_rows[:, at].astype(F32) * inverse * gain[g : g + 1, :].astype(F32)
        fresh = NN[...].astype(BF16)
        both = jnp.dot(fresh, W[...].reshape(D, 384), preferred_element_type=F32)
        gates_new = lax.dot_general(fresh, GW[...], NT, preferred_element_type=F32)
        for n in range(4):
            for h in range(2):
                at = slice(2 * n + h, 2 * n + h + 1)
                KN8[at, :] = both[n : n + 1, 0:128]
                VN8[at, :] = both[n : n + 1, 128 * (h + 1) : 128 * (h + 2)]
                GN8[at, :] = gates_new[n : n + 1, :]

    for copy in small:
        copy.wait()
    for n in range(4):
        gates(n)
    local_weights()
    arrived(W.at[0, 0], wc)
    for o in range(1, 4):
        shard_to(far_z, half_z + (z + o) % 4, w2)
    arrived(W.at[0:3, 0], wh)
    y_send(half_z, y, up, 0)
    y_send(half_z, y, down, 1)
    start_leg(1)

    @pl.when(inner == 0)
    def _():
        start_leg(2)

    stage_a(0)
    stage_b(0)

    @pl.when(inner == 1)
    def _():
        start_leg(2)

    start_leg(3)
    arrived(W.at[0:4, 0], wy.at[0])
    y_send(half_z, down, up, 2)
    arrived(W.at[0:3, 0], w2)
    y_send(other_z, y, up, 3)
    y_send(other_z, y, down, 4)
    stage_a(1)
    stage_c(0)
    arrived(W.at[0:4, 0], wy.at[4])
    y_send(other_z, up, down, 5)
    stage_a(2)
    stage_b(1)
    stage_n(0)
    log_weights()
    stage_b(2)
    stage_a(3)
    stage_c(1)
    for which in (1, 2, 3, 5):
        arrived(W.at[0:4, 0], wy.at[which])
    own_read(0)
    stage_c(2)
    own_read(1)
    stage_b(3)
    own_read(2)
    own_read(3)
    sum_y()
    stage_c(3)
    stage_n(1)
    stage_d(0)
    stage_d(1)
    sum_z()
    new_row_parts()
    stage_n(2)
    stage_d(2)
    stage_n(3)
    stage_d(3)
    finish()
    arrived(OK, loc.at[6])
    arrived(OV, loc.at[7])

    arrived(R.at[0:31], lws)
    arrived(E1.at[0:3], es.at[0])
    arrived(E2.at[0:7], es.at[1])
    arrived(W.at[0:7, 0], ws1)
    arrived(W.at[0:6], ws2)
    arrived(T.at[0 : 28 * BLOCK], xs)

    def leg_done(i):
        dest, _, _, remote = first_leg(i)

        @pl.when(dest != s)
        def _():
            remote.wait_send()

    for i in range(4):
        leg_done(i)


def place(keys, values, weights, read, out_keys, out_values, out_weights, out_read, sems):
    copies = [
        pltpu.make_async_copy(keys, out_keys.at[0], sems.at[0]),
        pltpu.make_async_copy(values, out_values.at[0], sems.at[1]),
        pltpu.make_async_copy(weights, out_weights.at[0], sems.at[2]),
        pltpu.make_async_copy(read, out_read, sems.at[3]),
    ]
    for copy in copies:
        copy.start()
    for copy in copies:
        copy.wait()


def per_device(
    tokens,
    new_rows,
    new_query,
    norm_gain,
    key_weight,
    value_weight,
    input_weight,
    forget_weight,
    forget_bias,
    gate_offsets,
):
    any_space = pl.BlockSpec(memory_space=pl.ANY)
    vmem = pl.BlockSpec(memory_space=pltpu.VMEM)
    smem = pl.BlockSpec(memory_space=pltpu.SMEM)
    dma = pltpu.SemaphoreType.DMA
    keys, values, weights, read = pl.pallas_call(
        kernel,
        out_shape=(
            jax.ShapeDtypeStruct((ROWS, 128), BF16),
            jax.ShapeDtypeStruct((ROWS, 256), BF16),
            jax.ShapeDtypeStruct((2, ROWS), F32),
            jax.ShapeDtypeStruct((4, 256), BF16),
        ),
        in_specs=[any_space] * 8 + [smem, any_space],
        out_specs=(any_space, any_space, vmem, vmem),
        scratch_shapes=[
            pltpu.VMEM((4, D), BF16),
            pltpu.VMEM((4, 128), BF16),
            pltpu.VMEM((16, 128), BF16),
            pltpu.VMEM((4, 2, 2, GROUP), F32),
            pltpu.VMEM((ROWS, D), BF16),
            pltpu.VMEM((ROWS, D), BF16),
            pltpu.VMEM((ROWS, D), BF16),
            pltpu.VMEM((8, 4, 64, 384), BF16),
            pltpu.VMEM((ROWS, 128), BF16),
            pltpu.VMEM((ROWS, 256), BF16),
            pltpu.VMEM((4, 32, GROUP), F32),
            pltpu.VMEM((32, D), BF16),
            pltpu.VMEM((8, D), F32),
            pltpu.VMEM((8, GROUP), F32),
            pltpu.VMEM((8, GROUP), F32),
            pltpu.VMEM((8, GROUP), F32),
            pltpu.VMEM((8, GROUP), F32),
            pltpu.VMEM((32, 1, 128), F32),
            pltpu.VMEM((32, 1, 128), F32),
            pltpu.VMEM((32, 128), F32),
            pltpu.VMEM((2, ROWS), F32),
            pltpu.VMEM((8, 128), F32),
            pltpu.VMEM((8, 128), F32),
            pltpu.VMEM((8, 256), F32),
            pltpu.VMEM((8, 128), F32),
            pltpu.VMEM((8, 128), F32),
            pltpu.VMEM((8, 128), F32),
            pltpu.VMEM((8, 32), F32),
            pltpu.VMEM((4, 16, 128), F32),
            pltpu.VMEM((8, 16, 128), F32),
            pltpu.VMEM((4, 256), F32),
            dma((4,)),
            dma((4,)),
            dma((4,)),
            dma((4,)),
            dma((4, 2)),
            dma((4,)),
            dma,
            dma,
            dma,
            dma,
            dma,
            dma,
            dma((6,)),
            dma,
            dma,
            dma((2,)),
            dma((2,)),
            dma((14,)),
        ],
        compiler_params=pltpu.CompilerParams(collective_id=0, has_side_effects=True),
    )(
        tokens.reshape(ROWS, D),
        new_rows,
        new_query,
        norm_gain.reshape(16, 128),
        key_weight,
        value_weight,
        input_weight.T,
        forget_weight.T,
        forget_bias,
        jnp.transpose(gate_offsets, (0, 2, 3, 1)),
    )
    return pl.pallas_call(
        place,
        out_shape=(
            jax.ShapeDtypeStruct((1, ROWS, 128), BF16),
            jax.ShapeDtypeStruct((1, ROWS, 256), BF16),
            jax.ShapeDtypeStruct((1, 2, ROWS), F32),
            jax.ShapeDtypeStruct((4, 256), BF16),
        ),
        in_specs=[vmem] * 4,
        out_specs=[any_space] * 4,
        scratch_shapes=[dma((4,))],
    )(keys, values, weights, read)


def solution(mesh):
    return jax.shard_map(
        per_device,
        mesh=mesh,
        in_specs=(
            P("gr", "sp", None),
            P("gr", None),
            P("gr", "tp"),
            P(),
            P("sp", "tp"),
            P("sp", "tp"),
            P(),
            P(),
            P("tp"),
            P("gr", "sp", None, "tp"),
        ),
        out_specs=(
            P(("gr", "sp"), None, "tp"),
            P(("gr", "sp"), None, "tp"),
            P(("gr", "sp"), "tp", None),
            P("gr", "tp"),
        ),
        check_vma=False,
    )
```

```python
import jax
import jax.numpy as jnp
from jax import lax
from jax.experimental import pallas as pl
from jax.experimental.pallas import tpu as pltpu
from jax.sharding import PartitionSpec as P

EPSILON = 1e-06
MESH = pl.DeviceIdType.MESH
F32 = jnp.float32
BF16 = jnp.bfloat16
NT = (((1,), (1,)), ((), ()))

D = 2048
ROWS = 1024
GROUP = 256
BLOCK = 32
CHUNK = 64


def iota(shape, dim):
    return lax.broadcasted_iota(jnp.int32, shape, dim)


def xor2(a, b):
    return 2 * ((a // 2 + b // 2) % 2) + (a % 2 + b % 2) % 2


def norm_chunk(read, write, gain_ref, rows):
    total = jnp.zeros((rows, 128), F32)
    for c in range(D // 128):
        v = read(c).astype(F32)
        total = total + v * v
    inverse = lax.rsqrt(jnp.sum(total, axis=-1, keepdims=True) * (1.0 / D) + EPSILON)
    for c in range(D // 128):
        v = read(c).astype(F32)
        write(c, (v * inverse * gain_ref[c : c + 1, :].astype(F32)).astype(BF16))


def norm_group(src, start, dst, first, gain_ref):
    def body(u, carry):
        at = pl.multiple_of(start + u * CHUNK, CHUNK)
        to = pl.multiple_of(first + u * CHUNK, CHUNK)

        def read(c):
            return src[pl.ds(at, CHUNK), c * 128 : (c + 1) * 128]

        def write(c, v):
            dst[pl.ds(to, CHUNK), c * 128 : (c + 1) * 128] = v

        norm_chunk(read, write, gain_ref, CHUNK)
        return carry

    lax.fori_loop(0, GROUP // CHUNK, body, 0)


def kernel(
    tokens,
    new_rows_in,
    new_query_in,
    gain_in,
    key_weight,
    value_weight,
    input_weight,
    forget_weight,
    bias,
    offsets_in,
    out_keys,
    out_values,
    out_weights,
    out_read,
    new_rows,
    new_query,
    gain,
    offsets,
    T,
    X,
    N,
    W,
    OK,
    OV,
    G,
    GW,
    NN,
    IG,
    PRE,
    LF,
    LOC,
    S,
    R,
    L,
    LW,
    PEAK,
    Q8,
    NUM,
    DEN,
    KN8,
    VN8,
    GN8,
    E1,
    E2,
    A0,
    p1s,
    p1r,
    xl,
    xr,
    xf,
    dr,
    xs,
    lws,
    lwr,
    wc,
    wh,
    w2,
    wy,
    ws1,
    ws2,
    es,
    er,
    loc,
):
    s = lax.axis_index("sp")
    t = lax.axis_index("tp")
    z, y = s // 4, s % 4
    x, c = t // 2, t % 2
    k_me = s // 8
    n_me = s // 8
    right = ((x + 1) % 4) * 2 + c
    left = ((x + 3) % 4) * 2 + c
    across = ((x + 2) % 4) * 2 + c
    mate = t + 1 - 2 * c

    barrier = pltpu.get_barrier_semaphore()

    def greet(o, carry):
        pl.semaphore_signal(barrier, inc=1, device_id={"sp": (s + o) % 32}, device_id_type=MESH)
        return carry

    lax.fori_loop(1, 32, greet, 0)
    for who in (right, left, mate):
        pl.semaphore_signal(barrier, inc=1, device_id={"tp": who}, device_id_type=MESH)

    own_k = pltpu.make_async_copy(key_weight, W.at[z, y, :, 0:128], loc.at[4])
    own_v = pltpu.make_async_copy(value_weight, W.at[z, y, :, 128:384], loc.at[5])
    own_k.start()
    own_v.start()
    loads = [
        pltpu.make_async_copy(tokens.at[n * GROUP : (n + 1) * GROUP], X.at[n * GROUP : (n + 1) * GROUP], loc.at[n])
        for n in range(4)
    ]
    loads[0].start()
    small = [
        pltpu.make_async_copy(src, dst, loc.at[8 + at])
        for at, (src, dst) in enumerate(
            (
                (gain_in, gain),
                (input_weight, GW.at[0:16]),
                (forget_weight, GW.at[16:32]),
                (offsets_in, offsets),
                (new_rows_in, new_rows),
                (new_query_in, new_query),
            )
        )
    ]
    for copy in small:
        copy.start()
    for load in loads[1:]:
        load.start()
    own_k.wait()
    own_v.wait()
    pl.semaphore_wait(barrier, 34)

    half_z = (z // 4) * 4
    other_z = 4 - half_z
    far_z = (z + 4) % 8

    def shard_to(row, to_z, recv):
        pltpu.make_async_remote_copy(
            src_ref=W.at[row, y],
            dst_ref=W.at[row, y],
            send_sem=ws1,
            recv_sem=recv,
            device_id={"sp": to_z * 4 + y},
            device_id_type=MESH,
        ).start()

    inner = (k_me // 2 + k_me % 2) % 2

    def sent_at(j):
        return inner * (0, 1, 2, 3)[j] + (1 - inner) * (0, 3, 2, 1)[j]

    def due_at(j):
        return inner * (0, 2, 1, 3)[j] + (1 - inner) * (0, 1, 3, 2)[j]

    def slot(i):
        return xor2(k_me, i)

    def first_leg(i):
        dest = (t - s + i + 32) % 8 + 8 * slot(i)
        src = tokens.at[pl.ds(pl.multiple_of(dest * BLOCK, BLOCK), BLOCK)]
        dst = T.at[pl.ds(pl.multiple_of(s * BLOCK, BLOCK), BLOCK)]
        remote = pltpu.make_async_remote_copy(
            src_ref=src,
            dst_ref=dst,
            send_sem=p1s.at[i],
            recv_sem=p1r.at[i],
            device_id={"sp": dest},
            device_id_type=MESH,
        )
        return dest, src, dst, remote

    def start_leg(j):
        i = sent_at(j)
        dest, src, dst, remote = first_leg(i)

        @pl.when(dest != s)
        def _():
            remote.start()

        @pl.when(dest == s)
        def _():
            pltpu.make_async_copy(src, dst, p1r.at[i]).start()

    start_leg(0)
    shard_to(z, far_z, wc)
    for o in range(1, 4):
        shard_to(z, half_z + (z + o) % 4, wh)


    def y_send(rows, column, to_y, which):
        pltpu.make_async_remote_copy(
            src_ref=W.at[pl.ds(rows, 4), column],
            dst_ref=W.at[pl.ds(rows, 4), column],
            send_sem=ws2,
            recv_sem=wy.at[which],
            device_id={"sp": z * 4 + to_y},
            device_id_type=MESH,
        ).start()

    def arrived(ref, sem):
        pltpu.make_async_copy(ref, ref, sem).wait()

    up, down = (y + 1) % 4, (y + 3) % 4

    def gates(n):
        loads[n].wait()
        norm_group(X, n * GROUP, X, n * GROUP, gain)
        own = X[n * GROUP : (n + 1) * GROUP, :]
        G[n] = lax.dot_general(GW[...], own, NT, preferred_element_type=F32)

    lane = iota((8, 128), 1)
    head_row = iota((8, 128), 0)

    def local_weights():
        gate_row = iota((32, GROUP), 0)
        for n in range(4):
            for h in range(2):
                at = slice(2 * n + h, 2 * n + h + 1)
                mine = jnp.where(gate_row == 2 * t + h, G[n], 0.0)
                IG[at, :] = jnp.sum(mine, axis=0, keepdims=True) + offsets[n, 0, h : h + 1, :]
                mine = jnp.where(gate_row == 16 + 2 * t + h, G[n], 0.0)
                PRE[at, :] = jnp.sum(mine, axis=0, keepdims=True) + bias[h]
                LF[at, :] = offsets[n, 1, h : h + 1, :]

        wide_lane = iota((8, GROUP), 1)
        pre = PRE[...]
        soft = jnp.minimum(pre, 0.0) - jnp.log1p(jnp.exp(-jnp.abs(pre)))
        log_forget = soft + LF[...]
        suffix = log_forget
        step = 1
        while step < GROUP:
            suffix = suffix + jnp.where(wide_lane < GROUP - step, pltpu.roll(suffix, GROUP - step, 1), 0.0)
            step *= 2
        exclusive = jnp.where(wide_lane < GROUP - 1, pltpu.roll(suffix, GROUP - 1, 1), 0.0)
        local = IG[...] + exclusive
        LOC[...] = local
        total = suffix[:, 0:1]
        most = jnp.max(local, axis=1, keepdims=True)
        tail_part = jnp.where(lane - 64 == head_row, total, jnp.where(lane - 72 == head_row, most, 0.0))
        tail_part = jnp.broadcast_to(jnp.sum(tail_part, axis=0, keepdims=True), (8, 128))
        for half in range(2):
            part = local[:, half * 128 : (half + 1) * 128]
            for k in range(4):
                first = pltpu.roll(part, (128 - 32 * k) % 128, 1) if k else part
                second = pltpu.roll(pltpu.roll(part, 7, 0), (160 - 32 * k) % 128, 1) if k != 1 else pltpu.roll(part, 7, 0)
                row = jnp.where(lane < 32, first, jnp.where(lane < 64, second, tail_part))
                for n in range(4):
                    S[n * 8 + half * 4 + k] = row[2 * n : 2 * n + 1, :]
        R[pl.ds(s, 1)] = S[pl.ds(s, 1)]

        def send_rows(o, carry):
            peer = (s + o) % 32
            pltpu.make_async_remote_copy(
                src_ref=S.at[peer],
                dst_ref=R.at[s],
                send_sem=lws,
                recv_sem=lwr,
                device_id={"sp": peer},
                device_id_type=MESH,
            ).start()
            return carry

        lax.fori_loop(1, 32, send_rows, 0)

    def block_of(owner, i):
        at = ((owner - s + i + 32) % 8 + 8 * slot(i)) * BLOCK
        return T.at[pl.ds(pl.multiple_of(at, BLOCK), BLOCK)]

    def pass_on(owner, i, to, recv):
        block = block_of(owner, i)
        pltpu.make_async_remote_copy(
            src_ref=block,
            dst_ref=block,
            send_sem=xs,
            recv_sem=recv,
            device_id={"tp": to},
            device_id_type=MESH,
        ).start()

    half_block = BLOCK // 2

    def pass_half(owner, i, half, to):
        at = ((owner - s + i + 32) % 8 + 8 * slot(i)) * BLOCK + half * half_block
        part = T.at[pl.ds(pl.multiple_of(at, half_block), half_block)]
        pltpu.make_async_remote_copy(
            src_ref=part,
            dst_ref=part,
            send_sem=xs,
            recv_sem=xf.at[i, half],
            device_id={"tp": to},
            device_id_type=MESH,
        ).start()

    one_block = T.at[0:BLOCK]

    def stage_a(j):
        i = due_at(j)
        arrived(one_block, p1r.at[i])
        pass_on(t, i, right, xl.at[i])
        pass_on(t, i, left, xr.at[i])
        pass_on(t, i, mate, dr.at[i])

    def stage_b(j):
        i = due_at(j)
        arrived(one_block, xl.at[i])
        pass_half(left, i, 0, right)
        pass_on(left, i, mate, dr.at[i])
        arrived(one_block, xr.at[i])
        pass_half(right, i, 1, left)
        pass_on(right, i, mate, dr.at[i])

    def stage_c(j):
        i = due_at(j)
        arrived(T.at[0:half_block], xf.at[i, 0])
        arrived(T.at[0:half_block], xf.at[i, 1])
        pass_on(across, i, mate, dr.at[i])

    def write_out(i):
        at = pl.ds(pl.multiple_of(slot(i) * GROUP, GROUP), GROUP)
        return (
            pltpu.make_async_copy(OK.at[at], out_keys.at[at], loc.at[6]),
            pltpu.make_async_copy(OV.at[at], out_values.at[at], loc.at[7]),
        )

    def stage_n(j):
        i = due_at(j)
        arrived(T.at[0 : 4 * BLOCK], dr.at[i])
        start = pl.multiple_of(slot(i) * GROUP, GROUP)
        norm_group(T, start, N, j * GROUP, gain)

    def stage_d(j):
        i = due_at(j)
        start = pl.multiple_of(slot(i) * GROUP, GROUP)
        keys, values = project(N[j * GROUP : (j + 1) * GROUP, :])
        OK[pl.ds(start, GROUP), :] = keys
        OV[pl.ds(start, GROUP), :] = values
        for copy in write_out(i):
            copy.start()

    def column(row, first):
        return jnp.sum(jnp.where(lane - first == head_row, row, 0.0), axis=1, keepdims=True)

    def log_weights():
        arrived(R.at[0:31], lwr)
        received = R[:, 0, :]
        row = iota((32, 128), 0)
        lane32 = iota((32, 128), 1)
        suffix = received
        step = 1
        while step < 32:
            suffix = suffix + jnp.where(row < 32 - step, pltpu.roll(suffix, 32 - step, 0), 0.0)
            step *= 2
        exclusive = jnp.where(row < 31, pltpu.roll(suffix, 31, 0), 0.0)
        peaks = jnp.max(received + pltpu.roll(exclusive, 8, 1), axis=0, keepdims=True)
        PEAK[...] = jnp.broadcast_to(column(peaks, 72), (8, 128))
        mine = jnp.sum(jnp.where(row == s, exclusive, 0.0), axis=0, keepdims=True)
        LOC[...] += column(mine, 64)
        tails = [
            jnp.sum(jnp.where(lane32 == 64 + 2 * n_me + h, exclusive, 0.0), axis=1, keepdims=True)
            for h in range(2)
        ]
        L[...] = received + jnp.where(lane32 < 32, tails[0], tails[1])
        for h in range(2):
            wide = jnp.zeros((8, 128), F32)
            for k in range(4):
                rows = L[pl.ds(k, 8, stride=4), :]
                shift = (32 * k - 32 * h) % 128
                moved = pltpu.roll(rows, shift, 1) if shift else rows
                wide = jnp.where((lane >= 32 * k) & (lane < 32 * k + 32), moved, wide)
            for g in range(8):
                LW[h : h + 1, g * 128 : (g + 1) * 128] = wide[g : g + 1, :]
        out_weights[...] = LW[...]

        query = new_query[...].astype(F32)
        for n in range(4):
            Q8[2 * n : 2 * n + 1, :] = jnp.where(lane1 < 64, query[n : n + 1, :], 0.0)
            Q8[2 * n + 1 : 2 * n + 2, :] = jnp.where(lane1 < 64, 0.0, query[n : n + 1, :])
        NUM[...] = jnp.zeros_like(NUM)
        DEN[...] = jnp.zeros_like(DEN)

    def project(rows):
        both = jnp.dot(rows, W[...].reshape(D, 384), preferred_element_type=F32)
        return (both[:, 0:128] * 0.125).astype(BF16), both[:, 128:384].astype(BF16)

    def own_read(n):
        keys, values = project(X[n * GROUP : (n + 1) * GROUP, :])
        scores = lax.dot_general(Q8[...].astype(BF16), keys, NT, preferred_element_type=F32)
        terms = jnp.exp(LOC[...] - PEAK[:, 0:1]) * scores
        terms = jnp.where(iota((8, GROUP), 0) // 2 == n, terms, 0.0)
        DEN[...] += jnp.broadcast_to(jnp.sum(terms, axis=1, keepdims=True), (8, 128))
        NUM[...] += jnp.dot(terms.astype(BF16), values, preferred_element_type=F32)

    def share(buffer, slot_of, peers, send, recv):
        for to in peers:
            pltpu.make_async_remote_copy(
                src_ref=buffer.at[slot_of],
                dst_ref=buffer.at[slot_of],
                send_sem=send,
                recv_sem=recv,
                device_id={"sp": to},
                device_id_type=MESH,
            ).start()

    def sum_y():
        value = jnp.where(head_row % 2 == 0, NUM[:, 0:128], NUM[:, 128:256])
        E1[pl.ds(y, 1)] = jnp.concatenate([value, DEN[...]], axis=0).reshape(1, 16, 128)
        share(E1, y, [z * 4 + (y + o) % 4 for o in range(1, 4)], es.at[0], er.at[0])

    def sum_z():
        arrived(E1.at[0:3], er.at[0])
        E2[pl.ds(z, 1)] = ((E1[0] + E1[1]) + (E1[2] + E1[3])).reshape(1, 16, 128)
        share(E2, z, [((z + o) % 8) * 4 + y for o in range(1, 8)], es.at[1], er.at[1])

    def finish():
        arrived(E2.at[0:7], er.at[1])
        total = jnp.sum(E2[...], axis=0)
        numerator, denominator = total[0:8], total[8:16, 0:1]
        peak = PEAK[:, 0:1]
        gate = jnp.sum(
            jnp.where(iota((8, 32), 1) == 2 * t + iota((8, 32), 0) % 2, GN8[...], 0.0), axis=1, keepdims=True
        )
        own = jnp.sum(Q8[...] * (KN8[...] * 0.125).astype(BF16).astype(F32), axis=1, keepdims=True)
        top = jnp.maximum(peak, gate)
        old_part = jnp.exp(peak - top)
        new_part = jnp.exp(gate - top) * own
        value = old_part * numerator + new_part * VN8[...].astype(BF16).astype(F32)
        weight = old_part * denominator + new_part
        read = value / jnp.maximum(jnp.abs(weight), 1.0)
        for n in range(4):
            for h in range(2):
                A0[n : n + 1, h * 128 : (h + 1) * 128] = read[2 * n + h : 2 * n + h + 1, :]
        out_read[...] = A0[...].astype(BF16)

    lane1 = iota((1, 128), 1)

    def new_row_parts():
        total = jnp.zeros((4, 128), F32)
        for g in range(D // 128):
            v = new_rows[:, g * 128 : (g + 1) * 128].astype(F32)
            total = total + v * v
        inverse = lax.rsqrt(jnp.sum(total, axis=-1, keepdims=True) * (1.0 / D) + EPSILON)
        NN[...] = jnp.zeros_like(NN)
        for g in range(D // 128):
            at = slice(g * 128, (g + 1) * 128)
            NN[0:4, at] = new_rows[:, at].astype(F32) * inverse * gain[g : g + 1, :].astype(F32)
        fresh = NN[...].astype(BF16)
        both = jnp.dot(fresh, W[...].reshape(D, 384), preferred_element_type=F32)
        gates_new = lax.dot_general(fresh, GW[...], NT, preferred_element_type=F32)
        for n in range(4):
            for h in range(2):
                at = slice(2 * n + h, 2 * n + h + 1)
                KN8[at, :] = both[n : n + 1, 0:128]
                VN8[at, :] = both[n : n + 1, 128 * (h + 1) : 128 * (h + 2)]
                GN8[at, :] = gates_new[n : n + 1, :]

    for copy in small:
        copy.wait()
    for n in range(4):
        gates(n)
    local_weights()
    arrived(W.at[0, 0], wc)
    for o in range(1, 4):
        shard_to(far_z, half_z + (z + o) % 4, w2)
    arrived(W.at[0:3, 0], wh)
    y_send(half_z, y, up, 0)
    y_send(half_z, y, down, 1)
    start_leg(1)

    @pl.when(inner == 0)
    def _():
        start_leg(2)

    arrived(W.at[0:4, 0], wy.at[0])
    y_send(half_z, down, up, 2)

    @pl.when(inner == 1)
    def _():
        start_leg(2)

    start_leg(3)
    stage_a(0)
    arrived(W.at[0:3, 0], w2)
    y_send(other_z, y, up, 3)
    y_send(other_z, y, down, 4)
    stage_b(0)
    stage_a(1)
    stage_c(0)
    arrived(W.at[0:4, 0], wy.at[4])
    y_send(other_z, up, down, 5)
    stage_a(2)
    stage_b(1)
    stage_n(0)
    log_weights()
    stage_b(2)
    stage_a(3)
    for which in (1, 2, 3, 5):
        arrived(W.at[0:4, 0], wy.at[which])
    own_read(0)
    own_read(1)
    stage_c(1)
    stage_c(2)
    own_read(2)
    own_read(3)
    sum_y()
    stage_b(3)
    stage_n(1)
    stage_d(0)
    sum_z()
    stage_c(3)
    stage_d(1)
    new_row_parts()
    stage_n(2)
    stage_d(2)
    stage_n(3)
    stage_d(3)
    finish()
    arrived(OK, loc.at[6])
    arrived(OV, loc.at[7])

    arrived(R.at[0:31], lws)
    arrived(E1.at[0:3], es.at[0])
    arrived(E2.at[0:7], es.at[1])
    arrived(W.at[0:7, 0], ws1)
    arrived(W.at[0:6], ws2)
    arrived(T.at[0 : 28 * BLOCK], xs)

    def leg_done(i):
        dest, _, _, remote = first_leg(i)

        @pl.when(dest != s)
        def _():
            remote.wait_send()

    for i in range(4):
        leg_done(i)


def place(keys, values, weights, read, out_keys, out_values, out_weights, out_read, sems):
    copies = [
        pltpu.make_async_copy(keys, out_keys.at[0], sems.at[0]),
        pltpu.make_async_copy(values, out_values.at[0], sems.at[1]),
        pltpu.make_async_copy(weights, out_weights.at[0], sems.at[2]),
        pltpu.make_async_copy(read, out_read, sems.at[3]),
    ]
    for copy in copies:
        copy.start()
    for copy in copies:
        copy.wait()


def per_device(
    tokens,
    new_rows,
    new_query,
    norm_gain,
    key_weight,
    value_weight,
    input_weight,
    forget_weight,
    forget_bias,
    gate_offsets,
):
    any_space = pl.BlockSpec(memory_space=pl.ANY)
    vmem = pl.BlockSpec(memory_space=pltpu.VMEM)
    smem = pl.BlockSpec(memory_space=pltpu.SMEM)
    dma = pltpu.SemaphoreType.DMA
    keys, values, weights, read = pl.pallas_call(
        kernel,
        out_shape=(
            jax.ShapeDtypeStruct((ROWS, 128), BF16),
            jax.ShapeDtypeStruct((ROWS, 256), BF16),
            jax.ShapeDtypeStruct((2, ROWS), F32),
            jax.ShapeDtypeStruct((4, 256), BF16),
        ),
        in_specs=[any_space] * 8 + [smem, any_space],
        out_specs=(any_space, any_space, vmem, vmem),
        scratch_shapes=[
            pltpu.VMEM((4, D), BF16),
            pltpu.VMEM((4, 128), BF16),
            pltpu.VMEM((16, 128), BF16),
            pltpu.VMEM((4, 2, 2, GROUP), F32),
            pltpu.VMEM((ROWS, D), BF16),
            pltpu.VMEM((ROWS, D), BF16),
            pltpu.VMEM((ROWS, D), BF16),
            pltpu.VMEM((8, 4, 64, 384), BF16),
            pltpu.VMEM((ROWS, 128), BF16),
            pltpu.VMEM((ROWS, 256), BF16),
            pltpu.VMEM((4, 32, GROUP), F32),
            pltpu.VMEM((32, D), BF16),
            pltpu.VMEM((8, D), F32),
            pltpu.VMEM((8, GROUP), F32),
            pltpu.VMEM((8, GROUP), F32),
            pltpu.VMEM((8, GROUP), F32),
            pltpu.VMEM((8, GROUP), F32),
            pltpu.VMEM((32, 1, 128), F32),
            pltpu.VMEM((32, 1, 128), F32),
            pltpu.VMEM((32, 128), F32),
            pltpu.VMEM((2, ROWS), F32),
            pltpu.VMEM((8, 128), F32),
            pltpu.VMEM((8, 128), F32),
            pltpu.VMEM((8, 256), F32),
            pltpu.VMEM((8, 128), F32),
            pltpu.VMEM((8, 128), F32),
            pltpu.VMEM((8, 128), F32),
            pltpu.VMEM((8, 32), F32),
            pltpu.VMEM((4, 16, 128), F32),
            pltpu.VMEM((8, 16, 128), F32),
            pltpu.VMEM((4, 256), F32),
            dma((4,)),
            dma((4,)),
            dma((4,)),
            dma((4,)),
            dma((4, 2)),
            dma((4,)),
            dma,
            dma,
            dma,
            dma,
            dma,
            dma,
            dma((6,)),
            dma,
            dma,
            dma((2,)),
            dma((2,)),
            dma((14,)),
        ],
        compiler_params=pltpu.CompilerParams(collective_id=0, has_side_effects=True),
    )(
        tokens.reshape(ROWS, D),
        new_rows,
        new_query,
        norm_gain.reshape(16, 128),
        key_weight,
        value_weight,
        input_weight.T,
        forget_weight.T,
        forget_bias,
        jnp.transpose(gate_offsets, (0, 2, 3, 1)),
    )
    return pl.pallas_call(
        place,
        out_shape=(
            jax.ShapeDtypeStruct((1, ROWS, 128), BF16),
            jax.ShapeDtypeStruct((1, ROWS, 256), BF16),
            jax.ShapeDtypeStruct((1, 2, ROWS), F32),
            jax.ShapeDtypeStruct((4, 256), BF16),
        ),
        in_specs=[vmem] * 4,
        out_specs=[any_space] * 4,
        scratch_shapes=[dma((4,))],
    )(keys, values, weights, read)


def solution(mesh):
    return jax.shard_map(
        per_device,
        mesh=mesh,
        in_specs=(
            P("gr", "sp", None),
            P("gr", None),
            P("gr", "tp"),
            P(),
            P("sp", "tp"),
            P("sp", "tp"),
            P(),
            P(),
            P("tp"),
            P("gr", "sp", None, "tp"),
        ),
        out_specs=(
            P(("gr", "sp"), None, "tp"),
            P(("gr", "sp"), None, "tp"),
            P(("gr", "sp"), "tp", None),
            P("gr", "tp"),
        ),
        check_vma=False,
    )
```

```python
import jax
import jax.numpy as jnp
from jax import lax
from jax.experimental import pallas as pl
from jax.experimental.pallas import tpu as pltpu
from jax.sharding import PartitionSpec as P

EPSILON = 1e-06
MESH = pl.DeviceIdType.MESH
F32 = jnp.float32
BF16 = jnp.bfloat16
NT = (((1,), (1,)), ((), ()))

D = 2048
ROWS = 1024
GROUP = 256
BLOCK = 32
CHUNK = 64


def iota(shape, dim):
    return lax.broadcasted_iota(jnp.int32, shape, dim)


def xor2(a, b):
    return 2 * ((a // 2 + b // 2) % 2) + (a % 2 + b % 2) % 2


def norm_chunk(read, write, gain_ref, rows):
    total = jnp.zeros((rows, 128), F32)
    for c in range(D // 128):
        v = read(c).astype(F32)
        total = total + v * v
    inverse = lax.rsqrt(jnp.sum(total, axis=-1, keepdims=True) * (1.0 / D) + EPSILON)
    for c in range(D // 128):
        v = read(c).astype(F32)
        write(c, (v * inverse * gain_ref[c : c + 1, :].astype(F32)).astype(BF16))


def norm_group(src, start, dst, first, gain_ref):
    def body(u, carry):
        at = pl.multiple_of(start + u * CHUNK, CHUNK)
        to = pl.multiple_of(first + u * CHUNK, CHUNK)

        def read(c):
            return src[pl.ds(at, CHUNK), c * 128 : (c + 1) * 128]

        def write(c, v):
            dst[pl.ds(to, CHUNK), c * 128 : (c + 1) * 128] = v

        norm_chunk(read, write, gain_ref, CHUNK)
        return carry

    lax.fori_loop(0, GROUP // CHUNK, body, 0)


def kernel(
    tokens,
    new_rows_in,
    new_query_in,
    gain_in,
    key_weight,
    value_weight,
    input_weight,
    forget_weight,
    bias,
    offsets_in,
    out_keys,
    out_values,
    out_weights,
    out_read,
    new_rows,
    new_query,
    gain,
    offsets,
    T,
    X,
    N,
    W,
    OK,
    OV,
    G,
    GW,
    NN,
    IG,
    PRE,
    LF,
    LOC,
    S,
    R,
    L,
    LW,
    PEAK,
    Q8,
    NUM,
    DEN,
    KN8,
    VN8,
    GN8,
    E1,
    E2,
    A0,
    p1s,
    p1r,
    xl,
    xr,
    xf,
    dr,
    xs,
    lws,
    lwr,
    wc,
    wh,
    w2,
    wy,
    ws1,
    ws2,
    es,
    er,
    loc,
):
    s = lax.axis_index("sp")
    t = lax.axis_index("tp")
    z, y = s // 4, s % 4
    x, c = t // 2, t % 2
    k_me = s // 8
    n_me = s // 8
    right = ((x + 1) % 4) * 2 + c
    left = ((x + 3) % 4) * 2 + c
    across = ((x + 2) % 4) * 2 + c
    mate = t + 1 - 2 * c

    barrier = pltpu.get_barrier_semaphore()

    def greet(o, carry):
        pl.semaphore_signal(barrier, inc=1, device_id={"sp": (s + o) % 32}, device_id_type=MESH)
        return carry

    lax.fori_loop(1, 32, greet, 0)
    for who in (right, left, mate):
        pl.semaphore_signal(barrier, inc=1, device_id={"tp": who}, device_id_type=MESH)

    own_k = pltpu.make_async_copy(key_weight, W.at[z, y, :, 0:128], loc.at[4])
    own_v = pltpu.make_async_copy(value_weight, W.at[z, y, :, 128:384], loc.at[5])
    own_k.start()
    own_v.start()
    loads = [
        pltpu.make_async_copy(tokens.at[n * GROUP : (n + 1) * GROUP], X.at[n * GROUP : (n + 1) * GROUP], loc.at[n])
        for n in range(4)
    ]
    loads[0].start()
    small = [
        pltpu.make_async_copy(src, dst, loc.at[8 + at])
        for at, (src, dst) in enumerate(
            (
                (gain_in, gain),
                (input_weight, GW.at[0:16]),
                (forget_weight, GW.at[16:32]),
                (offsets_in, offsets),
                (new_rows_in, new_rows),
                (new_query_in, new_query),
            )
        )
    ]
    for copy in small:
        copy.start()
    for load in loads[1:]:
        load.start()
    own_k.wait()
    own_v.wait()
    pl.semaphore_wait(barrier, 34)

    half_z = (z // 4) * 4
    other_z = 4 - half_z
    far_z = (z + 4) % 8

    def shard_to(row, to_z, recv):
        pltpu.make_async_remote_copy(
            src_ref=W.at[row, y],
            dst_ref=W.at[row, y],
            send_sem=ws1,
            recv_sem=recv,
            device_id={"sp": to_z * 4 + y},
            device_id_type=MESH,
        ).start()

    inner = (k_me // 2 + k_me % 2) % 2

    def sent_at(j):
        return inner * (0, 1, 2, 3)[j] + (1 - inner) * ((1 - c) * (0, 3, 2, 1)[j] + c * (0, 2, 3, 1)[j])

    def due_at(j):
        return inner * (0, 2, 1, 3)[j] + (1 - inner) * ((1 - c) * (0, 3, 1, 2)[j] + c * (0, 1, 3, 2)[j])

    def slot(i):
        return xor2(k_me, i)

    def first_leg(i):
        dest = (t - s + i + 32) % 8 + 8 * slot(i)
        src = tokens.at[pl.ds(pl.multiple_of(dest * BLOCK, BLOCK), BLOCK)]
        dst = T.at[pl.ds(pl.multiple_of(s * BLOCK, BLOCK), BLOCK)]
        remote = pltpu.make_async_remote_copy(
            src_ref=src,
            dst_ref=dst,
            send_sem=p1s.at[i],
            recv_sem=p1r.at[i],
            device_id={"sp": dest},
            device_id_type=MESH,
        )
        return dest, src, dst, remote

    def start_leg(j):
        i = sent_at(j)
        dest, src, dst, remote = first_leg(i)

        @pl.when(dest != s)
        def _():
            remote.start()

        @pl.when(dest == s)
        def _():
            pltpu.make_async_copy(src, dst, p1r.at[i]).start()

    start_leg(0)
    shard_to(z, far_z, wc)
    for o in range(1, 4):
        shard_to(z, half_z + (z + o) % 4, wh)


    def y_send(rows, column, to_y, which):
        pltpu.make_async_remote_copy(
            src_ref=W.at[pl.ds(rows, 4), column],
            dst_ref=W.at[pl.ds(rows, 4), column],
            send_sem=ws2,
            recv_sem=wy.at[which],
            device_id={"sp": z * 4 + to_y},
            device_id_type=MESH,
        ).start()

    def arrived(ref, sem):
        pltpu.make_async_copy(ref, ref, sem).wait()

    up, down = (y + 1) % 4, (y + 3) % 4

    def gates(n):
        loads[n].wait()
        norm_group(X, n * GROUP, X, n * GROUP, gain)
        own = X[n * GROUP : (n + 1) * GROUP, :]
        G[n] = lax.dot_general(GW[...], own, NT, preferred_element_type=F32)

    lane = iota((8, 128), 1)
    head_row = iota((8, 128), 0)

    def local_weights():
        gate_row = iota((32, GROUP), 0)
        for n in range(4):
            for h in range(2):
                at = slice(2 * n + h, 2 * n + h + 1)
                mine = jnp.where(gate_row == 2 * t + h, G[n], 0.0)
                IG[at, :] = jnp.sum(mine, axis=0, keepdims=True) + offsets[n, 0, h : h + 1, :]
                mine = jnp.where(gate_row == 16 + 2 * t + h, G[n], 0.0)
                PRE[at, :] = jnp.sum(mine, axis=0, keepdims=True) + bias[h]
                LF[at, :] = offsets[n, 1, h : h + 1, :]

        wide_lane = iota((8, GROUP), 1)
        pre = PRE[...]
        soft = jnp.minimum(pre, 0.0) - jnp.log1p(jnp.exp(-jnp.abs(pre)))
        log_forget = soft + LF[...]
        suffix = log_forget
        step = 1
        while step < GROUP:
            suffix = suffix + jnp.where(wide_lane < GROUP - step, pltpu.roll(suffix, GROUP - step, 1), 0.0)
            step *= 2
        exclusive = jnp.where(wide_lane < GROUP - 1, pltpu.roll(suffix, GROUP - 1, 1), 0.0)
        local = IG[...] + exclusive
        LOC[...] = local
        total = suffix[:, 0:1]
        most = jnp.max(local, axis=1, keepdims=True)
        tail_part = jnp.where(lane - 64 == head_row, total, jnp.where(lane - 72 == head_row, most, 0.0))
        tail_part = jnp.broadcast_to(jnp.sum(tail_part, axis=0, keepdims=True), (8, 128))
        for half in range(2):
            part = local[:, half * 128 : (half + 1) * 128]
            for k in range(4):
                first = pltpu.roll(part, (128 - 32 * k) % 128, 1) if k else part
                second = pltpu.roll(pltpu.roll(part, 7, 0), (160 - 32 * k) % 128, 1) if k != 1 else pltpu.roll(part, 7, 0)
                row = jnp.where(lane < 32, first, jnp.where(lane < 64, second, tail_part))
                for n in range(4):
                    S[n * 8 + half * 4 + k] = row[2 * n : 2 * n + 1, :]
        R[pl.ds(s, 1)] = S[pl.ds(s, 1)]

        def send_rows(o, carry):
            peer = (s + o) % 32
            pltpu.make_async_remote_copy(
                src_ref=S.at[peer],
                dst_ref=R.at[s],
                send_sem=lws,
                recv_sem=lwr,
                device_id={"sp": peer},
                device_id_type=MESH,
            ).start()
            return carry

        lax.fori_loop(1, 32, send_rows, 0)

    def block_of(owner, i):
        at = ((owner - s + i + 32) % 8 + 8 * slot(i)) * BLOCK
        return T.at[pl.ds(pl.multiple_of(at, BLOCK), BLOCK)]

    def pass_on(owner, i, to, recv):
        block = block_of(owner, i)
        pltpu.make_async_remote_copy(
            src_ref=block,
            dst_ref=block,
            send_sem=xs,
            recv_sem=recv,
            device_id={"tp": to},
            device_id_type=MESH,
        ).start()

    half_block = BLOCK // 2

    def pass_half(owner, i, half, to, recv):
        at = ((owner - s + i + 32) % 8 + 8 * slot(i)) * BLOCK + half * half_block
        part = T.at[pl.ds(pl.multiple_of(at, half_block), half_block)]
        pltpu.make_async_remote_copy(
            src_ref=part,
            dst_ref=part,
            send_sem=xs,
            recv_sem=recv,
            device_id={"tp": to},
            device_id_type=MESH,
        ).start()

    one_block = T.at[0:BLOCK]

    half_rows = T.at[0:half_block]

    def stage_a(j):
        i = due_at(j)
        arrived(one_block, p1r.at[i])
        for half in range(2):
            pass_half(t, i, half, right, xl.at[i, half])
            pass_half(t, i, 1 - half, left, xr.at[i, 1 - half])
        pass_on(t, i, mate, dr.at[i])

    def stage_b(j):
        i = due_at(j)
        arrived(half_rows, xl.at[i, 0])
        pass_half(left, i, 0, right, xf.at[i, 0])
        arrived(half_rows, xr.at[i, 1])
        pass_half(right, i, 1, left, xf.at[i, 1])
        arrived(half_rows, xl.at[i, 1])
        pass_on(left, i, mate, dr.at[i])
        arrived(half_rows, xr.at[i, 0])
        pass_on(right, i, mate, dr.at[i])

    def stage_c(j):
        i = due_at(j)
        arrived(half_rows, xf.at[i, 0])
        arrived(half_rows, xf.at[i, 1])
        pass_on(across, i, mate, dr.at[i])

    def write_out(i):
        at = pl.ds(pl.multiple_of(slot(i) * GROUP, GROUP), GROUP)
        return (
            pltpu.make_async_copy(OK.at[at], out_keys.at[at], loc.at[6]),
            pltpu.make_async_copy(OV.at[at], out_values.at[at], loc.at[7]),
        )

    def stage_n(j):
        i = due_at(j)
        arrived(T.at[0 : 4 * BLOCK], dr.at[i])
        start = pl.multiple_of(slot(i) * GROUP, GROUP)
        norm_group(T, start, N, j * GROUP, gain)

    def stage_d(j, groups=1):
        keys, values = project(N[j * GROUP : (j + groups) * GROUP, :])
        for g in range(groups):
            i = due_at(j + g)
            start = pl.multiple_of(slot(i) * GROUP, GROUP)
            OK[pl.ds(start, GROUP), :] = keys[g * GROUP : (g + 1) * GROUP]
            OV[pl.ds(start, GROUP), :] = values[g * GROUP : (g + 1) * GROUP]
            for copy in write_out(i):
                copy.start()

    def column(row, first):
        return jnp.sum(jnp.where(lane - first == head_row, row, 0.0), axis=1, keepdims=True)

    def log_weights():
        arrived(R.at[0:31], lwr)
        received = R[:, 0, :]
        row = iota((32, 128), 0)
        lane32 = iota((32, 128), 1)
        suffix = received
        step = 1
        while step < 32:
            suffix = suffix + jnp.where(row < 32 - step, pltpu.roll(suffix, 32 - step, 0), 0.0)
            step *= 2
        exclusive = jnp.where(row < 31, pltpu.roll(suffix, 31, 0), 0.0)
        peaks = jnp.max(received + pltpu.roll(exclusive, 8, 1), axis=0, keepdims=True)
        PEAK[...] = jnp.broadcast_to(column(peaks, 72), (8, 128))
        mine = jnp.sum(jnp.where(row == s, exclusive, 0.0), axis=0, keepdims=True)
        LOC[...] += column(mine, 64)
        tails = [
            jnp.sum(jnp.where(lane32 == 64 + 2 * n_me + h, exclusive, 0.0), axis=1, keepdims=True)
            for h in range(2)
        ]
        L[...] = received + jnp.where(lane32 < 32, tails[0], tails[1])
        for h in range(2):
            wide = jnp.zeros((8, 128), F32)
            for k in range(4):
                rows = L[pl.ds(k, 8, stride=4), :]
                shift = (32 * k - 32 * h) % 128
                moved = pltpu.roll(rows, shift, 1) if shift else rows
                wide = jnp.where((lane >= 32 * k) & (lane < 32 * k + 32), moved, wide)
            for g in range(8):
                LW[h : h + 1, g * 128 : (g + 1) * 128] = wide[g : g + 1, :]
        out_weights[...] = LW[...]

        query = new_query[...].astype(F32)
        for n in range(4):
            Q8[2 * n : 2 * n + 1, :] = jnp.where(lane1 < 64, query[n : n + 1, :], 0.0)
            Q8[2 * n + 1 : 2 * n + 2, :] = jnp.where(lane1 < 64, 0.0, query[n : n + 1, :])
        NUM[...] = jnp.zeros_like(NUM)
        DEN[...] = jnp.zeros_like(DEN)

    def project(rows):
        both = jnp.dot(rows, W[...].reshape(D, 384), preferred_element_type=F32)
        return (both[:, 0:128] * 0.125).astype(BF16), both[:, 128:384].astype(BF16)

    def own_read(n):
        keys, values = project(X[n * GROUP : (n + 2) * GROUP, :])
        scores = lax.dot_general(Q8[...].astype(BF16), keys, NT, preferred_element_type=F32)
        weight = jnp.exp(LOC[...] - PEAK[:, 0:1])
        terms = jnp.concatenate([weight, weight], axis=1) * scores
        prompt = n + iota((8, 2 * GROUP), 1) // GROUP
        terms = jnp.where(iota((8, 2 * GROUP), 0) // 2 == prompt, terms, 0.0)
        DEN[...] += jnp.broadcast_to(jnp.sum(terms, axis=1, keepdims=True), (8, 128))
        NUM[...] += jnp.dot(terms.astype(BF16), values, preferred_element_type=F32)

    def share(buffer, slot_of, peers, send, recv):
        for to in peers:
            pltpu.make_async_remote_copy(
                src_ref=buffer.at[slot_of],
                dst_ref=buffer.at[slot_of],
                send_sem=send,
                recv_sem=recv,
                device_id={"sp": to},
                device_id_type=MESH,
            ).start()

    def sum_y():
        value = jnp.where(head_row % 2 == 0, NUM[:, 0:128], NUM[:, 128:256])
        E1[pl.ds(y, 1)] = jnp.concatenate([value, DEN[...]], axis=0).reshape(1, 16, 128)
        share(E1, y, [z * 4 + (y + o) % 4 for o in range(1, 4)], es.at[0], er.at[0])

    def sum_z():
        arrived(E1.at[0:3], er.at[0])
        E2[pl.ds(z, 1)] = ((E1[0] + E1[1]) + (E1[2] + E1[3])).reshape(1, 16, 128)
        share(E2, z, [((z + o) % 8) * 4 + y for o in range(1, 8)], es.at[1], er.at[1])

    def finish():
        arrived(E2.at[0:7], er.at[1])
        total = jnp.sum(E2[...], axis=0)
        numerator, denominator = total[0:8], total[8:16, 0:1]
        peak = PEAK[:, 0:1]
        gate = jnp.sum(
            jnp.where(iota((8, 32), 1) == 2 * t + iota((8, 32), 0) % 2, GN8[...], 0.0), axis=1, keepdims=True
        )
        own = jnp.sum(Q8[...] * (KN8[...] * 0.125).astype(BF16).astype(F32), axis=1, keepdims=True)
        top = jnp.maximum(peak, gate)
        old_part = jnp.exp(peak - top)
        new_part = jnp.exp(gate - top) * own
        value = old_part * numerator + new_part * VN8[...].astype(BF16).astype(F32)
        weight = old_part * denominator + new_part
        read = value / jnp.maximum(jnp.abs(weight), 1.0)
        for n in range(4):
            for h in range(2):
                A0[n : n + 1, h * 128 : (h + 1) * 128] = read[2 * n + h : 2 * n + h + 1, :]
        out_read[...] = A0[...].astype(BF16)

    lane1 = iota((1, 128), 1)

    def new_row_parts():
        total = jnp.zeros((4, 128), F32)
        for g in range(D // 128):
            v = new_rows[:, g * 128 : (g + 1) * 128].astype(F32)
            total = total + v * v
        inverse = lax.rsqrt(jnp.sum(total, axis=-1, keepdims=True) * (1.0 / D) + EPSILON)
        NN[...] = jnp.zeros_like(NN)
        for g in range(D // 128):
            at = slice(g * 128, (g + 1) * 128)
            NN[0:4, at] = new_rows[:, at].astype(F32) * inverse * gain[g : g + 1, :].astype(F32)
        fresh = NN[...].astype(BF16)
        both = jnp.dot(fresh, W[...].reshape(D, 384), preferred_element_type=F32)
        gates_new = lax.dot_general(fresh, GW[...], NT, preferred_element_type=F32)
        for n in range(4):
            for h in range(2):
                at = slice(2 * n + h, 2 * n + h + 1)
                KN8[at, :] = both[n : n + 1, 0:128]
                VN8[at, :] = both[n : n + 1, 128 * (h + 1) : 128 * (h + 2)]
                GN8[at, :] = gates_new[n : n + 1, :]

    for copy in small:
        copy.wait()
    for n in range(4):
        gates(n)
    local_weights()
    arrived(W.at[0, 0], wc)
    for o in range(1, 4):
        shard_to(far_z, half_z + (z + o) % 4, w2)
    arrived(W.at[0:3, 0], wh)
    y_send(half_z, y, up, 0)
    y_send(half_z, y, down, 1)
    start_leg(1)

    @pl.when(inner == 0)
    def _():
        start_leg(2)

    arrived(W.at[0:4, 0], wy.at[0])
    y_send(half_z, down, up, 2)

    @pl.when(inner == 1)
    def _():
        start_leg(2)

    start_leg(3)
    stage_a(0)
    arrived(W.at[0:3, 0], w2)
    y_send(other_z, y, up, 3)
    y_send(other_z, y, down, 4)
    stage_b(0)
    stage_a(1)
    stage_c(0)
    arrived(W.at[0:4, 0], wy.at[4])
    y_send(other_z, up, down, 5)
    stage_a(2)
    stage_b(1)
    stage_n(0)
    log_weights()
    stage_b(2)
    stage_a(3)
    for which in (1, 2, 3, 5):
        arrived(W.at[0:4, 0], wy.at[which])
    own_read(0)
    stage_c(1)
    stage_c(2)
    own_read(2)
    sum_y()
    stage_b(3)
    stage_n(1)
    stage_d(0, 2)
    sum_z()
    stage_c(3)
    stage_n(2)
    new_row_parts()
    stage_d(2)
    stage_n(3)
    stage_d(3)
    finish()
    arrived(OK, loc.at[6])
    arrived(OV, loc.at[7])

    arrived(R.at[0:31], lws)
    arrived(E1.at[0:3], es.at[0])
    arrived(E2.at[0:7], es.at[1])
    arrived(W.at[0:7, 0], ws1)
    arrived(W.at[0:6], ws2)
    arrived(T.at[0 : 28 * BLOCK], xs)

    def leg_done(i):
        dest, _, _, remote = first_leg(i)

        @pl.when(dest != s)
        def _():
            remote.wait_send()

    for i in range(4):
        leg_done(i)


def place(keys, values, weights, read, out_keys, out_values, out_weights, out_read, sems):
    copies = [
        pltpu.make_async_copy(keys, out_keys.at[0], sems.at[0]),
        pltpu.make_async_copy(values, out_values.at[0], sems.at[1]),
        pltpu.make_async_copy(weights, out_weights.at[0], sems.at[2]),
        pltpu.make_async_copy(read, out_read, sems.at[3]),
    ]
    for copy in copies:
        copy.start()
    for copy in copies:
        copy.wait()


def per_device(
    tokens,
    new_rows,
    new_query,
    norm_gain,
    key_weight,
    value_weight,
    input_weight,
    forget_weight,
    forget_bias,
    gate_offsets,
):
    any_space = pl.BlockSpec(memory_space=pl.ANY)
    vmem = pl.BlockSpec(memory_space=pltpu.VMEM)
    smem = pl.BlockSpec(memory_space=pltpu.SMEM)
    dma = pltpu.SemaphoreType.DMA
    keys, values, weights, read = pl.pallas_call(
        kernel,
        out_shape=(
            jax.ShapeDtypeStruct((ROWS, 128), BF16),
            jax.ShapeDtypeStruct((ROWS, 256), BF16),
            jax.ShapeDtypeStruct((2, ROWS), F32),
            jax.ShapeDtypeStruct((4, 256), BF16),
        ),
        in_specs=[any_space] * 8 + [smem, any_space],
        out_specs=(any_space, any_space, vmem, vmem),
        scratch_shapes=[
            pltpu.VMEM((4, D), BF16),
            pltpu.VMEM((4, 128), BF16),
            pltpu.VMEM((16, 128), BF16),
            pltpu.VMEM((4, 2, 2, GROUP), F32),
            pltpu.VMEM((ROWS, D), BF16),
            pltpu.VMEM((ROWS, D), BF16),
            pltpu.VMEM((ROWS, D), BF16),
            pltpu.VMEM((8, 4, 64, 384), BF16),
            pltpu.VMEM((ROWS, 128), BF16),
            pltpu.VMEM((ROWS, 256), BF16),
            pltpu.VMEM((4, 32, GROUP), F32),
            pltpu.VMEM((32, D), BF16),
            pltpu.VMEM((8, D), F32),
            pltpu.VMEM((8, GROUP), F32),
            pltpu.VMEM((8, GROUP), F32),
            pltpu.VMEM((8, GROUP), F32),
            pltpu.VMEM((8, GROUP), F32),
            pltpu.VMEM((32, 1, 128), F32),
            pltpu.VMEM((32, 1, 128), F32),
            pltpu.VMEM((32, 128), F32),
            pltpu.VMEM((2, ROWS), F32),
            pltpu.VMEM((8, 128), F32),
            pltpu.VMEM((8, 128), F32),
            pltpu.VMEM((8, 256), F32),
            pltpu.VMEM((8, 128), F32),
            pltpu.VMEM((8, 128), F32),
            pltpu.VMEM((8, 128), F32),
            pltpu.VMEM((8, 32), F32),
            pltpu.VMEM((4, 16, 128), F32),
            pltpu.VMEM((8, 16, 128), F32),
            pltpu.VMEM((4, 256), F32),
            dma((4,)),
            dma((4,)),
            dma((4, 2)),
            dma((4, 2)),
            dma((4, 2)),
            dma((4,)),
            dma,
            dma,
            dma,
            dma,
            dma,
            dma,
            dma((6,)),
            dma,
            dma,
            dma((2,)),
            dma((2,)),
            dma((14,)),
        ],
        compiler_params=pltpu.CompilerParams(collective_id=0, has_side_effects=True),
    )(
        tokens.reshape(ROWS, D),
        new_rows,
        new_query,
        norm_gain.reshape(16, 128),
        key_weight,
        value_weight,
        input_weight.T,
        forget_weight.T,
        forget_bias,
        jnp.transpose(gate_offsets, (0, 2, 3, 1)),
    )
    return pl.pallas_call(
        place,
        out_shape=(
            jax.ShapeDtypeStruct((1, ROWS, 128), BF16),
            jax.ShapeDtypeStruct((1, ROWS, 256), BF16),
            jax.ShapeDtypeStruct((1, 2, ROWS), F32),
            jax.ShapeDtypeStruct((4, 256), BF16),
        ),
        in_specs=[vmem] * 4,
        out_specs=[any_space] * 4,
        scratch_shapes=[dma((4,))],
    )(keys, values, weights, read)


def solution(mesh):
    return jax.shard_map(
        per_device,
        mesh=mesh,
        in_specs=(
            P("gr", "sp", None),
            P("gr", None),
            P("gr", "tp"),
            P(),
            P("sp", "tp"),
            P("sp", "tp"),
            P(),
            P(),
            P("tp"),
            P("gr", "sp", None, "tp"),
        ),
        out_specs=(
            P(("gr", "sp"), None, "tp"),
            P(("gr", "sp"), None, "tp"),
            P(("gr", "sp"), "tp", None),
            P("gr", "tp"),
        ),
        check_vma=False,
    )
```

```python
import jax
import jax.numpy as jnp
from jax import lax
from jax.experimental import pallas as pl
from jax.experimental.pallas import tpu as pltpu
from jax.sharding import PartitionSpec as P

EPSILON = 1e-06
MESH = pl.DeviceIdType.MESH
F32 = jnp.float32
BF16 = jnp.bfloat16
NT = (((1,), (1,)), ((), ()))

D = 2048
ROWS = 1024
GROUP = 256
BLOCK = 32
CHUNK = 64


def iota(shape, dim):
    return lax.broadcasted_iota(jnp.int32, shape, dim)


def xor2(a, b):
    return 2 * ((a // 2 + b // 2) % 2) + (a % 2 + b % 2) % 2


def norm_chunk(read, write, gain_ref, rows):
    total = jnp.zeros((rows, 128), F32)
    for c in range(D // 128):
        v = read(c).astype(F32)
        total = total + v * v
    inverse = lax.rsqrt(jnp.sum(total, axis=-1, keepdims=True) * (1.0 / D) + EPSILON)
    for c in range(D // 128):
        v = read(c).astype(F32)
        write(c, (v * inverse * gain_ref[c : c + 1, :].astype(F32)).astype(BF16))


def norm_group(src, start, dst, first, gain_ref):
    def body(u, carry):
        at = pl.multiple_of(start + u * CHUNK, CHUNK)
        to = pl.multiple_of(first + u * CHUNK, CHUNK)

        def read(c):
            return src[pl.ds(at, CHUNK), c * 128 : (c + 1) * 128]

        def write(c, v):
            dst[pl.ds(to, CHUNK), c * 128 : (c + 1) * 128] = v

        norm_chunk(read, write, gain_ref, CHUNK)
        return carry

    lax.fori_loop(0, GROUP // CHUNK, body, 0)


def kernel(
    tokens,
    new_rows_in,
    new_query_in,
    gain_in,
    key_weight,
    value_weight,
    input_weight,
    forget_weight,
    bias,
    offsets_in,
    out_keys,
    out_values,
    out_weights,
    out_read,
    new_rows,
    new_query,
    gain,
    offsets,
    T,
    X,
    N,
    W,
    OK,
    OV,
    G,
    GW,
    NN,
    IG,
    PRE,
    LF,
    LOC,
    S,
    R,
    L,
    LW,
    PEAK,
    Q8,
    NUM,
    DEN,
    KN8,
    VN8,
    GN8,
    E1,
    E2,
    A0,
    p1s,
    p1r,
    xl,
    xr,
    xf,
    dr,
    xs,
    lws,
    lwr,
    wc,
    wh,
    w2,
    wy,
    ws1,
    ws2,
    es,
    er,
    loc,
):
    s = lax.axis_index("sp")
    t = lax.axis_index("tp")
    z, y = s // 4, s % 4
    x, c = t // 2, t % 2
    k_me = s // 8
    n_me = s // 8
    right = ((x + 1) % 4) * 2 + c
    left = ((x + 3) % 4) * 2 + c
    across = ((x + 2) % 4) * 2 + c
    mate = t + 1 - 2 * c

    barrier = pltpu.get_barrier_semaphore()

    def greet(o, carry):
        pl.semaphore_signal(barrier, inc=1, device_id={"sp": (s + o) % 32}, device_id_type=MESH)
        return carry

    lax.fori_loop(1, 32, greet, 0)
    for who in (right, left, mate):
        pl.semaphore_signal(barrier, inc=1, device_id={"tp": who}, device_id_type=MESH)

    own_k = pltpu.make_async_copy(key_weight, W.at[z, y, :, 0:128], loc.at[4])
    own_v = pltpu.make_async_copy(value_weight, W.at[z, y, :, 128:384], loc.at[5])
    own_k.start()
    own_v.start()
    loads = [
        pltpu.make_async_copy(tokens.at[n * GROUP : (n + 1) * GROUP], X.at[n * GROUP : (n + 1) * GROUP], loc.at[n])
        for n in range(4)
    ]
    loads[0].start()
    small = [
        pltpu.make_async_copy(src, dst, loc.at[8 + at])
        for at, (src, dst) in enumerate(
            (
                (gain_in, gain),
                (input_weight, GW.at[0:16]),
                (forget_weight, GW.at[16:32]),
                (offsets_in, offsets),
                (new_rows_in, new_rows),
                (new_query_in, new_query),
            )
        )
    ]
    for copy in small:
        copy.start()
    for load in loads[1:]:
        load.start()
    own_k.wait()
    own_v.wait()
    pl.semaphore_wait(barrier, 34)

    half_z = (z // 4) * 4
    other_z = 4 - half_z
    far_z = (z + 4) % 8

    def shard_to(row, to_z, recv):
        pltpu.make_async_remote_copy(
            src_ref=W.at[row, y],
            dst_ref=W.at[row, y],
            send_sem=ws1,
            recv_sem=recv,
            device_id={"sp": to_z * 4 + y},
            device_id_type=MESH,
        ).start()

    inner = (k_me // 2 + k_me % 2) % 2

    def sent_at(j):
        return inner * (0, 1, 2, 3)[j] + (1 - inner) * ((1 - c) * (0, 3, 2, 1)[j] + c * (0, 2, 3, 1)[j])

    def due_at(j):
        return inner * (0, 2, 1, 3)[j] + (1 - inner) * ((1 - c) * (0, 3, 1, 2)[j] + c * (0, 1, 3, 2)[j])

    def slot(i):
        return xor2(k_me, i)

    def first_leg(i):
        dest = (t - s + i + 32) % 8 + 8 * slot(i)
        src = tokens.at[pl.ds(pl.multiple_of(dest * BLOCK, BLOCK), BLOCK)]
        dst = T.at[pl.ds(pl.multiple_of(s * BLOCK, BLOCK), BLOCK)]
        remote = pltpu.make_async_remote_copy(
            src_ref=src,
            dst_ref=dst,
            send_sem=p1s.at[i],
            recv_sem=p1r.at[i],
            device_id={"sp": dest},
            device_id_type=MESH,
        )
        return dest, src, dst, remote

    def start_leg(j):
        i = sent_at(j)
        dest, src, dst, remote = first_leg(i)

        @pl.when(dest != s)
        def _():
            remote.start()

        @pl.when(dest == s)
        def _():
            pltpu.make_async_copy(src, dst, p1r.at[i]).start()

    start_leg(0)
    shard_to(z, far_z, wc)
    for o in range(1, 4):
        shard_to(z, half_z + (z + o) % 4, wh)


    def y_send(rows, column, to_y, which):
        pltpu.make_async_remote_copy(
            src_ref=W.at[pl.ds(rows, 4), column],
            dst_ref=W.at[pl.ds(rows, 4), column],
            send_sem=ws2,
            recv_sem=wy.at[which],
            device_id={"sp": z * 4 + to_y},
            device_id_type=MESH,
        ).start()

    def arrived(ref, sem):
        pltpu.make_async_copy(ref, ref, sem).wait()

    up, down = (y + 1) % 4, (y + 3) % 4

    def gates(n):
        loads[n].wait()
        norm_group(X, n * GROUP, X, n * GROUP, gain)
        own = X[n * GROUP : (n + 1) * GROUP, :]
        G[n] = lax.dot_general(GW[...], own, NT, preferred_element_type=F32)

    lane = iota((8, 128), 1)
    head_row = iota((8, 128), 0)

    def local_weights():
        gate_row = iota((32, GROUP), 0)
        for n in range(4):
            for h in range(2):
                at = slice(2 * n + h, 2 * n + h + 1)
                mine = jnp.where(gate_row == 2 * t + h, G[n], 0.0)
                IG[at, :] = jnp.sum(mine, axis=0, keepdims=True) + offsets[n, 0, h : h + 1, :]
                mine = jnp.where(gate_row == 16 + 2 * t + h, G[n], 0.0)
                PRE[at, :] = jnp.sum(mine, axis=0, keepdims=True) + bias[h]
                LF[at, :] = offsets[n, 1, h : h + 1, :]

        wide_lane = iota((8, GROUP), 1)
        pre = PRE[...]
        soft = jnp.minimum(pre, 0.0) - jnp.log1p(jnp.exp(-jnp.abs(pre)))
        log_forget = soft + LF[...]
        suffix = log_forget
        step = 1
        while step < GROUP:
            suffix = suffix + jnp.where(wide_lane < GROUP - step, pltpu.roll(suffix, GROUP - step, 1), 0.0)
            step *= 2
        exclusive = jnp.where(wide_lane < GROUP - 1, pltpu.roll(suffix, GROUP - 1, 1), 0.0)
        local = IG[...] + exclusive
        LOC[...] = local
        total = suffix[:, 0:1]
        most = jnp.max(local, axis=1, keepdims=True)
        tail_part = jnp.where(lane - 64 == head_row, total, jnp.where(lane - 72 == head_row, most, 0.0))
        tail_part = jnp.broadcast_to(jnp.sum(tail_part, axis=0, keepdims=True), (8, 128))
        for half in range(2):
            part = local[:, half * 128 : (half + 1) * 128]
            for k in range(4):
                first = pltpu.roll(part, (128 - 32 * k) % 128, 1) if k else part
                second = pltpu.roll(pltpu.roll(part, 7, 0), (160 - 32 * k) % 128, 1) if k != 1 else pltpu.roll(part, 7, 0)
                row = jnp.where(lane < 32, first, jnp.where(lane < 64, second, tail_part))
                for n in range(4):
                    S[n * 8 + half * 4 + k] = row[2 * n : 2 * n + 1, :]
        R[pl.ds(s, 1)] = S[pl.ds(s, 1)]

        def send_rows(o, carry):
            peer = (s + o) % 32
            pltpu.make_async_remote_copy(
                src_ref=S.at[peer],
                dst_ref=R.at[s],
                send_sem=lws,
                recv_sem=lwr,
                device_id={"sp": peer},
                device_id_type=MESH,
            ).start()
            return carry

        lax.fori_loop(1, 32, send_rows, 0)

    def block_of(owner, i):
        at = ((owner - s + i + 32) % 8 + 8 * slot(i)) * BLOCK
        return T.at[pl.ds(pl.multiple_of(at, BLOCK), BLOCK)]

    def pass_on(owner, i, to, recv):
        block = block_of(owner, i)
        pltpu.make_async_remote_copy(
            src_ref=block,
            dst_ref=block,
            send_sem=xs,
            recv_sem=recv,
            device_id={"tp": to},
            device_id_type=MESH,
        ).start()

    half_block = BLOCK // 2

    def pass_half(owner, i, half, to, recv):
        at = ((owner - s + i + 32) % 8 + 8 * slot(i)) * BLOCK + half * half_block
        part = T.at[pl.ds(pl.multiple_of(at, half_block), half_block)]
        pltpu.make_async_remote_copy(
            src_ref=part,
            dst_ref=part,
            send_sem=xs,
            recv_sem=recv,
            device_id={"tp": to},
            device_id_type=MESH,
        ).start()

    one_block = T.at[0:BLOCK]

    half_rows = T.at[0:half_block]

    def stage_a(j):
        i = due_at(j)
        arrived(one_block, p1r.at[i])
        for half in range(2):
            pass_half(t, i, half, right, xl.at[i, half])
            pass_half(t, i, 1 - half, left, xr.at[i, 1 - half])
        pass_on(t, i, mate, dr.at[i])

    def stage_b(j):
        i = due_at(j)
        arrived(half_rows, xl.at[i, 0])
        pass_half(left, i, 0, right, xf.at[i, 0])
        arrived(half_rows, xr.at[i, 1])
        pass_half(right, i, 1, left, xf.at[i, 1])
        arrived(half_rows, xl.at[i, 1])
        pass_on(left, i, mate, dr.at[i])
        arrived(half_rows, xr.at[i, 0])
        pass_on(right, i, mate, dr.at[i])

    def stage_c(j):
        i = due_at(j)
        arrived(half_rows, xf.at[i, 0])
        arrived(half_rows, xf.at[i, 1])
        pass_on(across, i, mate, dr.at[i])

    def write_out(i):
        at = pl.ds(pl.multiple_of(slot(i) * GROUP, GROUP), GROUP)
        return (
            pltpu.make_async_copy(OK.at[at], out_keys.at[at], loc.at[6]),
            pltpu.make_async_copy(OV.at[at], out_values.at[at], loc.at[7]),
        )

    def stage_n(j):
        i = due_at(j)
        arrived(T.at[0 : 4 * BLOCK], dr.at[i])
        start = pl.multiple_of(slot(i) * GROUP, GROUP)
        norm_group(T, start, N, j * GROUP, gain)

    def stage_d(j, groups=1):
        keys, values = project(N[j * GROUP : (j + groups) * GROUP, :])
        for g in range(groups):
            i = due_at(j + g)
            start = pl.multiple_of(slot(i) * GROUP, GROUP)
            OK[pl.ds(start, GROUP), :] = keys[g * GROUP : (g + 1) * GROUP]
            OV[pl.ds(start, GROUP), :] = values[g * GROUP : (g + 1) * GROUP]
            for copy in write_out(i):
                copy.start()

    def column(row, first):
        return jnp.sum(jnp.where(lane - first == head_row, row, 0.0), axis=1, keepdims=True)

    def log_weights():
        arrived(R.at[0:31], lwr)
        received = R[:, 0, :]
        row = iota((32, 128), 0)
        lane32 = iota((32, 128), 1)
        suffix = received
        step = 1
        while step < 32:
            suffix = suffix + jnp.where(row < 32 - step, pltpu.roll(suffix, 32 - step, 0), 0.0)
            step *= 2
        exclusive = jnp.where(row < 31, pltpu.roll(suffix, 31, 0), 0.0)
        peaks = jnp.max(received + pltpu.roll(exclusive, 8, 1), axis=0, keepdims=True)
        PEAK[...] = jnp.broadcast_to(column(peaks, 72), (8, 128))
        mine = jnp.sum(jnp.where(row == s, exclusive, 0.0), axis=0, keepdims=True)
        LOC[...] += column(mine, 64)
        tails = [
            jnp.sum(jnp.where(lane32 == 64 + 2 * n_me + h, exclusive, 0.0), axis=1, keepdims=True)
            for h in range(2)
        ]
        L[...] = received + jnp.where(lane32 < 32, tails[0], tails[1])
        for h in range(2):
            wide = jnp.zeros((8, 128), F32)
            for k in range(4):
                rows = L[pl.ds(k, 8, stride=4), :]
                shift = (32 * k - 32 * h) % 128
                moved = pltpu.roll(rows, shift, 1) if shift else rows
                wide = jnp.where((lane >= 32 * k) & (lane < 32 * k + 32), moved, wide)
            for g in range(8):
                LW[h : h + 1, g * 128 : (g + 1) * 128] = wide[g : g + 1, :]
        out_weights[...] = LW[...]

        query = new_query[...].astype(F32)
        for n in range(4):
            Q8[2 * n : 2 * n + 1, :] = jnp.where(lane1 < 64, query[n : n + 1, :], 0.0)
            Q8[2 * n + 1 : 2 * n + 2, :] = jnp.where(lane1 < 64, 0.0, query[n : n + 1, :])
        NUM[...] = jnp.zeros_like(NUM)
        DEN[...] = jnp.zeros_like(DEN)

    def project(rows):
        both = jnp.dot(rows, W[...].reshape(D, 384), preferred_element_type=F32)
        return (both[:, 0:128] * 0.125).astype(BF16), both[:, 128:384].astype(BF16)

    def own_read(n):
        keys, values = project(X[n * GROUP : (n + 2) * GROUP, :])
        scores = lax.dot_general(Q8[...].astype(BF16), keys, NT, preferred_element_type=F32)
        weight = jnp.exp(LOC[...] - PEAK[:, 0:1])
        terms = jnp.concatenate([weight, weight], axis=1) * scores
        prompt = n + iota((8, 2 * GROUP), 1) // GROUP
        terms = jnp.where(iota((8, 2 * GROUP), 0) // 2 == prompt, terms, 0.0)
        DEN[...] += jnp.broadcast_to(jnp.sum(terms, axis=1, keepdims=True), (8, 128))
        NUM[...] += jnp.dot(terms.astype(BF16), values, preferred_element_type=F32)

    def share(buffer, slot_of, peers, send, recv):
        for to in peers:
            pltpu.make_async_remote_copy(
                src_ref=buffer.at[slot_of],
                dst_ref=buffer.at[slot_of],
                send_sem=send,
                recv_sem=recv,
                device_id={"sp": to},
                device_id_type=MESH,
            ).start()

    def sum_y():
        value = jnp.where(head_row % 2 == 0, NUM[:, 0:128], NUM[:, 128:256])
        E1[pl.ds(y, 1)] = jnp.concatenate([value, DEN[...]], axis=0).reshape(1, 16, 128)
        share(E1, y, [z * 4 + (y + o) % 4 for o in range(1, 4)], es.at[0], er.at[0])

    def sum_z():
        arrived(E1.at[0:3], er.at[0])
        E2[pl.ds(z, 1)] = ((E1[0] + E1[1]) + (E1[2] + E1[3])).reshape(1, 16, 128)
        share(E2, z, [((z + o) % 8) * 4 + y for o in range(1, 8)], es.at[1], er.at[1])

    def finish():
        arrived(E2.at[0:7], er.at[1])
        total = jnp.sum(E2[...], axis=0)
        numerator, denominator = total[0:8], total[8:16, 0:1]
        peak = PEAK[:, 0:1]
        gate = jnp.sum(
            jnp.where(iota((8, 32), 1) == 2 * t + iota((8, 32), 0) % 2, GN8[...], 0.0), axis=1, keepdims=True
        )
        own = jnp.sum(Q8[...] * (KN8[...] * 0.125).astype(BF16).astype(F32), axis=1, keepdims=True)
        top = jnp.maximum(peak, gate)
        old_part = jnp.exp(peak - top)
        new_part = jnp.exp(gate - top) * own
        value = old_part * numerator + new_part * VN8[...].astype(BF16).astype(F32)
        weight = old_part * denominator + new_part
        read = value / jnp.maximum(jnp.abs(weight), 1.0)
        for n in range(4):
            for h in range(2):
                A0[n : n + 1, h * 128 : (h + 1) * 128] = read[2 * n + h : 2 * n + h + 1, :]
        out_read[...] = A0[...].astype(BF16)

    lane1 = iota((1, 128), 1)

    def new_row_parts():
        total = jnp.zeros((4, 128), F32)
        for g in range(D // 128):
            v = new_rows[:, g * 128 : (g + 1) * 128].astype(F32)
            total = total + v * v
        inverse = lax.rsqrt(jnp.sum(total, axis=-1, keepdims=True) * (1.0 / D) + EPSILON)
        NN[...] = jnp.zeros_like(NN)
        for g in range(D // 128):
            at = slice(g * 128, (g + 1) * 128)
            NN[0:4, at] = new_rows[:, at].astype(F32) * inverse * gain[g : g + 1, :].astype(F32)
        fresh = NN[...].astype(BF16)
        both = jnp.dot(fresh, W[...].reshape(D, 384), preferred_element_type=F32)
        gates_new = lax.dot_general(fresh, GW[...], NT, preferred_element_type=F32)
        for n in range(4):
            for h in range(2):
                at = slice(2 * n + h, 2 * n + h + 1)
                KN8[at, :] = both[n : n + 1, 0:128]
                VN8[at, :] = both[n : n + 1, 128 * (h + 1) : 128 * (h + 2)]
                GN8[at, :] = gates_new[n : n + 1, :]

    for copy in small:
        copy.wait()
    for n in range(4):
        gates(n)
    local_weights()
    arrived(W.at[0, 0], wc)
    for o in range(1, 4):
        shard_to(far_z, half_z + (z + o) % 4, w2)
    start_leg(1)

    @pl.when(inner == 0)
    def _():
        start_leg(2)

    arrived(W.at[0:3, 0], wh)
    y_send(half_z, y, up, 0)
    y_send(half_z, y, down, 1)
    arrived(W.at[0:4, 0], wy.at[0])
    y_send(half_z, down, up, 2)

    @pl.when(inner == 1)
    def _():
        start_leg(2)

    @pl.when(inner == 0)
    def _():
        start_leg(3)

    stage_a(0)
    arrived(W.at[0:3, 0], w2)
    y_send(other_z, y, up, 3)
    y_send(other_z, y, down, 4)

    @pl.when(inner == 1)
    def _():
        start_leg(3)

    stage_b(0)
    stage_a(1)
    stage_c(0)
    arrived(W.at[0:4, 0], wy.at[4])
    y_send(other_z, up, down, 5)
    stage_a(2)
    stage_b(1)
    stage_n(0)
    log_weights()
    stage_b(2)
    stage_a(3)
    for which in (1, 2, 3, 5):
        arrived(W.at[0:4, 0], wy.at[which])
    own_read(0)
    own_read(2)
    sum_y()
    stage_c(1)
    stage_b(3)
    stage_c(2)
    stage_n(1)
    sum_z()
    stage_c(3)
    stage_d(0, 2)
    stage_n(2)
    stage_d(2)
    stage_n(3)
    stage_d(3)
    new_row_parts()
    finish()
    arrived(OK, loc.at[6])
    arrived(OV, loc.at[7])

    arrived(R.at[0:31], lws)
    arrived(E1.at[0:3], es.at[0])
    arrived(E2.at[0:7], es.at[1])
    arrived(W.at[0:7, 0], ws1)
    arrived(W.at[0:6], ws2)
    arrived(T.at[0 : 28 * BLOCK], xs)

    def leg_done(i):
        dest, _, _, remote = first_leg(i)

        @pl.when(dest != s)
        def _():
            remote.wait_send()

    for i in range(4):
        leg_done(i)


def place(keys, values, weights, read, out_keys, out_values, out_weights, out_read, sems):
    copies = [
        pltpu.make_async_copy(keys, out_keys.at[0], sems.at[0]),
        pltpu.make_async_copy(values, out_values.at[0], sems.at[1]),
        pltpu.make_async_copy(weights, out_weights.at[0], sems.at[2]),
        pltpu.make_async_copy(read, out_read, sems.at[3]),
    ]
    for copy in copies:
        copy.start()
    for copy in copies:
        copy.wait()


def per_device(
    tokens,
    new_rows,
    new_query,
    norm_gain,
    key_weight,
    value_weight,
    input_weight,
    forget_weight,
    forget_bias,
    gate_offsets,
):
    any_space = pl.BlockSpec(memory_space=pl.ANY)
    vmem = pl.BlockSpec(memory_space=pltpu.VMEM)
    smem = pl.BlockSpec(memory_space=pltpu.SMEM)
    dma = pltpu.SemaphoreType.DMA
    keys, values, weights, read = pl.pallas_call(
        kernel,
        out_shape=(
            jax.ShapeDtypeStruct((ROWS, 128), BF16),
            jax.ShapeDtypeStruct((ROWS, 256), BF16),
            jax.ShapeDtypeStruct((2, ROWS), F32),
            jax.ShapeDtypeStruct((4, 256), BF16),
        ),
        in_specs=[any_space] * 8 + [smem, any_space],
        out_specs=(any_space, any_space, vmem, vmem),
        scratch_shapes=[
            pltpu.VMEM((4, D), BF16),
            pltpu.VMEM((4, 128), BF16),
            pltpu.VMEM((16, 128), BF16),
            pltpu.VMEM((4, 2, 2, GROUP), F32),
            pltpu.VMEM((ROWS, D), BF16),
            pltpu.VMEM((ROWS, D), BF16),
            pltpu.VMEM((ROWS, D), BF16),
            pltpu.VMEM((8, 4, 64, 384), BF16),
            pltpu.VMEM((ROWS, 128), BF16),
            pltpu.VMEM((ROWS, 256), BF16),
            pltpu.VMEM((4, 32, GROUP), F32),
            pltpu.VMEM((32, D), BF16),
            pltpu.VMEM((8, D), F32),
            pltpu.VMEM((8, GROUP), F32),
            pltpu.VMEM((8, GROUP), F32),
            pltpu.VMEM((8, GROUP), F32),
            pltpu.VMEM((8, GROUP), F32),
            pltpu.VMEM((32, 1, 128), F32),
            pltpu.VMEM((32, 1, 128), F32),
            pltpu.VMEM((32, 128), F32),
            pltpu.VMEM((2, ROWS), F32),
            pltpu.VMEM((8, 128), F32),
            pltpu.VMEM((8, 128), F32),
            pltpu.VMEM((8, 256), F32),
            pltpu.VMEM((8, 128), F32),
            pltpu.VMEM((8, 128), F32),
            pltpu.VMEM((8, 128), F32),
            pltpu.VMEM((8, 32), F32),
            pltpu.VMEM((4, 16, 128), F32),
            pltpu.VMEM((8, 16, 128), F32),
            pltpu.VMEM((4, 256), F32),
            dma((4,)),
            dma((4,)),
            dma((4, 2)),
            dma((4, 2)),
            dma((4, 2)),
            dma((4,)),
            dma,
            dma,
            dma,
            dma,
            dma,
            dma,
            dma((6,)),
            dma,
            dma,
            dma((2,)),
            dma((2,)),
            dma((14,)),
        ],
        compiler_params=pltpu.CompilerParams(collective_id=0, has_side_effects=True),
    )(
        tokens.reshape(ROWS, D),
        new_rows,
        new_query,
        norm_gain.reshape(16, 128),
        key_weight,
        value_weight,
        input_weight.T,
        forget_weight.T,
        forget_bias,
        jnp.transpose(gate_offsets, (0, 2, 3, 1)),
    )
    return pl.pallas_call(
        place,
        out_shape=(
            jax.ShapeDtypeStruct((1, ROWS, 128), BF16),
            jax.ShapeDtypeStruct((1, ROWS, 256), BF16),
            jax.ShapeDtypeStruct((1, 2, ROWS), F32),
            jax.ShapeDtypeStruct((4, 256), BF16),
        ),
        in_specs=[vmem] * 4,
        out_specs=[any_space] * 4,
        scratch_shapes=[dma((4,))],
    )(keys, values, weights, read)


def solution(mesh):
    return jax.shard_map(
        per_device,
        mesh=mesh,
        in_specs=(
            P("gr", "sp", None),
            P("gr", None),
            P("gr", "tp"),
            P(),
            P("sp", "tp"),
            P("sp", "tp"),
            P(),
            P(),
            P("tp"),
            P("gr", "sp", None, "tp"),
        ),
        out_specs=(
            P(("gr", "sp"), None, "tp"),
            P(("gr", "sp"), None, "tp"),
            P(("gr", "sp"), "tp", None),
            P("gr", "tp"),
        ),
        check_vma=False,
    )
```

```python
import jax
import jax.numpy as jnp
from jax import lax
from jax.experimental import pallas as pl
from jax.experimental.pallas import tpu as pltpu
from jax.sharding import PartitionSpec as P

EPSILON = 1e-06
MESH = pl.DeviceIdType.MESH
F32 = jnp.float32
BF16 = jnp.bfloat16
NT = (((1,), (1,)), ((), ()))

D = 2048
ROWS = 1024
GROUP = 256
BLOCK = 32
CHUNK = 64


def iota(shape, dim):
    return lax.broadcasted_iota(jnp.int32, shape, dim)


def xor2(a, b):
    return 2 * ((a // 2 + b // 2) % 2) + (a % 2 + b % 2) % 2


def norm_chunk(read, write, gain_ref, rows):
    total = jnp.zeros((rows, 128), F32)
    for c in range(D // 128):
        v = read(c).astype(F32)
        total = total + v * v
    inverse = lax.rsqrt(jnp.sum(total, axis=-1, keepdims=True) * (1.0 / D) + EPSILON)
    for c in range(D // 128):
        v = read(c).astype(F32)
        write(c, (v * inverse * gain_ref[c : c + 1, :].astype(F32)).astype(BF16))


def norm_group(src, start, dst, first, gain_ref):
    def body(u, carry):
        at = pl.multiple_of(start + u * CHUNK, CHUNK)
        to = pl.multiple_of(first + u * CHUNK, CHUNK)

        def read(c):
            return src[pl.ds(at, CHUNK), c * 128 : (c + 1) * 128]

        def write(c, v):
            dst[pl.ds(to, CHUNK), c * 128 : (c + 1) * 128] = v

        norm_chunk(read, write, gain_ref, CHUNK)
        return carry

    lax.fori_loop(0, GROUP // CHUNK, body, 0)


def kernel(
    tokens,
    new_rows_in,
    new_query_in,
    gain_in,
    key_weight,
    value_weight,
    input_weight,
    forget_weight,
    bias,
    offsets_in,
    out_keys,
    out_values,
    out_weights,
    out_read,
    new_rows,
    new_query,
    gain,
    offsets,
    T,
    X,
    N,
    W,
    OK,
    OV,
    G,
    GW,
    NN,
    IG,
    PRE,
    LF,
    LOC,
    S,
    R,
    L,
    LW,
    PEAK,
    Q8,
    NUM,
    DEN,
    KN8,
    VN8,
    GN8,
    E1,
    E2,
    A0,
    p1s,
    p1r,
    xl,
    xr,
    xf,
    dr,
    xs,
    lws,
    lwr,
    wc,
    wh,
    w2,
    wy,
    ws1,
    ws2,
    es,
    er,
    loc,
):
    s = lax.axis_index("sp")
    t = lax.axis_index("tp")
    z, y = s // 4, s % 4
    x, c = t // 2, t % 2
    k_me = s // 8
    n_me = s // 8
    right = ((x + 1) % 4) * 2 + c
    left = ((x + 3) % 4) * 2 + c
    across = ((x + 2) % 4) * 2 + c
    mate = t + 1 - 2 * c

    barrier = pltpu.get_barrier_semaphore()

    def greet(o, carry):
        pl.semaphore_signal(barrier, inc=1, device_id={"sp": (s + o) % 32}, device_id_type=MESH)
        return carry

    lax.fori_loop(1, 32, greet, 0)
    for who in (right, left, mate):
        pl.semaphore_signal(barrier, inc=1, device_id={"tp": who}, device_id_type=MESH)

    own_k = pltpu.make_async_copy(key_weight, W.at[z, y, :, 0:128], loc.at[4])
    own_v = pltpu.make_async_copy(value_weight, W.at[z, y, :, 128:384], loc.at[5])
    own_k.start()
    own_v.start()
    loads = [
        pltpu.make_async_copy(tokens.at[n * GROUP : (n + 1) * GROUP], X.at[n * GROUP : (n + 1) * GROUP], loc.at[n])
        for n in range(4)
    ]
    loads[0].start()
    small = [
        pltpu.make_async_copy(src, dst, loc.at[8 + at])
        for at, (src, dst) in enumerate(
            (
                (gain_in, gain),
                (input_weight, GW.at[0:16]),
                (forget_weight, GW.at[16:32]),
                (offsets_in, offsets),
                (new_rows_in, new_rows),
                (new_query_in, new_query),
            )
        )
    ]
    for copy in small:
        copy.start()
    for load in loads[1:]:
        load.start()
    own_k.wait()
    own_v.wait()
    pl.semaphore_wait(barrier, 34)

    half_z = (z // 4) * 4
    other_z = 4 - half_z
    far_z = (z + 4) % 8

    def shard_to(row, to_z, recv):
        pltpu.make_async_remote_copy(
            src_ref=W.at[row, y],
            dst_ref=W.at[row, y],
            send_sem=ws1,
            recv_sem=recv,
            device_id={"sp": to_z * 4 + y},
            device_id_type=MESH,
        ).start()

    inner = (k_me // 2 + k_me % 2) % 2

    def sent_at(j):
        return inner * (0, 1, 2, 3)[j] + (1 - inner) * ((1 - c) * (0, 3, 2, 1)[j] + c * (0, 2, 3, 1)[j])

    def due_at(j):
        return inner * (0, 2, 1, 3)[j] + (1 - inner) * ((1 - c) * (0, 3, 1, 2)[j] + c * (0, 1, 3, 2)[j])

    def slot(i):
        return xor2(k_me, i)

    def first_leg(i):
        dest = (t - s + i + 32) % 8 + 8 * slot(i)
        src = tokens.at[pl.ds(pl.multiple_of(dest * BLOCK, BLOCK), BLOCK)]
        dst = T.at[pl.ds(pl.multiple_of(s * BLOCK, BLOCK), BLOCK)]
        remote = pltpu.make_async_remote_copy(
            src_ref=src,
            dst_ref=dst,
            send_sem=p1s.at[i],
            recv_sem=p1r.at[i],
            device_id={"sp": dest},
            device_id_type=MESH,
        )
        return dest, src, dst, remote

    def start_leg(j):
        i = sent_at(j)
        dest, src, dst, remote = first_leg(i)

        @pl.when(dest != s)
        def _():
            remote.start()

        @pl.when(dest == s)
        def _():
            pltpu.make_async_copy(src, dst, p1r.at[i]).start()

    start_leg(0)
    shard_to(z, far_z, wc)
    for o in range(1, 4):
        shard_to(z, half_z + (z + o) % 4, wh)


    def y_send(rows, column, to_y, which):
        pltpu.make_async_remote_copy(
            src_ref=W.at[pl.ds(rows, 4), column],
            dst_ref=W.at[pl.ds(rows, 4), column],
            send_sem=ws2,
            recv_sem=wy.at[which],
            device_id={"sp": z * 4 + to_y},
            device_id_type=MESH,
        ).start()

    def arrived(ref, sem):
        pltpu.make_async_copy(ref, ref, sem).wait()

    up, down = (y + 1) % 4, (y + 3) % 4

    def gates(n):
        loads[n].wait()
        norm_group(X, n * GROUP, X, n * GROUP, gain)
        own = X[n * GROUP : (n + 1) * GROUP, :]
        G[n] = lax.dot_general(GW[...], own, NT, preferred_element_type=F32)

    lane = iota((8, 128), 1)
    head_row = iota((8, 128), 0)

    def local_weights():
        gate_row = iota((32, GROUP), 0)
        for n in range(4):
            for h in range(2):
                at = slice(2 * n + h, 2 * n + h + 1)
                mine = jnp.where(gate_row == 2 * t + h, G[n], 0.0)
                IG[at, :] = jnp.sum(mine, axis=0, keepdims=True) + offsets[n, 0, h : h + 1, :]
                mine = jnp.where(gate_row == 16 + 2 * t + h, G[n], 0.0)
                PRE[at, :] = jnp.sum(mine, axis=0, keepdims=True) + bias[h]
                LF[at, :] = offsets[n, 1, h : h + 1, :]

        wide_lane = iota((8, GROUP), 1)
        pre = PRE[...]
        soft = jnp.minimum(pre, 0.0) - jnp.log1p(jnp.exp(-jnp.abs(pre)))
        log_forget = soft + LF[...]
        suffix = log_forget
        step = 1
        while step < GROUP:
            suffix = suffix + jnp.where(wide_lane < GROUP - step, pltpu.roll(suffix, GROUP - step, 1), 0.0)
            step *= 2
        exclusive = jnp.where(wide_lane < GROUP - 1, pltpu.roll(suffix, GROUP - 1, 1), 0.0)
        local = IG[...] + exclusive
        LOC[...] = local
        total = suffix[:, 0:1]
        most = jnp.max(local, axis=1, keepdims=True)
        tail_part = jnp.where(lane - 64 == head_row, total, jnp.where(lane - 72 == head_row, most, 0.0))
        tail_part = jnp.broadcast_to(jnp.sum(tail_part, axis=0, keepdims=True), (8, 128))
        for half in range(2):
            part = local[:, half * 128 : (half + 1) * 128]
            for k in range(4):
                first = pltpu.roll(part, (128 - 32 * k) % 128, 1) if k else part
                second = pltpu.roll(pltpu.roll(part, 7, 0), (160 - 32 * k) % 128, 1) if k != 1 else pltpu.roll(part, 7, 0)
                row = jnp.where(lane < 32, first, jnp.where(lane < 64, second, tail_part))
                for n in range(4):
                    S[n * 8 + half * 4 + k] = row[2 * n : 2 * n + 1, :]
        R[pl.ds(s, 1)] = S[pl.ds(s, 1)]

        def send_rows(o, carry):
            peer = (s + o) % 32
            pltpu.make_async_remote_copy(
                src_ref=S.at[peer],
                dst_ref=R.at[s],
                send_sem=lws,
                recv_sem=lwr,
                device_id={"sp": peer},
                device_id_type=MESH,
            ).start()
            return carry

        lax.fori_loop(1, 32, send_rows, 0)

    def block_of(owner, i):
        at = ((owner - s + i + 32) % 8 + 8 * slot(i)) * BLOCK
        return T.at[pl.ds(pl.multiple_of(at, BLOCK), BLOCK)]

    def pass_on(owner, i, to, recv):
        block = block_of(owner, i)
        pltpu.make_async_remote_copy(
            src_ref=block,
            dst_ref=block,
            send_sem=xs,
            recv_sem=recv,
            device_id={"tp": to},
            device_id_type=MESH,
        ).start()

    half_block = BLOCK // 2

    def pass_half(owner, i, half, to, recv):
        at = ((owner - s + i + 32) % 8 + 8 * slot(i)) * BLOCK + half * half_block
        part = T.at[pl.ds(pl.multiple_of(at, half_block), half_block)]
        pltpu.make_async_remote_copy(
            src_ref=part,
            dst_ref=part,
            send_sem=xs,
            recv_sem=recv,
            device_id={"tp": to},
            device_id_type=MESH,
        ).start()

    one_block = T.at[0:BLOCK]

    half_rows = T.at[0:half_block]

    def stage_a(j):
        i = due_at(j)
        arrived(one_block, p1r.at[i])
        for half in range(2):
            pass_half(t, i, half, right, xl.at[i, half])
            pass_half(t, i, 1 - half, left, xr.at[i, 1 - half])
        pass_on(t, i, mate, dr.at[i])

    def stage_b(j):
        i = due_at(j)
        arrived(half_rows, xl.at[i, 0])
        pass_half(left, i, 0, right, xf.at[i, 0])
        arrived(half_rows, xr.at[i, 1])
        pass_half(right, i, 1, left, xf.at[i, 1])
        arrived(half_rows, xl.at[i, 1])
        pass_on(left, i, mate, dr.at[i])
        arrived(half_rows, xr.at[i, 0])
        pass_on(right, i, mate, dr.at[i])

    def stage_c(j):
        i = due_at(j)
        arrived(half_rows, xf.at[i, 0])
        arrived(half_rows, xf.at[i, 1])
        pass_on(across, i, mate, dr.at[i])

    def write_out(i):
        at = pl.ds(pl.multiple_of(slot(i) * GROUP, GROUP), GROUP)
        return (
            pltpu.make_async_copy(OK.at[at], out_keys.at[at], loc.at[6]),
            pltpu.make_async_copy(OV.at[at], out_values.at[at], loc.at[7]),
        )

    def stage_n(j):
        i = due_at(j)
        arrived(T.at[0 : 4 * BLOCK], dr.at[i])
        start = pl.multiple_of(slot(i) * GROUP, GROUP)
        norm_group(T, start, N, j * GROUP, gain)

    def stage_d(j, groups=1):
        keys, values = project(N[j * GROUP : (j + groups) * GROUP, :])
        for g in range(groups):
            i = due_at(j + g)
            start = pl.multiple_of(slot(i) * GROUP, GROUP)
            OK[pl.ds(start, GROUP), :] = keys[g * GROUP : (g + 1) * GROUP]
            OV[pl.ds(start, GROUP), :] = values[g * GROUP : (g + 1) * GROUP]
            for copy in write_out(i):
                copy.start()

    def column(row, first):
        return jnp.sum(jnp.where(lane - first == head_row, row, 0.0), axis=1, keepdims=True)

    def log_weights():
        arrived(R.at[0:31], lwr)
        received = R[:, 0, :]
        row = iota((32, 128), 0)
        lane32 = iota((32, 128), 1)
        suffix = received
        step = 1
        while step < 32:
            suffix = suffix + jnp.where(row < 32 - step, pltpu.roll(suffix, 32 - step, 0), 0.0)
            step *= 2
        exclusive = jnp.where(row < 31, pltpu.roll(suffix, 31, 0), 0.0)
        peaks = jnp.max(received + pltpu.roll(exclusive, 8, 1), axis=0, keepdims=True)
        PEAK[...] = jnp.broadcast_to(column(peaks, 72), (8, 128))
        mine = jnp.sum(jnp.where(row == s, exclusive, 0.0), axis=0, keepdims=True)
        LOC[...] += column(mine, 64)
        tails = [
            jnp.sum(jnp.where(lane32 == 64 + 2 * n_me + h, exclusive, 0.0), axis=1, keepdims=True)
            for h in range(2)
        ]
        L[...] = received + jnp.where(lane32 < 32, tails[0], tails[1])
        for h in range(2):
            wide = jnp.zeros((8, 128), F32)
            for k in range(4):
                rows = L[pl.ds(k, 8, stride=4), :]
                shift = (32 * k - 32 * h) % 128
                moved = pltpu.roll(rows, shift, 1) if shift else rows
                wide = jnp.where((lane >= 32 * k) & (lane < 32 * k + 32), moved, wide)
            for g in range(8):
                LW[h : h + 1, g * 128 : (g + 1) * 128] = wide[g : g + 1, :]
        out_weights[...] = LW[...]

        query = new_query[...].astype(F32)
        for n in range(4):
            Q8[2 * n : 2 * n + 1, :] = jnp.where(lane1 < 64, query[n : n + 1, :], 0.0)
            Q8[2 * n + 1 : 2 * n + 2, :] = jnp.where(lane1 < 64, 0.0, query[n : n + 1, :])
        NUM[...] = jnp.zeros_like(NUM)
        DEN[...] = jnp.zeros_like(DEN)

    def project(rows):
        both = jnp.dot(rows, W[...].reshape(D, 384), preferred_element_type=F32)
        return (both[:, 0:128] * 0.125).astype(BF16), both[:, 128:384].astype(BF16)

    def own_read(n):
        keys, values = project(X[n * GROUP : (n + 2) * GROUP, :])
        scores = lax.dot_general(Q8[...].astype(BF16), keys, NT, preferred_element_type=F32)
        weight = jnp.exp(LOC[...] - PEAK[:, 0:1])
        terms = jnp.concatenate([weight, weight], axis=1) * scores
        prompt = n + iota((8, 2 * GROUP), 1) // GROUP
        terms = jnp.where(iota((8, 2 * GROUP), 0) // 2 == prompt, terms, 0.0)
        DEN[...] += jnp.broadcast_to(jnp.sum(terms, axis=1, keepdims=True), (8, 128))
        NUM[...] += jnp.dot(terms.astype(BF16), values, preferred_element_type=F32)

    def share(buffer, slot_of, peers, send, recv):
        for to in peers:
            pltpu.make_async_remote_copy(
                src_ref=buffer.at[slot_of],
                dst_ref=buffer.at[slot_of],
                send_sem=send,
                recv_sem=recv,
                device_id={"sp": to},
                device_id_type=MESH,
            ).start()

    def sum_y():
        value = jnp.where(head_row % 2 == 0, NUM[:, 0:128], NUM[:, 128:256])
        E1[pl.ds(y, 1)] = jnp.concatenate([value, DEN[...]], axis=0).reshape(1, 16, 128)
        share(E1, y, [z * 4 + (y + o) % 4 for o in range(1, 4)], es.at[0], er.at[0])

    def sum_z():
        arrived(E1.at[0:3], er.at[0])
        E2[pl.ds(z, 1)] = ((E1[0] + E1[1]) + (E1[2] + E1[3])).reshape(1, 16, 128)
        share(E2, z, [((z + o) % 8) * 4 + y for o in range(1, 8)], es.at[1], er.at[1])

    def finish():
        arrived(E2.at[0:7], er.at[1])
        total = jnp.sum(E2[...], axis=0)
        numerator, denominator = total[0:8], total[8:16, 0:1]
        peak = PEAK[:, 0:1]
        gate = jnp.sum(
            jnp.where(iota((8, 32), 1) == 2 * t + iota((8, 32), 0) % 2, GN8[...], 0.0), axis=1, keepdims=True
        )
        own = jnp.sum(Q8[...] * (KN8[...] * 0.125).astype(BF16).astype(F32), axis=1, keepdims=True)
        top = jnp.maximum(peak, gate)
        old_part = jnp.exp(peak - top)
        new_part = jnp.exp(gate - top) * own
        value = old_part * numerator + new_part * VN8[...].astype(BF16).astype(F32)
        weight = old_part * denominator + new_part
        read = value / jnp.maximum(jnp.abs(weight), 1.0)
        for n in range(4):
            for h in range(2):
                A0[n : n + 1, h * 128 : (h + 1) * 128] = read[2 * n + h : 2 * n + h + 1, :]
        out_read[...] = A0[...].astype(BF16)

    lane1 = iota((1, 128), 1)

    def new_row_parts():
        total = jnp.zeros((4, 128), F32)
        for g in range(D // 128):
            v = new_rows[:, g * 128 : (g + 1) * 128].astype(F32)
            total = total + v * v
        inverse = lax.rsqrt(jnp.sum(total, axis=-1, keepdims=True) * (1.0 / D) + EPSILON)
        NN[...] = jnp.zeros_like(NN)
        for g in range(D // 128):
            at = slice(g * 128, (g + 1) * 128)
            NN[0:4, at] = new_rows[:, at].astype(F32) * inverse * gain[g : g + 1, :].astype(F32)
        fresh = NN[...].astype(BF16)
        both = jnp.dot(fresh, W[...].reshape(D, 384), preferred_element_type=F32)
        gates_new = lax.dot_general(fresh, GW[...], NT, preferred_element_type=F32)
        for n in range(4):
            for h in range(2):
                at = slice(2 * n + h, 2 * n + h + 1)
                KN8[at, :] = both[n : n + 1, 0:128]
                VN8[at, :] = both[n : n + 1, 128 * (h + 1) : 128 * (h + 2)]
                GN8[at, :] = gates_new[n : n + 1, :]

    for copy in small:
        copy.wait()
    for n in range(4):
        gates(n)
    local_weights()
    arrived(W.at[0, 0], wc)
    for o in range(1, 4):
        shard_to(far_z, half_z + (z + o) % 4, w2)
    start_leg(1)

    @pl.when(inner == 0)
    def _():
        start_leg(2)

    arrived(W.at[0:3, 0], wh)
    y_send(half_z, y, up, 0)
    y_send(half_z, y, down, 1)
    arrived(W.at[0:4, 0], wy.at[0])
    y_send(half_z, down, up, 2)

    @pl.when(inner == 1)
    def _():
        start_leg(2)

    start_leg(3)
    stage_a(0)
    arrived(W.at[0:3, 0], w2)
    y_send(other_z, y, up, 3)
    y_send(other_z, y, down, 4)
    stage_b(0)
    stage_a(1)
    stage_c(0)
    arrived(W.at[0:4, 0], wy.at[4])
    y_send(other_z, up, down, 5)
    stage_a(2)
    stage_b(1)
    stage_n(0)
    log_weights()
    stage_b(2)
    stage_a(3)
    for which in (1, 2, 3, 5):
        arrived(W.at[0:4, 0], wy.at[which])
    own_read(0)
    stage_c(1)
    stage_c(2)
    own_read(2)
    sum_y()
    stage_b(3)
    stage_n(1)
    stage_d(0, 2)
    sum_z()
    stage_c(3)
    stage_n(2)
    new_row_parts()
    stage_d(2)
    stage_n(3)
    stage_d(3)
    finish()
    arrived(OK, loc.at[6])
    arrived(OV, loc.at[7])

    arrived(R.at[0:31], lws)
    arrived(E1.at[0:3], es.at[0])
    arrived(E2.at[0:7], es.at[1])
    arrived(W.at[0:7, 0], ws1)
    arrived(W.at[0:6], ws2)
    arrived(T.at[0 : 28 * BLOCK], xs)

    def leg_done(i):
        dest, _, _, remote = first_leg(i)

        @pl.when(dest != s)
        def _():
            remote.wait_send()

    for i in range(4):
        leg_done(i)


def place(keys, values, weights, read, out_keys, out_values, out_weights, out_read, k, v, w, r, came, left):
    legs = []
    for at, (src, held, dst) in enumerate(
        (
            (values, v, out_values.at[0]),
            (keys, k, out_keys.at[0]),
            (weights, w, out_weights.at[0]),
            (read, r, out_read),
        )
    ):
        arrive = pltpu.make_async_copy(src, held, came.at[at])
        arrive.start()
        legs.append((arrive, pltpu.make_async_copy(held, dst, left.at[at])))
    for arrive, leave in reversed(legs):
        arrive.wait()
        leave.start()
    for _, leave in legs:
        leave.wait()


def per_device(
    tokens,
    new_rows,
    new_query,
    norm_gain,
    key_weight,
    value_weight,
    input_weight,
    forget_weight,
    forget_bias,
    gate_offsets,
):
    any_space = pl.BlockSpec(memory_space=pl.ANY)
    vmem = pl.BlockSpec(memory_space=pltpu.VMEM)
    smem = pl.BlockSpec(memory_space=pltpu.SMEM)
    dma = pltpu.SemaphoreType.DMA
    keys, values, weights, read = pl.pallas_call(
        kernel,
        out_shape=(
            jax.ShapeDtypeStruct((ROWS, 128), BF16),
            jax.ShapeDtypeStruct((ROWS, 256), BF16),
            jax.ShapeDtypeStruct((2, ROWS), F32),
            jax.ShapeDtypeStruct((4, 256), BF16),
        ),
        in_specs=[any_space] * 8 + [smem, any_space],
        out_specs=(any_space, any_space, vmem, vmem),
        scratch_shapes=[
            pltpu.VMEM((4, D), BF16),
            pltpu.VMEM((4, 128), BF16),
            pltpu.VMEM((16, 128), BF16),
            pltpu.VMEM((4, 2, 2, GROUP), F32),
            pltpu.VMEM((ROWS, D), BF16),
            pltpu.VMEM((ROWS, D), BF16),
            pltpu.VMEM((ROWS, D), BF16),
            pltpu.VMEM((8, 4, 64, 384), BF16),
            pltpu.VMEM((ROWS, 128), BF16),
            pltpu.VMEM((ROWS, 256), BF16),
            pltpu.VMEM((4, 32, GROUP), F32),
            pltpu.VMEM((32, D), BF16),
            pltpu.VMEM((8, D), F32),
            pltpu.VMEM((8, GROUP), F32),
            pltpu.VMEM((8, GROUP), F32),
            pltpu.VMEM((8, GROUP), F32),
            pltpu.VMEM((8, GROUP), F32),
            pltpu.VMEM((32, 1, 128), F32),
            pltpu.VMEM((32, 1, 128), F32),
            pltpu.VMEM((32, 128), F32),
            pltpu.VMEM((2, ROWS), F32),
            pltpu.VMEM((8, 128), F32),
            pltpu.VMEM((8, 128), F32),
            pltpu.VMEM((8, 256), F32),
            pltpu.VMEM((8, 128), F32),
            pltpu.VMEM((8, 128), F32),
            pltpu.VMEM((8, 128), F32),
            pltpu.VMEM((8, 32), F32),
            pltpu.VMEM((4, 16, 128), F32),
            pltpu.VMEM((8, 16, 128), F32),
            pltpu.VMEM((4, 256), F32),
            dma((4,)),
            dma((4,)),
            dma((4, 2)),
            dma((4, 2)),
            dma((4, 2)),
            dma((4,)),
            dma,
            dma,
            dma,
            dma,
            dma,
            dma,
            dma((6,)),
            dma,
            dma,
            dma((2,)),
            dma((2,)),
            dma((14,)),
        ],
        compiler_params=pltpu.CompilerParams(collective_id=0, has_side_effects=True),
    )(
        tokens.reshape(ROWS, D),
        new_rows,
        new_query,
        norm_gain.reshape(16, 128),
        key_weight,
        value_weight,
        input_weight.T,
        forget_weight.T,
        forget_bias,
        jnp.transpose(gate_offsets, (0, 2, 3, 1)),
    )
    return pl.pallas_call(
        place,
        out_shape=(
            jax.ShapeDtypeStruct((1, ROWS, 128), BF16),
            jax.ShapeDtypeStruct((1, ROWS, 256), BF16),
            jax.ShapeDtypeStruct((1, 2, ROWS), F32),
            jax.ShapeDtypeStruct((4, 256), BF16),
        ),
        in_specs=[any_space] * 4,
        out_specs=[any_space] * 4,
        scratch_shapes=[
            pltpu.VMEM((ROWS, 128), BF16),
            pltpu.VMEM((ROWS, 256), BF16),
            pltpu.VMEM((2, ROWS), F32),
            pltpu.VMEM((4, 256), BF16),
            dma((4,)),
            dma((4,)),
        ],
    )(keys, values, weights, read)


def solution(mesh):
    return jax.shard_map(
        per_device,
        mesh=mesh,
        in_specs=(
            P("gr", "sp", None),
            P("gr", None),
            P("gr", "tp"),
            P(),
            P("sp", "tp"),
            P("sp", "tp"),
            P(),
            P(),
            P("tp"),
            P("gr", "sp", None, "tp"),
        ),
        out_specs=(
            P(("gr", "sp"), None, "tp"),
            P(("gr", "sp"), None, "tp"),
            P(("gr", "sp"), "tp", None),
            P("gr", "tp"),
        ),
        check_vma=False,
    )
```

```python
import jax
import jax.numpy as jnp
from jax import lax
from jax.experimental import pallas as pl
from jax.experimental.pallas import tpu as pltpu
from jax.sharding import PartitionSpec as P

EPSILON = 1e-06
MESH = pl.DeviceIdType.MESH
F32 = jnp.float32
BF16 = jnp.bfloat16
NT = (((1,), (1,)), ((), ()))

D = 2048
ROWS = 1024
GROUP = 256
BLOCK = 32
CHUNK = 64


def iota(shape, dim):
    return lax.broadcasted_iota(jnp.int32, shape, dim)


def xor2(a, b):
    return 2 * ((a // 2 + b // 2) % 2) + (a % 2 + b % 2) % 2


def norm_chunk(read, write, gain_ref, rows):
    total = jnp.zeros((rows, 128), F32)
    for c in range(D // 128):
        v = read(c).astype(F32)
        total = total + v * v
    inverse = lax.rsqrt(jnp.sum(total, axis=-1, keepdims=True) * (1.0 / D) + EPSILON)
    for c in range(D // 128):
        v = read(c).astype(F32)
        write(c, (v * inverse * gain_ref[c : c + 1, :].astype(F32)).astype(BF16))


def norm_group(src, start, dst, first, gain_ref):
    def body(u, carry):
        at = pl.multiple_of(start + u * CHUNK, CHUNK)
        to = pl.multiple_of(first + u * CHUNK, CHUNK)

        def read(c):
            return src[pl.ds(at, CHUNK), c * 128 : (c + 1) * 128]

        def write(c, v):
            dst[pl.ds(to, CHUNK), c * 128 : (c + 1) * 128] = v

        norm_chunk(read, write, gain_ref, CHUNK)
        return carry

    lax.fori_loop(0, GROUP // CHUNK, body, 0)


def kernel(
    tokens,
    new_rows_in,
    new_query_in,
    gain_in,
    key_weight,
    value_weight,
    input_weight,
    forget_weight,
    bias,
    offsets_in,
    out_keys,
    out_values,
    out_weights,
    out_read,
    new_rows,
    new_query,
    gain,
    offsets,
    T,
    X,
    N,
    W,
    OK,
    OV,
    G,
    GW,
    NN,
    IG,
    PRE,
    LF,
    LOC,
    S,
    R,
    L,
    LW,
    PEAK,
    Q8,
    NUM,
    DEN,
    KN8,
    VN8,
    GN8,
    E1,
    E2,
    A0,
    p1s,
    p1r,
    xl,
    xr,
    xf,
    dr,
    xs,
    lws,
    lwr,
    wc,
    wh,
    w2,
    wy,
    ws1,
    ws2,
    es,
    er,
    loc,
):
    s = lax.axis_index("sp")
    t = lax.axis_index("tp")
    z, y = s // 4, s % 4
    x, c = t // 2, t % 2
    k_me = s // 8
    n_me = s // 8
    right = ((x + 1) % 4) * 2 + c
    left = ((x + 3) % 4) * 2 + c
    across = ((x + 2) % 4) * 2 + c
    mate = t + 1 - 2 * c

    barrier = pltpu.get_barrier_semaphore()

    way = 2 * (z // 4) - 1

    def greet(o, carry):
        pl.semaphore_signal(barrier, inc=1, device_id={"sp": (s + way * o + 32) % 32}, device_id_type=MESH)
        return carry

    lax.fori_loop(1, 32, greet, 0)
    for who in (right, left, mate):
        pl.semaphore_signal(barrier, inc=1, device_id={"tp": who}, device_id_type=MESH)

    own_k = pltpu.make_async_copy(key_weight, W.at[z, y, :, 0:128], loc.at[4])
    own_v = pltpu.make_async_copy(value_weight, W.at[z, y, :, 128:384], loc.at[5])
    own_k.start()
    own_v.start()
    loads = [
        pltpu.make_async_copy(tokens.at[n * GROUP : (n + 1) * GROUP], X.at[n * GROUP : (n + 1) * GROUP], loc.at[n])
        for n in range(4)
    ]
    loads[0].start()
    small = [
        pltpu.make_async_copy(src, dst, loc.at[8 + at])
        for at, (src, dst) in enumerate(
            (
                (gain_in, gain),
                (input_weight, GW.at[0:16]),
                (forget_weight, GW.at[16:32]),
                (offsets_in, offsets),
                (new_rows_in, new_rows),
                (new_query_in, new_query),
            )
        )
    ]
    for copy in small:
        copy.start()
    for load in loads[1:]:
        load.start()
    own_k.wait()
    own_v.wait()
    pl.semaphore_wait(barrier, 34)

    half_z = (z // 4) * 4
    other_z = 4 - half_z
    far_z = (z + 4) % 8

    def shard_to(row, to_z, recv):
        pltpu.make_async_remote_copy(
            src_ref=W.at[row, y],
            dst_ref=W.at[row, y],
            send_sem=ws1,
            recv_sem=recv,
            device_id={"sp": to_z * 4 + y},
            device_id_type=MESH,
        ).start()

    inner = (k_me // 2 + k_me % 2) % 2

    def sent_at(j):
        return inner * (0, 1, 2, 3)[j] + (1 - inner) * ((1 - c) * (0, 3, 2, 1)[j] + c * (0, 2, 3, 1)[j])

    def due_at(j):
        return inner * (0, 2, 1, 3)[j] + (1 - inner) * ((1 - c) * (0, 3, 1, 2)[j] + c * (0, 1, 3, 2)[j])

    def slot(i):
        return xor2(k_me, i)

    def first_leg(i):
        dest = (t - s + i + 32) % 8 + 8 * slot(i)
        src = tokens.at[pl.ds(pl.multiple_of(dest * BLOCK, BLOCK), BLOCK)]
        dst = T.at[pl.ds(pl.multiple_of(s * BLOCK, BLOCK), BLOCK)]
        remote = pltpu.make_async_remote_copy(
            src_ref=src,
            dst_ref=dst,
            send_sem=p1s.at[i],
            recv_sem=p1r.at[i],
            device_id={"sp": dest},
            device_id_type=MESH,
        )
        return dest, src, dst, remote

    def start_leg(j):
        i = sent_at(j)
        dest, src, dst, remote = first_leg(i)

        @pl.when(dest != s)
        def _():
            remote.start()

        @pl.when(dest == s)
        def _():
            pltpu.make_async_copy(src, dst, p1r.at[i]).start()

    start_leg(0)
    shard_to(z, far_z, wc)
    for o in range(1, 4):
        shard_to(z, half_z + (z + o) % 4, wh)


    def y_send(rows, column, to_y, which):
        pltpu.make_async_remote_copy(
            src_ref=W.at[pl.ds(rows, 4), column],
            dst_ref=W.at[pl.ds(rows, 4), column],
            send_sem=ws2,
            recv_sem=wy.at[which],
            device_id={"sp": z * 4 + to_y},
            device_id_type=MESH,
        ).start()

    def arrived(ref, sem):
        pltpu.make_async_copy(ref, ref, sem).wait()

    up, down = (y + 1) % 4, (y + 3) % 4

    def gates(n):
        loads[n].wait()
        norm_group(X, n * GROUP, X, n * GROUP, gain)
        own = X[n * GROUP : (n + 1) * GROUP, :]
        G[n] = lax.dot_general(GW[...], own, NT, preferred_element_type=F32)

    lane = iota((8, 128), 1)
    head_row = iota((8, 128), 0)

    def local_weights():
        gate_row = iota((32, GROUP), 0)
        for n in range(4):
            for h in range(2):
                at = slice(2 * n + h, 2 * n + h + 1)
                mine = jnp.where(gate_row == 2 * t + h, G[n], 0.0)
                IG[at, :] = jnp.sum(mine, axis=0, keepdims=True) + offsets[n, 0, h : h + 1, :]
                mine = jnp.where(gate_row == 16 + 2 * t + h, G[n], 0.0)
                PRE[at, :] = jnp.sum(mine, axis=0, keepdims=True) + bias[h]
                LF[at, :] = offsets[n, 1, h : h + 1, :]

        wide_lane = iota((8, GROUP), 1)
        pre = PRE[...]
        soft = jnp.minimum(pre, 0.0) - jnp.log1p(jnp.exp(-jnp.abs(pre)))
        log_forget = soft + LF[...]
        suffix = log_forget
        step = 1
        while step < GROUP:
            suffix = suffix + jnp.where(wide_lane < GROUP - step, pltpu.roll(suffix, GROUP - step, 1), 0.0)
            step *= 2
        exclusive = jnp.where(wide_lane < GROUP - 1, pltpu.roll(suffix, GROUP - 1, 1), 0.0)
        local = IG[...] + exclusive
        LOC[...] = local
        total = suffix[:, 0:1]
        most = jnp.max(local, axis=1, keepdims=True)
        tail_part = jnp.where(lane - 64 == head_row, total, jnp.where(lane - 72 == head_row, most, 0.0))
        tail_part = jnp.broadcast_to(jnp.sum(tail_part, axis=0, keepdims=True), (8, 128))
        for half in range(2):
            part = local[:, half * 128 : (half + 1) * 128]
            for k in range(4):
                first = pltpu.roll(part, (128 - 32 * k) % 128, 1) if k else part
                second = pltpu.roll(pltpu.roll(part, 7, 0), (160 - 32 * k) % 128, 1) if k != 1 else pltpu.roll(part, 7, 0)
                row = jnp.where(lane < 32, first, jnp.where(lane < 64, second, tail_part))
                for n in range(4):
                    S[n * 8 + half * 4 + k] = row[2 * n : 2 * n + 1, :]
        R[pl.ds(s, 1)] = S[pl.ds(s, 1)]

        def send_rows(o, carry):
            peer = (s + o) % 32
            pltpu.make_async_remote_copy(
                src_ref=S.at[peer],
                dst_ref=R.at[s],
                send_sem=lws,
                recv_sem=lwr,
                device_id={"sp": peer},
                device_id_type=MESH,
            ).start()
            return carry

        lax.fori_loop(1, 32, send_rows, 0)

    def block_of(owner, i):
        at = ((owner - s + i + 32) % 8 + 8 * slot(i)) * BLOCK
        return T.at[pl.ds(pl.multiple_of(at, BLOCK), BLOCK)]

    def pass_on(owner, i, to, recv):
        block = block_of(owner, i)
        pltpu.make_async_remote_copy(
            src_ref=block,
            dst_ref=block,
            send_sem=xs,
            recv_sem=recv,
            device_id={"tp": to},
            device_id_type=MESH,
        ).start()

    half_block = BLOCK // 2

    def pass_half(owner, i, half, to, recv):
        at = ((owner - s + i + 32) % 8 + 8 * slot(i)) * BLOCK + half * half_block
        part = T.at[pl.ds(pl.multiple_of(at, half_block), half_block)]
        pltpu.make_async_remote_copy(
            src_ref=part,
            dst_ref=part,
            send_sem=xs,
            recv_sem=recv,
            device_id={"tp": to},
            device_id_type=MESH,
        ).start()

    one_block = T.at[0:BLOCK]

    half_rows = T.at[0:half_block]

    def stage_a(j):
        i = due_at(j)
        arrived(one_block, p1r.at[i])
        for half in range(2):
            pass_half(t, i, half, right, xl.at[i, half])
            pass_half(t, i, 1 - half, left, xr.at[i, 1 - half])
        pass_on(t, i, mate, dr.at[i])

    def stage_b(j):
        i = due_at(j)
        arrived(half_rows, xl.at[i, 0])
        pass_half(left, i, 0, right, xf.at[i, 0])
        arrived(half_rows, xr.at[i, 1])
        pass_half(right, i, 1, left, xf.at[i, 1])
        arrived(half_rows, xl.at[i, 1])
        pass_on(left, i, mate, dr.at[i])
        arrived(half_rows, xr.at[i, 0])
        pass_on(right, i, mate, dr.at[i])

    def stage_c(j):
        i = due_at(j)
        arrived(half_rows, xf.at[i, 0])
        arrived(half_rows, xf.at[i, 1])
        pass_on(across, i, mate, dr.at[i])

    def write_out(i):
        at = pl.ds(pl.multiple_of(slot(i) * GROUP, GROUP), GROUP)
        return (
            pltpu.make_async_copy(OK.at[at], out_keys.at[at], loc.at[6]),
            pltpu.make_async_copy(OV.at[at], out_values.at[at], loc.at[7]),
        )

    def stage_n(j):
        i = due_at(j)
        arrived(T.at[0 : 4 * BLOCK], dr.at[i])
        start = pl.multiple_of(slot(i) * GROUP, GROUP)
        norm_group(T, start, N, j * GROUP, gain)

    def stage_d(j, groups=1):
        keys, values = project(N[j * GROUP : (j + groups) * GROUP, :])
        for g in range(groups):
            i = due_at(j + g)
            start = pl.multiple_of(slot(i) * GROUP, GROUP)
            OK[pl.ds(start, GROUP), :] = keys[g * GROUP : (g + 1) * GROUP]
            OV[pl.ds(start, GROUP), :] = values[g * GROUP : (g + 1) * GROUP]
            for copy in write_out(i):
                copy.start()

    def column(row, first):
        return jnp.sum(jnp.where(lane - first == head_row, row, 0.0), axis=1, keepdims=True)

    def log_weights():
        arrived(R.at[0:31], lwr)
        received = R[:, 0, :]
        row = iota((32, 128), 0)
        lane32 = iota((32, 128), 1)
        suffix = received
        step = 1
        while step < 32:
            suffix = suffix + jnp.where(row < 32 - step, pltpu.roll(suffix, 32 - step, 0), 0.0)
            step *= 2
        exclusive = jnp.where(row < 31, pltpu.roll(suffix, 31, 0), 0.0)
        peaks = jnp.max(received + pltpu.roll(exclusive, 8, 1), axis=0, keepdims=True)
        PEAK[...] = jnp.broadcast_to(column(peaks, 72), (8, 128))
        mine = jnp.sum(jnp.where(row == s, exclusive, 0.0), axis=0, keepdims=True)
        LOC[...] += column(mine, 64)
        tails = [
            jnp.sum(jnp.where(lane32 == 64 + 2 * n_me + h, exclusive, 0.0), axis=1, keepdims=True)
            for h in range(2)
        ]
        L[...] = received + jnp.where(lane32 < 32, tails[0], tails[1])
        for h in range(2):
            wide = jnp.zeros((8, 128), F32)
            for k in range(4):
                rows = L[pl.ds(k, 8, stride=4), :]
                shift = (32 * k - 32 * h) % 128
                moved = pltpu.roll(rows, shift, 1) if shift else rows
                wide = jnp.where((lane >= 32 * k) & (lane < 32 * k + 32), moved, wide)
            for g in range(8):
                LW[h : h + 1, g * 128 : (g + 1) * 128] = wide[g : g + 1, :]
        out_weights[...] = LW[...]

        query = new_query[...].astype(F32)
        for n in range(4):
            Q8[2 * n : 2 * n + 1, :] = jnp.where(lane1 < 64, query[n : n + 1, :], 0.0)
            Q8[2 * n + 1 : 2 * n + 2, :] = jnp.where(lane1 < 64, 0.0, query[n : n + 1, :])
        NUM[...] = jnp.zeros_like(NUM)
        DEN[...] = jnp.zeros_like(DEN)

    def project(rows):
        both = jnp.dot(rows, W[...].reshape(D, 384), preferred_element_type=F32)
        return (both[:, 0:128] * 0.125).astype(BF16), both[:, 128:384].astype(BF16)

    def own_read(n):
        keys, values = project(X[n * GROUP : (n + 2) * GROUP, :])
        scores = lax.dot_general(Q8[...].astype(BF16), keys, NT, preferred_element_type=F32)
        weight = jnp.exp(LOC[...] - PEAK[:, 0:1])
        terms = jnp.concatenate([weight, weight], axis=1) * scores
        prompt = n + iota((8, 2 * GROUP), 1) // GROUP
        terms = jnp.where(iota((8, 2 * GROUP), 0) // 2 == prompt, terms, 0.0)
        DEN[...] += jnp.broadcast_to(jnp.sum(terms, axis=1, keepdims=True), (8, 128))
        NUM[...] += jnp.dot(terms.astype(BF16), values, preferred_element_type=F32)

    def share(buffer, slot_of, peers, send, recv):
        for to in peers:
            pltpu.make_async_remote_copy(
                src_ref=buffer.at[slot_of],
                dst_ref=buffer.at[slot_of],
                send_sem=send,
                recv_sem=recv,
                device_id={"sp": to},
                device_id_type=MESH,
            ).start()

    def sum_y():
        value = jnp.where(head_row % 2 == 0, NUM[:, 0:128], NUM[:, 128:256])
        E1[pl.ds(y, 1)] = jnp.concatenate([value, DEN[...]], axis=0).reshape(1, 16, 128)
        share(E1, y, [z * 4 + (y + o) % 4 for o in range(1, 4)], es.at[0], er.at[0])

    def sum_z():
        arrived(E1.at[0:3], er.at[0])
        E2[pl.ds(z, 1)] = ((E1[0] + E1[1]) + (E1[2] + E1[3])).reshape(1, 16, 128)
        share(E2, z, [((z + o) % 8) * 4 + y for o in range(1, 8)], es.at[1], er.at[1])

    def finish():
        arrived(E2.at[0:7], er.at[1])
        total = jnp.sum(E2[...], axis=0)
        numerator, denominator = total[0:8], total[8:16, 0:1]
        peak = PEAK[:, 0:1]
        gate = jnp.sum(
            jnp.where(iota((8, 32), 1) == 2 * t + iota((8, 32), 0) % 2, GN8[...], 0.0), axis=1, keepdims=True
        )
        own = jnp.sum(Q8[...] * (KN8[...] * 0.125).astype(BF16).astype(F32), axis=1, keepdims=True)
        top = jnp.maximum(peak, gate)
        old_part = jnp.exp(peak - top)
        new_part = jnp.exp(gate - top) * own
        value = old_part * numerator + new_part * VN8[...].astype(BF16).astype(F32)
        weight = old_part * denominator + new_part
        read = value / jnp.maximum(jnp.abs(weight), 1.0)
        for n in range(4):
            for h in range(2):
                A0[n : n + 1, h * 128 : (h + 1) * 128] = read[2 * n + h : 2 * n + h + 1, :]
        out_read[...] = A0[...].astype(BF16)

    lane1 = iota((1, 128), 1)

    def new_row_parts():
        total = jnp.zeros((4, 128), F32)
        for g in range(D // 128):
            v = new_rows[:, g * 128 : (g + 1) * 128].astype(F32)
            total = total + v * v
        inverse = lax.rsqrt(jnp.sum(total, axis=-1, keepdims=True) * (1.0 / D) + EPSILON)
        NN[...] = jnp.zeros_like(NN)
        for g in range(D // 128):
            at = slice(g * 128, (g + 1) * 128)
            NN[0:4, at] = new_rows[:, at].astype(F32) * inverse * gain[g : g + 1, :].astype(F32)
        fresh = NN[...].astype(BF16)
        both = jnp.dot(fresh, W[...].reshape(D, 384), preferred_element_type=F32)
        gates_new = lax.dot_general(fresh, GW[...], NT, preferred_element_type=F32)
        for n in range(4):
            for h in range(2):
                at = slice(2 * n + h, 2 * n + h + 1)
                KN8[at, :] = both[n : n + 1, 0:128]
                VN8[at, :] = both[n : n + 1, 128 * (h + 1) : 128 * (h + 2)]
                GN8[at, :] = gates_new[n : n + 1, :]

    for copy in small:
        copy.wait()
    for n in range(4):
        gates(n)
    local_weights()
    arrived(W.at[0, 0], wc)
    for o in range(1, 4):
        shard_to(far_z, half_z + (z + o) % 4, w2)
    arrived(W.at[0:3, 0], wh)
    y_send(half_z, y, up, 0)
    y_send(half_z, y, down, 1)
    start_leg(1)

    @pl.when(inner == 0)
    def _():
        start_leg(2)

    arrived(W.at[0:4, 0], wy.at[0])
    y_send(half_z, down, up, 2)

    @pl.when(inner == 1)
    def _():
        start_leg(2)

    start_leg(3)
    stage_a(0)
    arrived(W.at[0:3, 0], w2)
    y_send(other_z, y, up, 3)
    y_send(other_z, y, down, 4)
    stage_b(0)
    stage_a(1)
    stage_c(0)
    arrived(W.at[0:4, 0], wy.at[4])
    y_send(other_z, up, down, 5)
    stage_a(2)
    stage_b(1)
    stage_n(0)
    log_weights()
    stage_b(2)
    stage_a(3)
    for which in (1, 2, 3, 5):
        arrived(W.at[0:4, 0], wy.at[which])
    own_read(0)
    stage_c(1)
    stage_c(2)
    own_read(2)
    sum_y()
    stage_b(3)
    stage_n(1)
    stage_d(0, 2)
    sum_z()
    stage_c(3)
    stage_n(2)
    new_row_parts()
    stage_d(2)
    stage_n(3)
    stage_d(3)
    finish()
    arrived(OK, loc.at[6])
    arrived(OV, loc.at[7])

    arrived(R.at[0:31], lws)
    arrived(E1.at[0:3], es.at[0])
    arrived(E2.at[0:7], es.at[1])
    arrived(W.at[0:7, 0], ws1)
    arrived(W.at[0:6], ws2)
    arrived(T.at[0 : 28 * BLOCK], xs)

    def leg_done(i):
        dest, _, _, remote = first_leg(i)

        @pl.when(dest != s)
        def _():
            remote.wait_send()

    for i in range(4):
        leg_done(i)


def place(keys, values, weights, read, out_keys, out_values, out_weights, out_read, sems):
    copies = [
        pltpu.make_async_copy(keys, out_keys.at[0], sems.at[0]),
        pltpu.make_async_copy(values, out_values.at[0], sems.at[1]),
        pltpu.make_async_copy(weights, out_weights.at[0], sems.at[2]),
        pltpu.make_async_copy(read, out_read, sems.at[3]),
    ]
    for copy in copies:
        copy.start()
    for copy in copies:
        copy.wait()


def per_device(
    tokens,
    new_rows,
    new_query,
    norm_gain,
    key_weight,
    value_weight,
    input_weight,
    forget_weight,
    forget_bias,
    gate_offsets,
):
    any_space = pl.BlockSpec(memory_space=pl.ANY)
    vmem = pl.BlockSpec(memory_space=pltpu.VMEM)
    smem = pl.BlockSpec(memory_space=pltpu.SMEM)
    dma = pltpu.SemaphoreType.DMA
    keys, values, weights, read = pl.pallas_call(
        kernel,
        out_shape=(
            jax.ShapeDtypeStruct((ROWS, 128), BF16),
            jax.ShapeDtypeStruct((ROWS, 256), BF16),
            jax.ShapeDtypeStruct((2, ROWS), F32),
            jax.ShapeDtypeStruct((4, 256), BF16),
        ),
        in_specs=[any_space] * 8 + [smem, any_space],
        out_specs=(any_space, any_space, vmem, vmem),
        scratch_shapes=[
            pltpu.VMEM((4, D), BF16),
            pltpu.VMEM((4, 128), BF16),
            pltpu.VMEM((16, 128), BF16),
            pltpu.VMEM((4, 2, 2, GROUP), F32),
            pltpu.VMEM((ROWS, D), BF16),
            pltpu.VMEM((ROWS, D), BF16),
            pltpu.VMEM((ROWS, D), BF16),
            pltpu.VMEM((8, 4, 64, 384), BF16),
            pltpu.VMEM((ROWS, 128), BF16),
            pltpu.VMEM((ROWS, 256), BF16),
            pltpu.VMEM((4, 32, GROUP), F32),
            pltpu.VMEM((32, D), BF16),
            pltpu.VMEM((8, D), F32),
            pltpu.VMEM((8, GROUP), F32),
            pltpu.VMEM((8, GROUP), F32),
            pltpu.VMEM((8, GROUP), F32),
            pltpu.VMEM((8, GROUP), F32),
            pltpu.VMEM((32, 1, 128), F32),
            pltpu.VMEM((32, 1, 128), F32),
            pltpu.VMEM((32, 128), F32),
            pltpu.VMEM((2, ROWS), F32),
            pltpu.VMEM((8, 128), F32),
            pltpu.VMEM((8, 128), F32),
            pltpu.VMEM((8, 256), F32),
            pltpu.VMEM((8, 128), F32),
            pltpu.VMEM((8, 128), F32),
            pltpu.VMEM((8, 128), F32),
            pltpu.VMEM((8, 32), F32),
            pltpu.VMEM((4, 16, 128), F32),
            pltpu.VMEM((8, 16, 128), F32),
            pltpu.VMEM((4, 256), F32),
            dma((4,)),
            dma((4,)),
            dma((4, 2)),
            dma((4, 2)),
            dma((4, 2)),
            dma((4,)),
            dma,
            dma,
            dma,
            dma,
            dma,
            dma,
            dma((6,)),
            dma,
            dma,
            dma((2,)),
            dma((2,)),
            dma((14,)),
        ],
        compiler_params=pltpu.CompilerParams(collective_id=0, has_side_effects=True),
    )(
        tokens.reshape(ROWS, D),
        new_rows,
        new_query,
        norm_gain.reshape(16, 128),
        key_weight,
        value_weight,
        input_weight.T,
        forget_weight.T,
        forget_bias,
        jnp.transpose(gate_offsets, (0, 2, 3, 1)),
    )
    return pl.pallas_call(
        place,
        out_shape=(
            jax.ShapeDtypeStruct((1, ROWS, 128), BF16),
            jax.ShapeDtypeStruct((1, ROWS, 256), BF16),
            jax.ShapeDtypeStruct((1, 2, ROWS), F32),
            jax.ShapeDtypeStruct((4, 256), BF16),
        ),
        in_specs=[vmem] * 4,
        out_specs=[any_space] * 4,
        scratch_shapes=[dma((4,))],
    )(keys, values, weights, read)


def solution(mesh):
    return jax.shard_map(
        per_device,
        mesh=mesh,
        in_specs=(
            P("gr", "sp", None),
            P("gr", None),
            P("gr", "tp"),
            P(),
            P("sp", "tp"),
            P("sp", "tp"),
            P(),
            P(),
            P("tp"),
            P("gr", "sp", None, "tp"),
        ),
        out_specs=(
            P(("gr", "sp"), None, "tp"),
            P(("gr", "sp"), None, "tp"),
            P(("gr", "sp"), "tp", None),
            P("gr", "tp"),
        ),
        check_vma=False,
    )
```
